32 devices in a mesh: fs: 16 (over z, y, x), tp: 2 (over core).
Axes of the slice: x: 2, y: 2, z: 4, core: 2. Of those that a mesh axis runs over, the one named last changes fastest.
Arguments:
- tokens: bfloat16 [2048, 2048], P('fs'), may hold values from -6 to 6
- norm_gain: float32 [2048], replicated, may hold values from 0.1 to 1.9
- w_query: bfloat16 [2048, 1024], P('fs', 'tp'), may hold values from -0.125 to 0.125
- w_key: bfloat16 [2048, 1024], P('fs', 'tp'), may hold values from -0.125 to 0.125
- w_value: bfloat16 [2048, 2048], P('fs', 'tp'), may hold values from -0.125 to 0.125
- w_gate: bfloat16 [2048, 2048], P('fs', 'tp'), may hold values from -0.125 to 0.125
- mixer_gain: float32 [2048], P('tp'), may hold values from 0.1 to 1.9
- w_out: bfloat16 [2048, 2048], P('tp', 'fs'), may hold values from -0.125 to 0.125
- channel_gain: float32 [2048], replicated, may hold values from 0.1 to 1.9
- w_left: bfloat16 [2048, 3072], P('fs', 'tp'), may hold values from -0.125 to 0.125
- w_right: bfloat16 [2048, 3072], P('fs', 'tp'), may hold values from -0.125 to 0.125
- taps_left: float32 [3, 3072], P(None, 'tp'), may hold values from -3.5 to 3.5
- taps_right: float32 [3, 3072], P(None, 'tp'), may hold values from -3.5 to 3.5
- w_down: bfloat16 [3072, 2048], P('tp', 'fs'), may hold values from -0.109375 to 0.109375
Outputs:
- layer_out: bfloat16 [2048, 2048], P('fs')
The draws below stay inside these ranges and needn't reach their ends.
All inputs are finite; a program needn't handle non-finite values.
Results may differ from the reference program's by a relative error of at most 0.018.
Values may be sent and summed in bfloat16 or wider, within the bound.
A program may use at most 64 MiB of HBM per device.

```python
import jax
import jax.numpy as jnp
from jax import lax

D = 2048
HEADS = 8
DK = 128
DV = 256
FF = 3072
BLOCK = 128
SEQ_LEN = 128
QW = 1024
VW = 2048
TOKENS = 2048
N_TP = 2


def shard_levels(key, shape, pieces, least, top_value):
    level = 1.0
    for axis_at, shards_of in pieces:
        heights = jax.random.uniform(jax.random.fold_in(jax.random.fold_in(key, 6), axis_at), (shards_of,), jnp.float32, least / len(pieces), top_value / len(pieces))
        level = level * jnp.repeat(jnp.exp(heights), shape[axis_at] // shards_of).reshape((-1,) + (1,) * (len(shape) - 1 - axis_at))
    return level


def normal_values(own_key, dims, spread, most, shards=(), held_as=jnp.bfloat16):
    level = shard_levels(own_key, dims, shards, -0.22, 0.18) if shards else 1.0
    drawn = jax.random.normal(own_key, dims, jnp.float32) * spread * level
    return jnp.minimum(jnp.maximum(drawn, -most), most).astype(held_as)


def setup_inputs(seed: int = 0) -> dict:
    keys = jax.random.split(jax.random.key(seed), 15)
    tokens = normal_values(keys[0], (TOKENS, D), 1.0, 6.0, ((0, 16),))
    norm_gain = jnp.clip(1.0 + 0.18 * jax.random.normal(keys[1], (D,), jnp.float32), 0.1, 1.9)
    w_query = normal_values(keys[2], (D, QW), D ** -0.5, 0.125, ((0, 16), (1, 2)))
    w_key = normal_values(keys[3], (D, QW), D ** -0.5, 0.125, ((0, 16), (1, 2)))
    w_value = normal_values(keys[4], (D, VW), D ** -0.5, 0.125, ((0, 16), (1, 2)))
    w_gate = normal_values(keys[5], (D, VW), D ** -0.5, 0.125, ((0, 16), (1, 2)))
    mixer_gain = jnp.clip(1.0 + 0.18 * jax.random.normal(keys[6], (VW,), jnp.float32), 0.1, 1.9)
    w_out = normal_values(keys[7], (VW, D), VW ** -0.5, 0.125, ((0, 2), (1, 16)))
    channel_gain = jnp.clip(1.0 + 0.18 * jax.random.normal(keys[8], (D,), jnp.float32), 0.1, 1.9)
    w_left = normal_values(keys[9], (D, FF), D ** -0.5, 0.125, ((0, 16), (1, 2)))
    w_right = normal_values(keys[10], (D, FF), D ** -0.5, 0.125, ((0, 16), (1, 2)))
    taps_left = normal_values(keys[11], (3, FF), 3 ** -0.5, 3.5, ((1, 2),), jnp.float32)
    taps_right = normal_values(keys[12], (3, FF), 3 ** -0.5, 3.5, ((1, 2),), jnp.float32)
    w_down = normal_values(keys[13], (FF, D), FF ** -0.5, 0.109375, ((0, 2), (1, 16)))
    return dict(tokens=tokens, norm_gain=norm_gain, w_query=w_query, w_key=w_key, w_value=w_value, w_gate=w_gate, mixer_gain=mixer_gain, w_out=w_out, channel_gain=channel_gain, w_left=w_left, w_right=w_right, taps_left=taps_left, taps_right=taps_right, w_down=w_down)


highest = lax.Precision.HIGHEST

def scale_rows(rows_in, gain_vec):
    floats = rows_in.astype(jnp.float32)
    factor = lax.rsqrt(lax.optimization_barrier(jnp.mean(floats * floats, axis=-1, keepdims=True)) + 1e-06)
    return (floats * factor * gain_vec.astype(jnp.float32)).astype(jnp.bfloat16)

def decays(first_head, count):
    head_ids = first_head + jnp.arange(count, dtype=jnp.float32)
    return jnp.log(1.0 - 2.0 ** (-5.0 - head_ids))

def rotate(heads_in, positions):
    width = heads_in.shape[-1]
    half = width // 2
    freqs = 10000.0 ** (-jnp.arange(half, dtype=jnp.float32) / half)
    angles = positions[:, None] * freqs[None, :]
    cosine = jnp.cos(angles)
    sine = jnp.sin(angles)
    first_half = heads_in[..., :half]
    second_half = heads_in[..., half:]
    return jnp.concatenate([first_half * cosine - second_half * sine, first_half * sine + second_half * cosine], axis=-1)

def retention(queries, keys_in, values_in, log_gamma):
    head_count, length, key_width = queries.shape
    value_width = values_in.shape[-1]
    blocks = length // BLOCK
    queries = queries.reshape(head_count, blocks, BLOCK, key_width)
    keys_in = keys_in.reshape(head_count, blocks, BLOCK, key_width)
    values_in = values_in.reshape(head_count, blocks, BLOCK, value_width)
    offsets = jnp.arange(BLOCK, dtype=jnp.float32)
    distance = offsets[:, None] - offsets[None, :]
    weights = jnp.where(distance >= 0, jnp.exp(log_gamma[:, None, None] * jnp.maximum(distance, 0.0)), 0.0)
    scores = jnp.einsum('hbnd,hbmd->hbnm', queries, keys_in, precision=highest) * weights[:, None]
    inner = jnp.einsum('hbnm,hbme->hbne', scores, values_in, precision=highest)
    key_weight = jnp.exp(log_gamma[:, None] * (BLOCK - 1 - offsets)[None, :])
    contrib = jnp.einsum('hbjd,hbje->hbde', keys_in * key_weight[:, None, :, None], values_in, precision=highest)
    block_decay = jnp.exp(log_gamma * BLOCK)[:, None, None]

    def advance(state, contrib_block):
        return (state * block_decay + contrib_block, state)
    _, states = lax.scan(advance, jnp.zeros((head_count, key_width, value_width), jnp.float32), jnp.moveaxis(contrib, 1, 0))
    states = jnp.moveaxis(states, 0, 1)
    query_weight = jnp.exp(log_gamma[:, None] * (offsets + 1.0)[None, :])
    carried = jnp.einsum('hbnd,hbde->hbne', queries, states, precision=highest) * query_weight[:, None, :, None]
    return (inner + carried).reshape(head_count, length, value_width)

def head_norm(retained):
    return retained * lax.rsqrt(lax.optimization_barrier(jnp.mean(retained * retained, axis=-1, keepdims=True)) + 1e-06)

def causal_taps(values_in, taps):
    length = values_in.shape[-2]
    spacing = [(0, 0)] * (values_in.ndim - 2) + [(taps.shape[0] - 1, 0), (0, 0)]
    padded = jnp.pad(values_in.astype(jnp.float32), spacing)
    result = padded[..., 0:length, :] * taps[0]
    for tap_index in range(1, taps.shape[0]):
        result = result + padded[..., tap_index:tap_index + length, :] * taps[tap_index]
    return result

def group_sum(left, weight):
    span = left.shape[1] // N_TP
    running = jnp.zeros((left.shape[0], weight.shape[1]), jnp.float32)
    for group in range(N_TP):
        partial_sum = jnp.dot(left[:, group * span:(group + 1) * span], weight[group * span:(group + 1) * span], preferred_element_type=jnp.float32).astype(jnp.bfloat16)
        running = running + lax.optimization_barrier(partial_sum).astype(jnp.float32)
    return running

def reference(tokens, norm_gain, w_query, w_key, w_value, w_gate, mixer_gain, w_out, channel_gain, w_left, w_right, taps_left, taps_right, w_down):
    seq_count = tokens.shape[0] // SEQ_LEN
    normed = scale_rows(tokens, norm_gain)

    def project(source, weight):
        return jnp.dot(source, weight, preferred_element_type=jnp.float32).astype(jnp.bfloat16)
    queries = project(normed, w_query)
    keys_proj = project(normed, w_key)
    values_proj = project(normed, w_value)
    gates = project(normed, w_gate)
    positions = jnp.arange(SEQ_LEN, dtype=jnp.float32)
    log_gamma = decays(0.0, HEADS)

    def split_heads(rows_in, width):
        return rows_in.astype(jnp.float32).reshape(seq_count, SEQ_LEN, HEADS, width).transpose(0, 2, 1, 3)

    def one_sequence(triple):
        query_heads, key_heads, value_heads = triple
        return head_norm(retention(rotate(query_heads, positions), rotate(key_heads, positions), value_heads, log_gamma))
    retained = lax.map(one_sequence, (split_heads(queries, DK), split_heads(keys_proj, DK), split_heads(values_proj, DV)))
    retained = retained.transpose(0, 2, 1, 3).reshape(seq_count * SEQ_LEN, VW)
    hidden = (retained * mixer_gain * jax.nn.silu(gates.astype(jnp.float32))).astype(jnp.bfloat16)
    middle = (tokens.astype(jnp.float32) + group_sum(hidden, w_out)).astype(jnp.bfloat16)
    normed_mid = scale_rows(middle, channel_gain)
    left = project(normed_mid, w_left)
    right = project(normed_mid, w_right)

    def convolve(rows_in, taps):
        return causal_taps(rows_in.reshape(seq_count, SEQ_LEN, FF), taps).reshape(seq_count * SEQ_LEN, FF)
    gated = (jax.nn.silu(convolve(left, taps_left)) * convolve(right, taps_right)).astype(jnp.bfloat16)
    return (middle.astype(jnp.float32) + group_sum(gated, w_down)).astype(jnp.bfloat16)
```

```python
import functools

import jax
import jax.numpy as jnp
import numpy as np
from jax import lax
from jax.experimental import pallas as pl
from jax.experimental.pallas import tpu as pltpu
from jax.sharding import PartitionSpec as P

DK = 128
DV = 256
BLOCK = 128
MESH = pl.DeviceIdType.MESH


highest = lax.Precision.HIGHEST


def scale_rows(rows_in, gain_vec):
    floats = rows_in.astype(jnp.float32)
    factor = lax.rsqrt(jnp.mean(floats * floats, axis=-1, keepdims=True) + 1e-06)
    return (floats * factor * gain_vec).astype(jnp.bfloat16)


def decays(first_head, count):
    head_ids = first_head + jnp.arange(count, dtype=jnp.float32)
    return jnp.log(1.0 - 2.0 ** (-5.0 - head_ids))


def rotate(heads_in, positions):
    width = heads_in.shape[-1]
    half = width // 2
    freqs = 10000.0 ** (-jnp.arange(half, dtype=jnp.float32) / half)
    angles = positions[:, None] * freqs[None, :]
    cosine = jnp.cos(angles)
    sine = jnp.sin(angles)
    first_half = heads_in[..., :half]
    second_half = heads_in[..., half:]
    return jnp.concatenate(
        [first_half * cosine - second_half * sine, first_half * sine + second_half * cosine],
        axis=-1,
    )


def retention(queries, keys_in, values_in, log_gamma):
    head_count, length, key_width = queries.shape
    value_width = values_in.shape[-1]
    blocks = length // BLOCK
    queries = queries.reshape(head_count, blocks, BLOCK, key_width)
    keys_in = keys_in.reshape(head_count, blocks, BLOCK, key_width)
    values_in = values_in.reshape(head_count, blocks, BLOCK, value_width)
    offsets = jnp.arange(BLOCK, dtype=jnp.float32)
    distance = offsets[:, None] - offsets[None, :]
    weights = jnp.where(
        distance >= 0, jnp.exp(log_gamma[:, None, None] * jnp.maximum(distance, 0.0)), 0.0
    )
    scores = jnp.einsum("hbnd,hbmd->hbnm", queries, keys_in, precision=highest) * weights[:, None]
    inner = jnp.einsum("hbnm,hbme->hbne", scores, values_in, precision=highest)
    key_weight = jnp.exp(log_gamma[:, None] * (BLOCK - 1 - offsets)[None, :])
    contrib = jnp.einsum(
        "hbjd,hbje->hbde", keys_in * key_weight[:, None, :, None], values_in, precision=highest
    )
    block_decay = jnp.exp(log_gamma * BLOCK)[:, None, None]

    def advance(state, contrib_block):
        return (state * block_decay + contrib_block, state)

    _, states = lax.scan(
        advance,
        jnp.zeros((head_count, key_width, value_width), jnp.float32),
        jnp.moveaxis(contrib, 1, 0),
    )
    states = jnp.moveaxis(states, 0, 1)
    query_weight = jnp.exp(log_gamma[:, None] * (offsets + 1.0)[None, :])
    carried = (
        jnp.einsum("hbnd,hbde->hbne", queries, states, precision=highest)
        * query_weight[:, None, :, None]
    )
    return (inner + carried).reshape(head_count, length, value_width)


def head_norm(retained):
    return retained * lax.rsqrt(jnp.mean(retained * retained, axis=-1, keepdims=True) + 1e-06)


def causal_taps(values_in, taps):
    length = values_in.shape[-2]
    padded = jnp.pad(values_in.astype(jnp.float32), ((taps.shape[0] - 1, 0), (0, 0)))
    result = padded[0:length] * taps[0]
    for tap_index in range(1, taps.shape[0]):
        result = result + padded[tap_index : tap_index + length] * taps[tap_index]
    return result


def fold_single(source, weight_piece):
    return jnp.dot(source, weight_piece, preferred_element_type=jnp.float32)


def collect_single(source, weight):
    return fold_single(source, lax.all_gather(weight, "fs", axis=0, tiled=True))


def plain_body(
    tokens,
    norm_gain,
    w_query,
    w_key,
    w_value,
    w_gate,
    mixer_gain,
    w_out,
    channel_gain,
    w_left,
    w_right,
    taps_left,
    taps_right,
    w_down,
):
    length = tokens.shape[0]
    normed = scale_rows(tokens, norm_gain)
    queries = collect_single(normed, w_query)
    keys_proj = collect_single(normed, w_key)
    values_proj = collect_single(normed, w_value)
    gates = collect_single(normed, w_gate)
    queries = queries.astype(jnp.bfloat16)
    keys_proj = keys_proj.astype(jnp.bfloat16)
    values_proj = values_proj.astype(jnp.bfloat16)
    gates = gates.astype(jnp.bfloat16)
    heads_here = w_query.shape[1] // DK
    first_head = (lax.axis_index("tp") * heads_here).astype(jnp.float32)
    log_gamma = decays(first_head, heads_here)
    positions = jnp.arange(length, dtype=jnp.float32)

    def split_heads(rows_in, width):
        return rows_in.astype(jnp.float32).reshape(length, heads_here, width).transpose(1, 0, 2)

    retained = head_norm(
        retention(
            rotate(split_heads(queries, DK), positions),
            rotate(split_heads(keys_proj, DK), positions),
            split_heads(values_proj, DV),
            log_gamma,
        )
    )
    retained = retained.transpose(1, 0, 2).reshape(length, heads_here * DV)
    hidden = (retained * mixer_gain * jax.nn.silu(gates.astype(jnp.float32))).astype(jnp.bfloat16)
    rows_own = length // lax.axis_size("tp")
    first_row = lax.axis_index("tp") * rows_own
    out_whole = lax.all_gather(w_out, "fs", axis=1, tiled=True)
    mixer_total = lax.psum_scatter(
        jnp.dot(hidden, out_whole, preferred_element_type=jnp.float32).astype(jnp.bfloat16),
        "tp",
        scatter_dimension=0,
        tiled=True,
    ).astype(jnp.float32)
    residual = lax.dynamic_slice_in_dim(tokens, first_row, rows_own, 0)
    middle_own = (residual.astype(jnp.float32) + mixer_total).astype(jnp.bfloat16)
    middle = lax.all_gather(middle_own, "tp", axis=0, tiled=True)
    normed_mid = scale_rows(middle, channel_gain)
    left = collect_single(normed_mid, w_left)
    right = collect_single(normed_mid, w_right)
    left = left.astype(jnp.bfloat16)
    right = right.astype(jnp.bfloat16)
    gated = (jax.nn.silu(causal_taps(left, taps_left)) * causal_taps(right, taps_right)).astype(
        jnp.bfloat16
    )
    down_whole = lax.all_gather(w_down, "fs", axis=1, tiled=True)
    channel_part = jnp.dot(gated, down_whole, preferred_element_type=jnp.float32)
    channel_total = lax.psum(channel_part.astype(jnp.bfloat16), "tp").astype(jnp.float32)
    return (middle.astype(jnp.float32) + channel_total).astype(jnp.bfloat16)


def log_gammas(head_count):
    table = np.log(1.0 - 2.0 ** (-5.0 - np.arange(head_count, dtype=np.float64)))
    return np.repeat(table[:, None], BLOCK, axis=1).astype(np.float32)


def turning(length, width):
    half = width // 2
    freqs = np.float32(10000.0) ** (-np.arange(half, dtype=np.float32) / np.float32(half))
    angles = (np.arange(length, dtype=np.float32)[:, None] * freqs[None, :]).astype(np.float64)
    cosine, sine = np.cos(angles), np.sin(angles)
    return (
        np.concatenate([cosine, cosine], axis=1).astype(np.float32),
        np.concatenate([-sine, sine], axis=1).astype(np.float32),
    )


def silu(v):
    return v / (1.0 + jnp.exp(-v))


def normed_rows(floats, gain):
    factor = lax.rsqrt(jnp.mean(floats * floats, axis=-1, keepdims=True) + 1e-06)
    return (floats * factor * gain).astype(jnp.bfloat16)


HOP, SUM, SWAP = 3, 4, 5
CHUNKS = 4
NT_PARTS = 2
CLASS_OF = (0, 0, 0, 1, 2, 3, 4, 5)
STAGES = (
    (0, 0),
    (0, 1),
    (1, 0),
    (1, 1),
    (2, 0),
    (2, 1),
    (2, 2),
    (2, 3),
    (3, 0),
    (3, 1),
    (3, 2),
    (3, 3),
    (4, 0),
    (5, 0),
    (4, 1),
    (5, 1),
    (4, 2),
    (5, 2),
    (4, 3),
    (5, 3),
    (6, 0),
    (6, 1),
    (6, 2),
    (6, 3),
)
PLAN = (
    (
        (
            (1, 0, 0, 0, 0, 0), (1, 1, 0, 0, 0, 0), (1, 3, 0, 0, 0), (1, 3, 0, 0, 1), (1, 1, 0, 1, 0, 0),
            (0, 1, 0, 0, 0, 0), (1, 3, 0, 0, 2), (1, 3, 0, 0, 3), (1, 0, 0, 1, 0, 0), (1, 3, 1, 0, 0),
            (1, 3, 1, 0, 1), (0, 3, 0, 0, 0), (0, 3, 0, 0, 1), (1, 3, 0, 0, 5), (1, 3, 0, 0, 4), (0, 0, 0, 0, 1, 1),
            (1, 1, 0, 0, 1, 1), (1, 3, 1, 0, 2), (1, 3, 1, 0, 3), (0, 3, 1, 0, 0), (0, 3, 1, 0, 1), (1, 2, 2, 3),
            (1, 3, 1, 0, 5), (1, 3, 1, 0, 4), (0, 1, 0, 0, 1, 1), (1, 3, 2, 0, 0), (1, 3, 2, 0, 1), (1, 3, 2, 0, 2),
            (1, 3, 2, 0, 3), (0, 0, 0, 1, 1, 1), (1, 1, 0, 1, 1, 1), (1, 3, 3, 0, 0), (1, 3, 3, 0, 1), (1, 2, 2, 1),
            (1, 3, 3, 0, 2), (1, 3, 3, 0, 3), (0, 3, 2, 0, 0), (0, 3, 2, 0, 1), (1, 2, 2, 2), (1, 3, 2, 0, 5),
            (1, 3, 2, 0, 4), (1, 3, 4, 0, 0), (1, 3, 4, 0, 1), (0, 3, 3, 0, 0), (0, 3, 3, 0, 1), (1, 3, 3, 0, 5),
            (1, 3, 3, 0, 4), (0, 0, 0, 0, 1, 2), (1, 1, 0, 0, 1, 2), (1, 2, 0, 3), (1, 3, 4, 0, 2), (1, 3, 4, 0, 3),
            (0, 1, 0, 0, 1, 2), (0, 3, 4, 0, 0), (0, 3, 4, 0, 1), (1, 3, 4, 0, 5), (1, 3, 4, 0, 4), (1, 2, 0, 1),
            (0, 0, 0, 1, 1, 2), (1, 1, 0, 1, 1, 2), (1, 2, 1, 3), (1, 3, 5, 0, 0), (1, 3, 5, 0, 1), (1, 3, 5, 0, 2),
            (1, 3, 5, 0, 3), (1, 2, 3, 3), (0, 2, 0, 3), (0, 3, 5, 0, 0), (0, 3, 5, 0, 1), (1, 3, 5, 0, 5),
            (1, 3, 5, 0, 4), (0, 0, 0, 0, 1, 3), (1, 1, 0, 0, 1, 3), (1, 2, 0, 2), (0, 2, 1, 3), (0, 2, 2, 3),
            (1, 3, 0, 3, 0), (1, 3, 0, 3, 1), (0, 1, 0, 0, 1, 3), (0, 1, 0, 1, 0, 0), (0, 1, 0, 1, 1, 1),
            (0, 1, 0, 1, 1, 2), (1, 2, 4, 3), (1, 3, 0, 3, 2), (1, 3, 0, 3, 3), (0, 3, 0, 3, 0), (0, 3, 0, 3, 1),
            (1, 3, 0, 3, 5), (1, 3, 0, 3, 4), (0, 2, 3, 3), (1, 2, 1, 1), (1, 3, 1, 3, 0), (1, 3, 1, 3, 1),
            (1, 2, 3, 1), (1, 3, 1, 3, 2), (1, 3, 1, 3, 3), (0, 0, 0, 1, 1, 3), (1, 1, 0, 1, 1, 3), (1, 2, 4, 1),
            (0, 3, 1, 3, 0), (0, 3, 1, 3, 1), (1, 3, 1, 3, 5), (1, 3, 1, 3, 4), (0, 2, 0, 2), (0, 1, 0, 1, 1, 3),
            (0, 3, 0, 0, 2), (0, 3, 0, 0, 3), (0, 3, 0, 0, 4), (0, 3, 0, 0, 5), (1, 2, 1, 2), (0, 2, 4, 3),
            (1, 3, 2, 3, 0), (1, 3, 2, 3, 1), (0, 2, 0, 1), (1, 3, 2, 3, 2), (1, 3, 2, 3, 3), (0, 2, 1, 1),
            (0, 2, 2, 1), (1, 2, 3, 2), (1, 3, 0, 1, 0), (1, 3, 0, 1, 1), (0, 3, 2, 3, 0), (0, 3, 2, 3, 1),
            (1, 3, 0, 1, 2), (1, 3, 0, 1, 3), (0, 2, 3, 1), (1, 2, 4, 2), (0, 2, 1, 2), (0, 2, 2, 2), (1, 3, 0, 2, 0),
            (1, 3, 0, 2, 1), (0, 3, 0, 1, 0), (0, 3, 0, 1, 1), (1, 3, 0, 1, 5), (1, 3, 0, 1, 4), (0, 2, 4, 1),
            (0, 3, 0, 1, 2), (0, 3, 0, 1, 3), (1, 2, 5, 3), (0, 2, 3, 2), (1, 3, 0, 2, 2), (1, 3, 0, 2, 3),
            (0, 3, 0, 2, 0), (0, 3, 0, 2, 1), (1, 3, 0, 2, 5), (1, 3, 0, 2, 4), (0, 3, 0, 1, 4), (0, 3, 0, 1, 5),
            (0, 2, 4, 2), (1, 3, 1, 1, 0), (1, 3, 1, 1, 1), (0, 2, 5, 1), (0, 3, 0, 2, 2), (0, 3, 0, 2, 3),
            (1, 3, 1, 1, 2), (1, 3, 1, 1, 3), (1, 2, 7, 3), (1, 3, 1, 2, 0), (1, 3, 1, 2, 1), (0, 3, 0, 2, 4),
            (0, 3, 0, 2, 5), (0, 3, 0, 3, 2), (0, 3, 0, 3, 3), (0, 3, 0, 3, 4), (0, 3, 0, 3, 5), (0, 3, 1, 0, 2),
            (0, 3, 1, 0, 3), (0, 3, 1, 0, 4), (0, 3, 1, 0, 5), (1, 3, 1, 2, 2), (1, 3, 1, 2, 3), (0, 3, 1, 1, 0),
            (0, 3, 1, 1, 1), (1, 3, 1, 1, 5), (1, 3, 1, 1, 4), (0, 3, 1, 1, 2), (0, 3, 1, 1, 3), (1, 3, 2, 3, 5),
            (1, 3, 2, 3, 4), (0, 3, 1, 2, 0), (0, 3, 1, 2, 1), (1, 3, 1, 2, 5), (1, 3, 1, 2, 4), (0, 2, 7, 1),
            (0, 2, 5, 3), (1, 3, 2, 1, 0), (1, 3, 2, 1, 1), (1, 2, 5, 1), (0, 3, 1, 1, 4), (0, 3, 1, 1, 5),
            (0, 3, 1, 2, 2), (0, 3, 1, 2, 3), (1, 3, 2, 1, 2), (1, 3, 2, 1, 3), (1, 3, 2, 2, 0), (1, 3, 2, 2, 1),
            (0, 3, 1, 2, 4), (0, 3, 1, 2, 5), (0, 3, 1, 3, 2), (0, 3, 1, 3, 3), (0, 3, 1, 3, 4), (0, 3, 1, 3, 5),
        ),
        (
            (1, 3, 2, 2, 2), (1, 3, 2, 2, 3), (1, 2, 7, 1), (0, 3, 2, 1, 0), (0, 3, 2, 1, 1), (1, 3, 2, 1, 5),
            (1, 3, 2, 1, 4),
        ),
        (
            (1, 3, 3, 1, 0), (1, 3, 3, 1, 1), (0, 3, 2, 2, 0), (0, 3, 2, 2, 1), (0, 2, 7, 3),
        ),
        (
            (1, 3, 2, 2, 5), (1, 3, 2, 2, 4), (1, 2, 5, 2), (1, 3, 3, 1, 2), (1, 3, 3, 1, 3), (0, 2, 5, 2),
            (1, 3, 3, 3, 0), (1, 3, 3, 3, 1),
        ),
        (
            (0, 3, 3, 1, 0), (0, 3, 3, 1, 1), (1, 2, 7, 2), (1, 3, 3, 1, 5), (1, 3, 3, 1, 4), (0, 2, 7, 2),
            (1, 3, 3, 3, 2), (1, 3, 3, 3, 3), (0, 3, 2, 0, 2), (0, 3, 2, 0, 3), (0, 3, 2, 0, 4), (0, 3, 2, 0, 5),
            (0, 3, 2, 1, 2), (0, 3, 2, 1, 3), (0, 3, 2, 1, 4), (0, 3, 2, 1, 5), (0, 3, 2, 2, 2), (0, 3, 2, 2, 3),
            (0, 3, 2, 2, 4), (0, 3, 2, 2, 5), (0, 3, 2, 3, 2), (0, 3, 2, 3, 3), (0, 3, 2, 3, 4), (0, 3, 2, 3, 5),
        ),
        (
        ),
        (
            (1, 2, 6, 3),
        ),
        (
            (0, 3, 3, 3, 0), (0, 3, 3, 3, 1), (1, 3, 3, 3, 5), (1, 3, 3, 3, 4),
        ),
        (
            (0, 5, 0, 0), (1, 3, 3, 2, 0), (1, 3, 3, 2, 1), (1, 4, 0, 0, 0, 3), (0, 5, 0, 1), (1, 3, 3, 2, 2),
            (1, 3, 3, 2, 3), (0, 5, 0, 2), (1, 4, 0, 0, 0, 2), (1, 3, 5, 1, 0), (1, 3, 5, 1, 1), (0, 5, 0, 3),
            (0, 3, 3, 2, 0), (0, 3, 3, 2, 1), (1, 3, 3, 2, 5), (1, 3, 3, 2, 4), (1, 4, 0, 0, 0, 1), (0, 2, 6, 3),
            (1, 3, 4, 3, 0), (1, 3, 4, 3, 1), (1, 4, 0, 3, 0, 3), (0, 3, 5, 1, 0), (0, 3, 5, 1, 1), (1, 3, 4, 3, 2),
            (1, 3, 4, 3, 3), (0, 2, 6, 1), (1, 4, 0, 3, 0, 2), (1, 3, 4, 1, 0), (1, 3, 4, 1, 1), (0, 3, 4, 3, 0),
            (0, 3, 4, 3, 1), (1, 3, 4, 3, 5), (1, 3, 4, 3, 4), (1, 4, 0, 3, 0, 1), (1, 3, 4, 1, 2), (1, 3, 4, 1, 3),
            (1, 4, 0, 1, 0, 3), (0, 2, 6, 2), (0, 3, 4, 1, 0), (0, 3, 4, 1, 1), (1, 3, 4, 1, 5), (1, 3, 4, 1, 4),
            (1, 4, 0, 1, 0, 2), (1, 3, 4, 2, 0), (1, 3, 4, 2, 1), (1, 3, 4, 2, 2), (1, 3, 4, 2, 3),
            (1, 4, 0, 1, 0, 1), (1, 3, 5, 1, 5), (1, 3, 5, 1, 4), (1, 4, 0, 2, 0, 3), (0, 4, 0, 0, 1, 0),
        ),
        (
            (1, 1, 1, 0, 0, 0), (0, 3, 4, 2, 0), (0, 3, 4, 2, 1), (1, 3, 4, 2, 5), (1, 3, 4, 2, 4),
            (1, 0, 1, 0, 0, 0), (1, 3, 5, 1, 2), (1, 3, 5, 1, 3), (0, 0, 1, 0, 1, 1), (1, 1, 1, 0, 1, 1),
            (1, 3, 5, 3, 0), (1, 3, 5, 3, 1), (1, 4, 0, 2, 0, 2), (1, 3, 5, 3, 2), (1, 3, 5, 3, 3),
            (1, 4, 0, 2, 0, 1), (1, 3, 5, 2, 0), (1, 3, 5, 2, 1), (0, 0, 1, 0, 1, 2), (1, 1, 1, 0, 1, 2),
            (1, 2, 6, 1), (0, 3, 5, 3, 0), (0, 3, 5, 3, 1), (1, 3, 5, 3, 5), (1, 3, 5, 3, 4), (1, 3, 5, 2, 2),
            (1, 3, 5, 2, 3), (0, 4, 0, 1, 1, 0),
        ),
        (
            (1, 1, 1, 1, 0, 0), (1, 0, 1, 1, 0, 0), (0, 3, 5, 2, 0), (0, 3, 5, 2, 1), (1, 3, 5, 2, 5),
            (1, 3, 5, 2, 4), (0, 0, 1, 1, 1, 1), (1, 1, 1, 1, 1, 1), (1, 2, 6, 2), (0, 4, 0, 2, 1, 0),
        ),
        (
            (0, 4, 0, 3, 1, 0),
        ),
        (
            (1, 1, 1, 2, 0, 0), (0, 1, 1, 0, 0, 0), (0, 1, 1, 0, 1, 1), (0, 1, 1, 0, 1, 2), (1, 1, 1, 3, 0, 0),
            (1, 0, 1, 3, 0, 0), (0, 0, 1, 0, 1, 3), (1, 1, 1, 0, 1, 3), (1, 0, 1, 2, 0, 0), (0, 1, 1, 0, 1, 3),
            (0, 3, 3, 0, 2), (0, 3, 3, 0, 3), (0, 3, 3, 0, 4), (0, 3, 3, 0, 5), (0, 3, 3, 1, 2), (0, 3, 3, 1, 3),
            (0, 3, 3, 1, 4), (0, 3, 3, 1, 5), (0, 3, 3, 2, 2), (0, 3, 3, 2, 3), (0, 3, 3, 2, 4), (0, 3, 3, 2, 5),
            (0, 3, 3, 3, 2), (0, 3, 3, 3, 3), (0, 3, 3, 3, 4), (0, 3, 3, 3, 5), (0, 3, 4, 0, 2), (0, 3, 4, 0, 3),
            (0, 3, 4, 0, 4), (0, 3, 4, 0, 5), (0, 3, 4, 1, 2), (0, 3, 4, 1, 3), (0, 3, 4, 1, 4), (0, 3, 4, 1, 5),
            (0, 3, 4, 2, 2), (0, 3, 4, 2, 3), (0, 3, 4, 2, 4), (0, 3, 4, 2, 5), (0, 3, 4, 3, 2), (0, 3, 4, 3, 3),
            (0, 3, 4, 3, 4), (0, 3, 4, 3, 5),
        ),
        (
            (0, 0, 1, 1, 1, 2), (1, 1, 1, 1, 1, 2), (0, 3, 5, 0, 2), (0, 3, 5, 0, 3), (0, 3, 5, 0, 4),
            (0, 3, 5, 0, 5), (0, 3, 5, 1, 2), (0, 3, 5, 1, 3), (0, 3, 5, 1, 4), (0, 3, 5, 1, 5), (0, 3, 5, 2, 2),
            (0, 3, 5, 2, 3), (0, 3, 5, 2, 4), (0, 3, 5, 2, 5), (0, 3, 5, 3, 2), (0, 3, 5, 3, 3), (0, 3, 5, 3, 4),
            (0, 3, 5, 3, 5),
        ),
        (
            (0, 1, 1, 1, 0, 0), (0, 1, 1, 1, 1, 1), (0, 1, 1, 1, 1, 2), (0, 0, 1, 2, 1, 1), (1, 1, 1, 2, 1, 1),
            (0, 5, 1, 0), (1, 4, 1, 0, 0, 3), (0, 0, 1, 3, 1, 1), (1, 1, 1, 3, 1, 1), (1, 4, 1, 0, 0, 2),
            (0, 0, 1, 1, 1, 3), (1, 1, 1, 1, 1, 3), (1, 4, 1, 0, 0, 1), (0, 1, 1, 1, 1, 3),
        ),
        (
            (0, 0, 1, 3, 1, 2), (1, 1, 1, 3, 1, 2),
        ),
        (
            (0, 1, 1, 2, 0, 0), (0, 1, 1, 2, 1, 1), (0, 0, 1, 2, 1, 2), (1, 1, 1, 2, 1, 2), (0, 5, 1, 1),
            (1, 4, 1, 1, 0, 3), (0, 0, 1, 3, 1, 3), (1, 1, 1, 3, 1, 3), (0, 1, 1, 2, 1, 2), (1, 4, 1, 1, 0, 2),
            (0, 0, 1, 2, 1, 3), (1, 1, 1, 2, 1, 3), (0, 1, 1, 2, 1, 3),
        ),
        (
            (1, 4, 1, 1, 0, 1),
        ),
        (
            (0, 1, 1, 3, 0, 0), (0, 1, 1, 3, 1, 1), (0, 1, 1, 3, 1, 2), (0, 1, 1, 3, 1, 3),
        ),
        (
        ),
        (
            (0, 5, 1, 2), (1, 4, 1, 2, 0, 3), (0, 5, 1, 3), (1, 4, 1, 3, 0, 3), (0, 4, 1, 0, 1, 0),
        ),
        (
            (1, 4, 1, 2, 0, 2), (1, 4, 1, 3, 0, 2), (0, 4, 1, 1, 1, 0),
        ),
        (
            (1, 4, 1, 2, 0, 1), (1, 4, 1, 3, 0, 1), (0, 4, 1, 2, 1, 0),
        ),
        (
            (0, 4, 1, 3, 1, 0),
        ),
        (
        ),
    ),
    (
        (
            (1, 0, 0, 0, 0, 0), (1, 0, 0, 0, 1, 0), (1, 1, 0, 0, 0, 0), (1, 3, 0, 1, 0), (1, 3, 0, 1, 1),
            (1, 1, 0, 1, 0, 0), (0, 1, 0, 0, 0, 0), (1, 3, 0, 1, 2), (1, 3, 0, 1, 3), (1, 0, 0, 1, 0, 0),
            (1, 0, 0, 1, 1, 0), (1, 3, 1, 1, 0), (1, 3, 1, 1, 1), (0, 3, 0, 1, 0), (0, 3, 0, 1, 1), (1, 3, 0, 1, 5),
            (1, 3, 0, 1, 4), (0, 0, 0, 0, 0, 1), (0, 0, 0, 0, 1, 1), (1, 1, 0, 0, 0, 1), (1, 3, 1, 1, 2),
            (1, 3, 1, 1, 3), (1, 1, 0, 0, 1, 1), (0, 3, 1, 1, 0), (0, 3, 1, 1, 1), (1, 0, 0, 0, 0, 1),
            (1, 0, 0, 0, 1, 1), (1, 3, 1, 1, 5), (1, 3, 1, 1, 4), (0, 1, 0, 0, 0, 1), (1, 3, 2, 1, 0),
            (1, 3, 2, 1, 1), (0, 1, 0, 0, 1, 1), (1, 3, 2, 1, 2), (1, 3, 2, 1, 3), (0, 0, 0, 1, 0, 1),
            (0, 0, 0, 1, 1, 1), (1, 1, 0, 1, 0, 1), (1, 3, 3, 1, 0), (1, 3, 3, 1, 1), (1, 1, 0, 1, 1, 1),
            (1, 3, 3, 1, 2), (1, 3, 3, 1, 3), (0, 3, 2, 1, 0), (0, 3, 2, 1, 1), (1, 0, 0, 1, 0, 1),
            (1, 0, 0, 1, 1, 1), (1, 3, 2, 1, 5), (1, 3, 2, 1, 4), (1, 3, 4, 1, 0), (1, 3, 4, 1, 1), (0, 3, 3, 1, 0),
            (0, 3, 3, 1, 1), (1, 3, 3, 1, 5), (1, 3, 3, 1, 4), (0, 0, 0, 0, 1, 2), (1, 1, 0, 0, 1, 2),
            (1, 0, 0, 0, 1, 2), (1, 3, 4, 1, 2), (1, 3, 4, 1, 3), (0, 1, 0, 0, 1, 2), (0, 1, 0, 1, 0, 0),
            (0, 1, 0, 1, 0, 1), (0, 1, 0, 1, 1, 1), (0, 3, 4, 1, 0), (0, 3, 4, 1, 1), (1, 3, 4, 1, 5),
            (1, 3, 4, 1, 4), (1, 2, 2, 2), (1, 3, 5, 1, 0), (1, 3, 5, 1, 1), (1, 3, 5, 1, 2), (1, 3, 5, 1, 3),
            (0, 0, 0, 1, 1, 2), (0, 2, 0, 0), (1, 1, 0, 1, 1, 2), (1, 2, 2, 3), (1, 0, 0, 1, 1, 2), (0, 3, 5, 1, 0),
            (0, 3, 5, 1, 1), (1, 3, 5, 1, 5), (1, 3, 5, 1, 4), (0, 1, 0, 1, 1, 2), (1, 2, 0, 2), (1, 2, 0, 3),
            (0, 2, 0, 3), (0, 2, 0, 2), (1, 2, 1, 2), (1, 2, 2, 0), (1, 2, 3, 2), (1, 2, 0, 0), (1, 2, 4, 2),
            (1, 2, 1, 0), (0, 2, 1, 0), (0, 2, 2, 0), (0, 2, 1, 2), (0, 2, 2, 2), (1, 3, 0, 0, 0), (1, 3, 0, 0, 1),
            (1, 2, 3, 0), (1, 2, 1, 3), (0, 2, 3, 0), (0, 2, 3, 2), (1, 3, 0, 0, 2), (1, 3, 0, 0, 3), (1, 2, 3, 3),
            (1, 2, 4, 0), (0, 2, 4, 0), (0, 2, 4, 2), (1, 3, 0, 2, 0), (1, 3, 0, 2, 1), (0, 3, 0, 0, 0),
            (0, 3, 0, 0, 1), (1, 3, 0, 0, 5), (1, 3, 0, 0, 4), (0, 3, 0, 0, 2), (0, 3, 0, 0, 3), (1, 2, 4, 3),
            (1, 2, 5, 0), (0, 2, 1, 3), (0, 2, 2, 3), (1, 3, 0, 2, 2), (1, 3, 0, 2, 3), (0, 3, 0, 2, 0),
            (0, 3, 0, 2, 1), (1, 3, 0, 2, 5), (1, 3, 0, 2, 4), (0, 3, 0, 0, 4), (0, 3, 0, 0, 5), (0, 3, 0, 1, 2),
            (0, 3, 0, 1, 3), (0, 3, 0, 1, 4), (0, 3, 0, 1, 5), (1, 2, 5, 2), (0, 2, 3, 3), (1, 3, 0, 3, 0),
            (1, 3, 0, 3, 1), (0, 3, 0, 2, 2), (0, 3, 0, 2, 3), (1, 2, 7, 0), (1, 3, 0, 3, 2), (1, 3, 0, 3, 3),
            (0, 3, 0, 2, 4), (0, 3, 0, 2, 5), (0, 2, 4, 3), (1, 3, 1, 0, 0), (1, 3, 1, 0, 1), (0, 3, 0, 3, 0),
            (0, 3, 0, 3, 1), (1, 3, 0, 3, 5), (1, 3, 0, 3, 4), (1, 2, 7, 2), (0, 3, 0, 3, 2), (0, 3, 0, 3, 3),
            (1, 3, 1, 0, 2), (1, 3, 1, 0, 3), (0, 3, 1, 0, 0), (0, 3, 1, 0, 1), (0, 2, 5, 2), (1, 3, 1, 0, 5),
            (1, 3, 1, 0, 4), (1, 3, 1, 2, 0), (1, 3, 1, 2, 1), (0, 3, 0, 3, 4), (0, 3, 0, 3, 5), (1, 3, 1, 2, 2),
            (1, 3, 1, 2, 3), (0, 3, 1, 0, 2), (0, 3, 1, 0, 3), (1, 3, 1, 3, 0), (1, 3, 1, 3, 1), (1, 2, 5, 3),
            (0, 3, 1, 0, 4), (0, 3, 1, 0, 5), (0, 3, 1, 1, 2), (0, 3, 1, 1, 3), (0, 3, 1, 1, 4), (0, 3, 1, 1, 5),
            (1, 3, 1, 3, 2), (1, 3, 1, 3, 3), (0, 3, 1, 2, 0), (0, 3, 1, 2, 1), (1, 3, 1, 2, 5), (1, 3, 1, 2, 4),
            (0, 3, 1, 2, 2), (0, 3, 1, 2, 3), (0, 2, 7, 2), (1, 3, 2, 0, 0), (1, 3, 2, 0, 1), (1, 2, 7, 3),
            (0, 3, 1, 3, 0), (0, 3, 1, 3, 1), (1, 3, 1, 3, 5), (1, 3, 1, 3, 4), (1, 3, 2, 0, 2), (1, 3, 2, 0, 3),
            (0, 3, 1, 2, 4), (0, 3, 1, 2, 5), (0, 3, 1, 3, 2), (0, 3, 1, 3, 3), (0, 2, 5, 0), (1, 3, 2, 2, 0),
            (1, 3, 2, 2, 1), (0, 3, 2, 0, 0), (0, 3, 2, 0, 1), (1, 3, 2, 0, 5), (1, 3, 2, 0, 4), (0, 3, 1, 3, 4),
            (0, 3, 1, 3, 5),
        ),
        (
            (1, 3, 2, 2, 2), (1, 3, 2, 2, 3), (0, 2, 7, 0), (1, 3, 2, 3, 0), (1, 3, 2, 3, 1),
        ),
        (
            (0, 3, 2, 2, 0), (0, 3, 2, 2, 1), (1, 3, 2, 2, 5), (1, 3, 2, 2, 4), (1, 3, 2, 3, 2), (1, 3, 2, 3, 3),
        ),
        (
            (1, 3, 3, 2, 0), (1, 3, 3, 2, 1), (0, 3, 2, 3, 0), (0, 3, 2, 3, 1), (0, 2, 5, 3), (1, 3, 2, 3, 5),
            (1, 3, 2, 3, 4),
        ),
        (
            (1, 3, 3, 2, 2), (1, 3, 3, 2, 3), (1, 3, 3, 0, 0), (1, 3, 3, 0, 1), (0, 2, 7, 3), (0, 3, 3, 2, 0),
            (0, 3, 3, 2, 1), (0, 3, 2, 0, 2), (0, 3, 2, 0, 3), (0, 3, 2, 0, 4), (0, 3, 2, 0, 5), (0, 3, 2, 1, 2),
            (0, 3, 2, 1, 3), (0, 3, 2, 1, 4), (0, 3, 2, 1, 5), (0, 3, 2, 2, 2), (0, 3, 2, 2, 3), (0, 3, 2, 2, 4),
            (0, 3, 2, 2, 5), (0, 3, 2, 3, 2), (0, 3, 2, 3, 3), (1, 2, 6, 2), (1, 2, 6, 0), (0, 3, 2, 3, 4),
            (0, 3, 2, 3, 5),
        ),
        (
            (1, 3, 3, 2, 5), (1, 3, 3, 2, 4),
        ),
        (
        ),
        (
        ),
        (
            (1, 3, 3, 0, 2), (1, 3, 3, 0, 3), (1, 2, 6, 3), (0, 5, 0, 0), (0, 4, 0, 0, 0, 2), (0, 3, 3, 0, 0),
            (0, 3, 3, 0, 1), (1, 3, 3, 0, 5), (1, 3, 3, 0, 4), (0, 5, 0, 1), (0, 4, 0, 0, 0, 1), (1, 3, 3, 3, 0),
            (1, 3, 3, 3, 1), (0, 5, 0, 2), (0, 2, 6, 2), (1, 4, 0, 0, 0, 2), (1, 3, 3, 3, 2), (1, 3, 3, 3, 3),
            (0, 5, 0, 3), (0, 4, 0, 0, 0, 0), (1, 3, 4, 2, 0), (1, 3, 4, 2, 1), (1, 4, 0, 0, 0, 1),
            (0, 4, 0, 3, 0, 2), (0, 3, 3, 3, 0), (0, 3, 3, 3, 1), (1, 3, 3, 3, 5), (1, 3, 3, 3, 4),
            (1, 4, 0, 3, 0, 2), (0, 4, 0, 3, 0, 1), (1, 3, 4, 2, 2), (1, 3, 4, 2, 3), (0, 4, 0, 0, 1, 1),
            (1, 4, 0, 0, 1, 1), (1, 4, 0, 3, 0, 1), (0, 3, 4, 2, 0), (0, 3, 4, 2, 1), (1, 3, 4, 2, 5),
            (1, 3, 4, 2, 4), (0, 4, 0, 0, 1, 0),
        ),
        (
            (1, 0, 1, 0, 1, 0), (1, 1, 1, 0, 0, 0), (1, 3, 5, 2, 0), (1, 3, 5, 2, 1), (1, 0, 1, 0, 0, 0),
            (0, 4, 0, 1, 0, 2), (0, 4, 0, 3, 1, 1), (1, 4, 0, 3, 1, 1), (1, 3, 5, 2, 2), (1, 3, 5, 2, 3),
            (1, 4, 0, 1, 0, 2), (0, 4, 0, 1, 0, 1), (1, 3, 5, 0, 0), (1, 3, 5, 0, 1), (1, 4, 0, 1, 0, 1),
            (0, 3, 5, 2, 0), (0, 3, 5, 2, 1), (1, 3, 5, 2, 5), (1, 3, 5, 2, 4), (0, 4, 0, 1, 0, 0),
            (0, 0, 1, 0, 1, 1), (1, 0, 1, 0, 1, 1), (1, 1, 1, 0, 1, 1), (1, 3, 5, 0, 2), (1, 3, 5, 0, 3),
            (0, 4, 0, 2, 0, 2), (0, 4, 0, 1, 1, 1), (1, 4, 0, 2, 0, 2), (1, 4, 0, 1, 1, 1), (0, 3, 5, 0, 0),
            (0, 3, 5, 0, 1), (1, 3, 5, 0, 5), (1, 3, 5, 0, 4), (0, 0, 1, 0, 0, 1), (1, 1, 1, 0, 0, 1),
            (1, 3, 5, 3, 0), (1, 3, 5, 3, 1), (0, 4, 0, 1, 1, 0),
        ),
        (
            (1, 0, 1, 0, 0, 1), (1, 0, 1, 1, 1, 0), (1, 1, 1, 1, 0, 0), (1, 3, 5, 3, 2), (1, 3, 5, 3, 3),
            (0, 4, 0, 2, 0, 1), (1, 0, 1, 1, 0, 0), (0, 4, 0, 2, 1, 1), (1, 4, 0, 2, 1, 1), (0, 4, 0, 2, 0, 0),
            (1, 4, 0, 2, 0, 1), (0, 3, 5, 3, 0), (0, 3, 5, 3, 1), (1, 3, 5, 3, 5), (1, 3, 5, 3, 4),
            (0, 0, 1, 0, 1, 2), (1, 1, 1, 0, 1, 2), (1, 0, 1, 0, 1, 2), (0, 2, 6, 0), (1, 3, 4, 0, 0),
            (1, 3, 4, 0, 1), (0, 0, 1, 1, 1, 1), (1, 1, 1, 1, 1, 1), (1, 0, 1, 1, 1, 1), (1, 3, 4, 0, 2),
            (1, 3, 4, 0, 3), (0, 0, 1, 1, 0, 1), (1, 0, 1, 1, 0, 1), (1, 1, 1, 1, 0, 1), (0, 4, 0, 2, 1, 0),
        ),
        (
            (0, 4, 0, 3, 0, 0), (0, 4, 0, 3, 1, 0),
        ),
        (
            (1, 0, 1, 2, 1, 0), (1, 1, 1, 2, 0, 0), (0, 1, 1, 0, 0, 0), (0, 1, 1, 0, 0, 1), (0, 1, 1, 0, 1, 1),
            (0, 1, 1, 0, 1, 2), (0, 3, 3, 0, 2), (0, 3, 3, 0, 3), (0, 3, 3, 0, 4), (0, 3, 3, 0, 5), (0, 3, 3, 1, 2),
            (0, 3, 3, 1, 3), (0, 3, 3, 1, 4), (0, 3, 3, 1, 5), (0, 3, 3, 2, 2), (0, 3, 3, 2, 3), (0, 3, 3, 2, 4),
            (0, 3, 3, 2, 5), (0, 3, 3, 3, 2), (0, 3, 3, 3, 3), (0, 3, 3, 3, 4), (0, 3, 3, 3, 5), (1, 1, 1, 3, 0, 0),
            (1, 0, 1, 3, 0, 0), (1, 0, 1, 3, 1, 0), (0, 3, 4, 0, 0), (0, 3, 4, 0, 1), (1, 3, 4, 0, 5),
            (1, 3, 4, 0, 4), (0, 3, 4, 0, 2), (0, 3, 4, 0, 3), (1, 0, 1, 2, 0, 0), (0, 2, 6, 3), (1, 3, 4, 3, 0),
            (1, 3, 4, 3, 1), (0, 0, 1, 1, 1, 2), (1, 0, 1, 1, 1, 2), (1, 1, 1, 1, 1, 2), (0, 0, 1, 3, 0, 1),
            (1, 1, 1, 3, 0, 1), (1, 3, 4, 3, 2), (1, 3, 4, 3, 3), (1, 0, 1, 3, 0, 1), (0, 3, 4, 0, 4),
            (0, 3, 4, 0, 5), (0, 3, 4, 1, 2), (0, 3, 4, 1, 3), (0, 3, 4, 1, 4), (0, 3, 4, 1, 5), (0, 3, 4, 2, 2),
            (0, 3, 4, 2, 3), (0, 3, 4, 2, 4), (0, 3, 4, 2, 5), (0, 0, 1, 3, 1, 1), (1, 0, 1, 3, 1, 1),
            (1, 1, 1, 3, 1, 1), (0, 0, 1, 2, 0, 1), (1, 1, 1, 2, 0, 1), (1, 0, 1, 2, 0, 1), (0, 3, 4, 3, 0),
            (0, 3, 4, 3, 1), (1, 3, 4, 3, 5), (1, 3, 4, 3, 4), (0, 0, 1, 2, 1, 1), (1, 0, 1, 2, 1, 1),
            (1, 1, 1, 2, 1, 1), (0, 3, 4, 3, 2), (0, 3, 4, 3, 3), (0, 0, 1, 3, 1, 2), (1, 0, 1, 3, 1, 2),
            (1, 1, 1, 3, 1, 2), (0, 0, 1, 2, 1, 2), (1, 0, 1, 2, 1, 2), (1, 1, 1, 2, 1, 2), (0, 3, 4, 3, 4),
            (0, 3, 4, 3, 5),
        ),
        (
            (0, 3, 5, 0, 2), (0, 3, 5, 0, 3), (0, 3, 5, 0, 4), (0, 3, 5, 0, 5), (0, 3, 5, 1, 2), (0, 3, 5, 1, 3),
            (0, 3, 5, 1, 4), (0, 3, 5, 1, 5), (0, 3, 5, 2, 2), (0, 3, 5, 2, 3), (0, 3, 5, 2, 4), (0, 3, 5, 2, 5),
            (0, 3, 5, 3, 2), (0, 3, 5, 3, 3), (0, 3, 5, 3, 4), (0, 3, 5, 3, 5),
        ),
        (
            (0, 1, 1, 1, 0, 0), (0, 1, 1, 1, 0, 1), (0, 1, 1, 1, 1, 1), (0, 1, 1, 1, 1, 2),
        ),
        (
        ),
        (
            (0, 1, 1, 2, 0, 0), (0, 1, 1, 2, 0, 1), (0, 1, 1, 2, 1, 1), (0, 1, 1, 2, 1, 2),
        ),
        (
            (0, 5, 1, 0), (0, 4, 1, 0, 0, 1), (0, 4, 1, 0, 0, 2), (1, 4, 1, 0, 0, 2),
        ),
        (
            (0, 1, 1, 3, 0, 0), (0, 1, 1, 3, 0, 1), (0, 1, 1, 3, 1, 1), (0, 1, 1, 3, 1, 2),
        ),
        (
            (0, 5, 1, 1), (1, 4, 1, 0, 0, 1),
        ),
        (
            (0, 4, 1, 0, 0, 0), (0, 4, 1, 1, 0, 2), (0, 5, 1, 2), (1, 4, 1, 1, 0, 2), (0, 4, 1, 0, 1, 1),
            (1, 4, 1, 0, 1, 1), (0, 4, 1, 1, 0, 1), (0, 5, 1, 3), (1, 4, 1, 1, 0, 1), (0, 4, 1, 0, 1, 0),
        ),
        (
            (0, 4, 1, 1, 0, 0), (0, 4, 1, 1, 1, 1), (1, 4, 1, 1, 1, 1), (0, 4, 1, 1, 1, 0),
        ),
        (
            (0, 4, 1, 2, 0, 2), (1, 4, 1, 2, 0, 2), (0, 4, 1, 3, 0, 2), (1, 4, 1, 3, 0, 2), (0, 4, 1, 2, 0, 1),
            (1, 4, 1, 2, 0, 1), (0, 4, 1, 2, 1, 1), (1, 4, 1, 2, 1, 1), (0, 4, 1, 3, 0, 1), (1, 4, 1, 3, 0, 1),
            (0, 4, 1, 3, 1, 1), (1, 4, 1, 3, 1, 1), (0, 4, 1, 2, 0, 0), (0, 4, 1, 2, 1, 0),
        ),
        (
            (0, 4, 1, 3, 0, 0), (0, 4, 1, 3, 1, 0),
        ),
        (
        ),
    ),
)

def layer_kernel(
    n_fs,
    groups,
    tokens,
    norm_gain,
    wq,
    wk,
    wv,
    wg,
    mixer_gain,
    wo,
    channel_gain,
    wl,
    wr,
    taps_left,
    taps_right,
    wd,
    cos_t,
    sin_t,
    gammas,
    out,
    w1,
    wout,
    wlr,
    wdown,
    nt,
    nm,
    qkvg,
    hid,
    gated,
    part1,
    part2,
    xb1,
    xb2,
    sb1,
    sb2,
    rb1,
    rb2,
    mid,
    acc,
    both,
    fin,
    fin_in,
    s1_send,
    s1_recv,
    self_sem,
    s2_send,
    s2_recv,
    a_send,
    a_recv,
    f_send,
    f_recv,
    x_send,
    x_recv,
    r_send,
    r_recv,
    o_send,
    o_recv,
):
    fs, tp = lax.axis_index("fs"), lax.axis_index("tp")
    planes = n_fs // groups
    z, q = fs // planes, lax.rem(fs, planes)
    other = 1 - tp
    length, width = tokens.shape
    own = length // 2
    part_rows = own // NT_PARTS
    span_c = length // CHUNKS
    few = span_c // 2
    kb = wq.shape[0]
    nb = wo.shape[1]
    cq, cv, cf = wq.shape[1] // groups, wv.shape[1] // groups, wl.shape[1] // groups
    upper = z * 2 >= groups
    place_z = jnp.where(upper, groups - 1 - z, z)

    def real(plane):
        return jnp.where(upper, groups - 1 - plane, plane)

    def flip(side):
        return jnp.where(upper, 1 - side, side)

    def zdev(target):
        return {"fs": target * planes + q, "tp": tp}

    partner = {"fs": fs, "tp": other}

    def lanes(index, size):
        return pl.ds(pl.multiple_of(index * size, 128), size)

    def rows(index, size):
        return pl.ds(pl.multiple_of(index * size, size), size)

    pieces = (
        (lambda c: wq.at[:, lanes(c, cq)], lambda f: w1.at[rows(f, kb), pl.ds(0, cq)]),
        (lambda c: wk.at[:, lanes(c, cq)], lambda f: w1.at[rows(f, kb), pl.ds(cq, cq)]),
        (lambda c: wv.at[:, lanes(c, cv)], lambda f: w1.at[rows(f, kb), pl.ds(2 * cq, cv)]),
        (lambda c: wg.at[:, lanes(c, cv)], lambda f: w1.at[rows(f, kb), pl.ds(2 * cq + cv, cv)]),
        (lambda c: wo.at[rows(c, cv), :], lambda f: wout.at[:, lanes(f, nb)]),
        (lambda c: wl.at[:, lanes(c, cf)], lambda f: wlr.at[rows(f, kb), pl.ds(0, cf)]),
        (lambda c: wr.at[:, lanes(c, cf)], lambda f: wlr.at[rows(f, kb), pl.ds(cf, cf)]),
        (lambda c: wd.at[rows(c, cf), :], lambda f: wdown.at[:, lanes(f, nb)]),
    )
    starts = (0, cq, 2 * cq, 2 * cq + cv, 0, 0, cf, 0)
    widths = (cq, cq, cv, cv, 0, cf, cf, 0)

    def half_of(cls, f, half):
        members = [i for i in range(len(pieces)) if CLASS_OF[i] == cls]
        low = starts[members[0]]
        wide = sum(widths[i] for i in members)
        if members[0] < 4:
            return w1.at[pl.ds(pl.multiple_of(f * kb + half * (kb // 2), kb // 2), kb // 2), pl.ds(low, wide)]
        if members[0] == 4:
            return wout.at[pl.ds(half * (cv // 2), cv // 2), lanes(f, nb)]
        if members[0] < 7:
            return wlr.at[pl.ds(pl.multiple_of(f * kb + half * (kb // 2), kb // 2), kb // 2), pl.ds(low, wide)]
        return wdown.at[pl.ds(half * (cf // 2), cf // 2), lanes(f, nb)]

    barrier = pltpu.get_barrier_semaphore()
    for step in range(1, groups):
        pl.semaphore_signal(barrier, inc=1, device_id=zdev(lax.rem(z + step, groups)), device_id_type=MESH)
    qx = q + 1 - 2 * lax.rem(q, 2)
    qy = q + 2 - 4 * (q // 2)
    diagonal = planes - 1 - q
    to_x = {"fs": z * planes + qx, "tp": tp}
    to_y = {"fs": z * planes + qy, "tp": tp}
    for device in (to_x, to_y):
        pl.semaphore_signal(barrier, inc=1, device_id=device, device_id_type=MESH)
    pl.semaphore_signal(barrier, inc=1, device_id=partner, device_id_type=MESH)

    keeps = []
    for i, (src, dst) in enumerate(pieces):
        keep = pltpu.make_async_copy(src(z), dst(fs), self_sem.at[i])
        keep.start()
        keeps.append(keep)

    my_half = pl.ds(pl.multiple_of(tp * own, own), own)
    nt[pl.ds(pl.multiple_of(z * length + tp * own, own), own), :] = normed_rows(
        tokens[my_half, :].astype(jnp.float32), norm_gain[...]
    )
    pl.semaphore_wait(barrier, groups - 1 + 2 + 1)

    def remote(src, dst, ssem, rsem, device):
        return pltpu.make_async_remote_copy(
            src_ref=src, dst_ref=dst, send_sem=ssem, recv_sem=rsem,
            device_id=device, device_id_type=MESH,
        )

    def block(key, c, seq, core):
        if key:
            first = c * groups * span_c + seq * span_c + core * few
            return nm.at[pl.ds(pl.multiple_of(first, few), few), :]
        first = seq * length + core * own + c * part_rows
        return nt.at[pl.ds(pl.multiple_of(first, part_rows), part_rows), :]

    part, xb, sb, rb = (part1, part2), (xb1, xb2), (sb1, sb2), (rb1, rb2)

    def pair(which, c, g):
        return part[which][c, tp, g].astype(jnp.float32) + xb[which][c, g].astype(jnp.float32)

    def exchange(which, c):
        return remote(part[which].at[c, other], xb[which].at[c], x_send.at[which, c], x_recv.at[which, c], partner)

    def gather_copy(me, key, c, side, d, landing):
        move = 1 - 2 * side
        ref = block(key, c, real(me - move * d), tp)
        at = key + c + key * (NT_PARTS - 1)
        if landing:
            return remote(ref, ref, a_send.at[at, 0, 0], a_recv.at[at, flip(side), d], partner)
        return remote(
            ref, ref, a_send.at[at, flip(side), d], a_recv.at[at, flip(side), d + 1], zdev(real(me + move))
        )

    def core_copy(me, key, c, side, d, landing):
        move = 1 - 2 * side
        ref = block(key, c, real(me - move * d), other if landing else tp)
        at = key + c + key * (NT_PARTS - 1)
        where_side = flip(side) if d else 0
        return remote(ref, ref, f_send.at[at, where_side, d], f_recv.at[at, where_side, d], partner)

    def weight_copy(me, i, plane, landing):
        src, dst = pieces[i]
        far = real(plane)
        if landing:
            return remote(src(z), dst(far * planes + q), s1_send.at[i, far], s1_recv.at[i, far], zdev(far))
        return remote(src(far), dst(fs), s1_send.at[i, far], s1_recv.at[i, z], zdev(far))

    def hop_copy(me, cls, plane, slot, landing):
        origin = ((q, q, q, q, qx, qy), (qx, qy, qx, qy, diagonal, diagonal))[landing][slot]
        source = real(plane)
        ref = half_of(cls, source * planes + origin, (0, 1, 1, 0, 0, 1)[slot])
        device = (to_x, to_y, to_x, to_y, to_y, to_x)[slot]
        return remote(ref, ref, s2_send.at[cls, source, slot], s2_recv.at[cls, source, slot], device)

    def sum_copy(me, which, c, side, d, landing):
        ref = sb[which].at[c, flip(side), d]
        at = d if landing else d - 1
        device = partner if landing else zdev(real(me + 1 - 2 * side))
        return remote(
            ref, rb[which].at[c, flip(side), at], r_send.at[which, c, flip(side), d],
            r_recv.at[which, c, flip(side), at], device,
        )

    makers = (gather_copy, core_copy, weight_copy, hop_copy, sum_copy)

    def act(me, op):
        sends, kind, args = op[0], op[1], op[2:]
        if kind == SWAP:
            exchange(*args).wait_recv()
            return
        if not sends:
            makers[kind](me, *args, True).wait_recv()
            return
        if kind == HOP and args[1] == me and args[2] == 0:
            for i, keep in enumerate(keeps):
                if CLASS_OF[i] == args[0]:
                    keep.wait()
        if kind == SUM:
            which, c, side, d = args
            move = 1 - 2 * side
            value = pair(which, c, real(me + move * d))
            if 0 <= me - move < groups:
                value = value + rb[which][c, flip(side), d].astype(jnp.float32)
            sb[which][c, flip(side), d] = value.astype(jnp.bfloat16)
        makers[kind](me, *args, False).start()

    def perform(stage):
        for me, ops in enumerate(PLAN):
            @pl.when(place_z == me)
            def _():
                for op in ops[stage]:
                    act(me, op)

    pending = []

    def multiply(left, weight, which, c):
        value = jnp.dot(
            left[rows(c, groups * span_c), :], weight[...], preferred_element_type=jnp.float32
        ).astype(jnp.bfloat16)
        for g in range(groups):
            part[which][c, 0, g] = value[g * span_c : g * span_c + few]
            part[which][c, 1, g] = value[g * span_c + few : (g + 1) * span_c]
        copy = exchange(which, c)
        copy.start()
        pending.append(copy)

    def collect(which, c):
        acc[c] = pair(which, c, z)
        for side, has in ((0, z > 0), (1, z < groups - 1)):
            @pl.when(has)
            def _():
                acc[c] = acc[c] + rb[which][c, side, 0].astype(jnp.float32)
        return acc[c]

    def natural(c, core):
        return pl.ds(pl.multiple_of(c * span_c + core * few, few), few)

    head = tp * groups + z
    chunk = groups * length // 2

    def project(at):
        span = rows(at, chunk)
        qkvg[span, :] = jnp.dot(
            nt[span, :], w1[...], preferred_element_type=jnp.float32
        ).astype(jnp.bfloat16)

    def retain(first):
        log_gamma = gammas[pl.ds(head, 1), :]
        distance = (
            lax.broadcasted_iota(jnp.int32, (length, length), 0)
            - lax.broadcasted_iota(jnp.int32, (length, length), 1)
        ).astype(jnp.float32)
        decay = jnp.where(distance >= 0, jnp.exp(log_gamma * jnp.maximum(distance, 0.0)), 0.0)

        @pl.loop(first * groups // 2, (first + 1) * groups // 2)
        def _(at):
            span = rows(at, length)
            held = qkvg[span, :].astype(jnp.float32)

            def turn(x):
                return x * cos_t[...] + pltpu.roll(x, cq // 2, 1) * sin_t[...]

            rq = turn(held[:, :cq])
            rk = turn(held[:, cq : 2 * cq])
            scores = lax.dot_general(
                rq, rk, (((1,), (1,)), ((), ())), precision=highest, preferred_element_type=jnp.float32
            ) * decay
            kept = jnp.dot(
                scores, held[:, 2 * cq : 2 * cq + cv], precision=highest,
                preferred_element_type=jnp.float32,
            )
            kept = kept * lax.rsqrt(jnp.mean(kept * kept, axis=-1, keepdims=True) + 1e-06)
            gain = mixer_gain[:, lanes(z, cv)]
            whole = (kept * gain * silu(held[:, 2 * cq + cv :])).astype(jnp.bfloat16)
            for c in range(CHUNKS):
                hid[rows(at + c * groups, span_c), :] = whole[c * span_c : (c + 1) * span_c]

    def renorm(c):
        middle = (
            tokens[natural(c, tp), :].astype(jnp.float32) + collect(0, c)
        ).astype(jnp.bfloat16).astype(jnp.float32)
        mid[c] = middle
        first = c * groups * span_c + z * span_c + tp * few
        nm[pl.ds(pl.multiple_of(first, few), few), :] = normed_rows(middle, channel_gain[...])

    place = lax.rem(lax.broadcasted_iota(jnp.int32, (groups * span_c, 1), 0), span_c)

    def convolve(c, low, taps):
        x = both[c, :, low : low + cf].astype(jnp.float32)
        count = taps.shape[0]
        weights = taps[:, lanes(z, cf)]
        result = x * weights[count - 1 :, :]
        for back in range(1, count):
            if c:
                before = both[c - 1, :, low : low + cf].astype(jnp.float32)
                before = pltpu.roll(before, back + (groups - 1) * span_c, 0)
            else:
                before = 0.0
            moved = jnp.where(place >= back, pltpu.roll(x, back, 0), before)
            result = result + moved * weights[count - 1 - back : count - back, :]
        return result

    def mix(c):
        both[c] = jnp.dot(
            nm[rows(c, groups * span_c), :], wlr[...], preferred_element_type=jnp.float32
        ).astype(jnp.bfloat16)
        gated[rows(c, groups * span_c), :] = (
            silu(convolve(c, 0, taps_left)) * convolve(c, cf, taps_right)
        ).astype(jnp.bfloat16)

    def finish(c):
        value = (mid[c] + collect(1, c)).astype(jnp.bfloat16)
        fin[c] = value
        copy = remote(fin.at[c], fin_in.at[c], o_send.at[c], o_recv.at[c], partner)
        copy.start()
        pending.append(copy)
        out[natural(c, tp), :] = value

    steps = (
        project,
        retain,
        lambda c: multiply(hid, wout, 0, c),
        renorm,
        mix,
        lambda c: multiply(gated, wdown, 1, c),
        finish,
    )
    perform(0)
    for stage, (name, index) in enumerate(STAGES):
        steps[name](index)
        perform(stage + 1)
    for c in range(CHUNKS):
        remote(fin.at[c], fin_in.at[c], o_send.at[c], o_recv.at[c], partner).wait_recv()
        out[natural(c, other), :] = fin_in[c]
    for copy in pending:
        copy.wait_send()
    for me, ops in enumerate(PLAN):
        @pl.when(place_z == me)
        def _():
            for stage in ops:
                for op in stage:
                    if op[0]:
                        makers[op[1]](me, *op[2:], False).wait_send()


def body(n_fs, *args):
    (tokens, norm_gain, w_query, w_key, w_value, w_gate, mixer_gain, w_out, channel_gain,
     w_left, w_right, taps_left, taps_right, w_down) = args
    groups = w_query.shape[1] // DK
    if (
        groups != 2 * len(PLAN)
        or n_fs % groups
        or n_fs != 4 * groups
        or lax.axis_size("tp") != 2
        or tokens.shape[0] != BLOCK
        or (w_left.shape[1] // groups) % 128
        or w_left.shape[1] % groups
        or w_out.shape[1] % 128
        or w_query.shape[0] % 32
        or tokens.shape[0] % (32 * CHUNKS)
    ):
        return plain_body(*args)
    length, width = tokens.shape
    heads = groups * lax.axis_size("tp")
    cq, cv, cf = w_query.shape[1] // groups, w_value.shape[1] // groups, w_left.shape[1] // groups
    planes = n_fs // groups
    span_c = length // CHUNKS
    few = span_c // 2
    classes = max(CLASS_OF) + 1
    cos_t, sin_t = turning(length, DK)
    vmem = pl.BlockSpec(memory_space=pltpu.VMEM)
    held = pl.BlockSpec(memory_space=pl.ANY)
    bf, f32, dma = jnp.bfloat16, jnp.float32, pltpu.SemaphoreType.DMA
    return pl.pallas_call(
        functools.partial(layer_kernel, n_fs, groups),
        out_shape=jax.ShapeDtypeStruct(tokens.shape, bf),
        in_specs=[vmem] * 2 + [held] * 4 + [vmem, held, vmem] + [held] * 2 + [vmem] * 2 + [held] + [vmem] * 3,
        out_specs=vmem,
        scratch_shapes=[
            pltpu.VMEM((width, 2 * cq + 2 * cv), bf),
            pltpu.VMEM((cv, width), bf),
            pltpu.VMEM((width, 2 * cf), bf),
            pltpu.VMEM((cf, width), bf),
            pltpu.VMEM((groups * length, width), bf),
            pltpu.VMEM((groups * length, width), bf),
            pltpu.VMEM((groups * length, 2 * cq + 2 * cv), bf),
            pltpu.VMEM((groups * length, cv), bf),
            pltpu.VMEM((groups * length, cf), bf),
            pltpu.VMEM((CHUNKS, 2, groups, few, width), bf),
            pltpu.VMEM((CHUNKS, 2, groups, few, width), bf),
            pltpu.VMEM((CHUNKS, groups, few, width), bf),
            pltpu.VMEM((CHUNKS, groups, few, width), bf),
            pltpu.VMEM((CHUNKS, 2, groups, few, width), bf),
            pltpu.VMEM((CHUNKS, 2, groups, few, width), bf),
            pltpu.VMEM((CHUNKS, 2, groups, few, width), bf),
            pltpu.VMEM((CHUNKS, 2, groups, few, width), bf),
            pltpu.VMEM((CHUNKS, few, width), f32),
            pltpu.VMEM((CHUNKS, few, width), f32),
            pltpu.VMEM((CHUNKS, groups * span_c, 2 * cf), bf),
            pltpu.VMEM((CHUNKS, few, width), bf),
            pltpu.VMEM((CHUNKS, few, width), bf),
            dma((8, groups)),
            dma((8, groups)),
            dma((8,)),
            dma((classes, groups, 6)),
            dma((classes, groups, 6)),
            dma((NT_PARTS + CHUNKS, 2, groups)),
            dma((NT_PARTS + CHUNKS, 2, groups)),
            dma((NT_PARTS + CHUNKS, 2, groups)),
            dma((NT_PARTS + CHUNKS, 2, groups)),
            dma((2, CHUNKS)),
            dma((2, CHUNKS)),
            dma((2, CHUNKS, 2, groups)),
            dma((2, CHUNKS, 2, groups)),
            dma((CHUNKS,)),
            dma((CHUNKS,)),
        ],
        compiler_params=pltpu.CompilerParams(
            collective_id=0, has_side_effects=True, vmem_limit_bytes=60 * 1024 * 1024
        ),
    )(
        tokens, norm_gain[None], w_query, w_key, w_value, w_gate, mixer_gain[None], w_out,
        channel_gain[None], w_left, w_right, taps_left, taps_right, w_down,
        cos_t, sin_t, log_gammas(heads),
    )


def solution(mesh):
    placed = (
        P("fs", None),
        P(),
        P("fs", "tp"),
        P("fs", "tp"),
        P("fs", "tp"),
        P("fs", "tp"),
        P("tp"),
        P("tp", "fs"),
        P(),
        P("fs", "tp"),
        P("fs", "tp"),
        P(None, "tp"),
        P(None, "tp"),
        P("tp", "fs"),
    )
    return jax.shard_map(
        functools.partial(body, mesh.shape["fs"]), mesh=mesh, in_specs=placed, out_specs=P("fs", None), check_vma=False)
```

```python
import functools

import jax
import jax.numpy as jnp
import numpy as np
from jax import lax
from jax.experimental import pallas as pl
from jax.experimental.pallas import tpu as pltpu
from jax.sharding import PartitionSpec as P

DK = 128
DV = 256
BLOCK = 128
MESH = pl.DeviceIdType.MESH


highest = lax.Precision.HIGHEST


def scale_rows(rows_in, gain_vec):
    floats = rows_in.astype(jnp.float32)
    factor = lax.rsqrt(jnp.mean(floats * floats, axis=-1, keepdims=True) + 1e-06)
    return (floats * factor * gain_vec).astype(jnp.bfloat16)


def decays(first_head, count):
    head_ids = first_head + jnp.arange(count, dtype=jnp.float32)
    return jnp.log(1.0 - 2.0 ** (-5.0 - head_ids))


def rotate(heads_in, positions):
    width = heads_in.shape[-1]
    half = width // 2
    freqs = 10000.0 ** (-jnp.arange(half, dtype=jnp.float32) / half)
    angles = positions[:, None] * freqs[None, :]
    cosine = jnp.cos(angles)
    sine = jnp.sin(angles)
    first_half = heads_in[..., :half]
    second_half = heads_in[..., half:]
    return jnp.concatenate(
        [first_half * cosine - second_half * sine, first_half * sine + second_half * cosine],
        axis=-1,
    )


def retention(queries, keys_in, values_in, log_gamma):
    head_count, length, key_width = queries.shape
    value_width = values_in.shape[-1]
    blocks = length // BLOCK
    queries = queries.reshape(head_count, blocks, BLOCK, key_width)
    keys_in = keys_in.reshape(head_count, blocks, BLOCK, key_width)
    values_in = values_in.reshape(head_count, blocks, BLOCK, value_width)
    offsets = jnp.arange(BLOCK, dtype=jnp.float32)
    distance = offsets[:, None] - offsets[None, :]
    weights = jnp.where(
        distance >= 0, jnp.exp(log_gamma[:, None, None] * jnp.maximum(distance, 0.0)), 0.0
    )
    scores = jnp.einsum("hbnd,hbmd->hbnm", queries, keys_in, precision=highest) * weights[:, None]
    inner = jnp.einsum("hbnm,hbme->hbne", scores, values_in, precision=highest)
    key_weight = jnp.exp(log_gamma[:, None] * (BLOCK - 1 - offsets)[None, :])
    contrib = jnp.einsum(
        "hbjd,hbje->hbde", keys_in * key_weight[:, None, :, None], values_in, precision=highest
    )
    block_decay = jnp.exp(log_gamma * BLOCK)[:, None, None]

    def advance(state, contrib_block):
        return (state * block_decay + contrib_block, state)

    _, states = lax.scan(
        advance,
        jnp.zeros((head_count, key_width, value_width), jnp.float32),
        jnp.moveaxis(contrib, 1, 0),
    )
    states = jnp.moveaxis(states, 0, 1)
    query_weight = jnp.exp(log_gamma[:, None] * (offsets + 1.0)[None, :])
    carried = (
        jnp.einsum("hbnd,hbde->hbne", queries, states, precision=highest)
        * query_weight[:, None, :, None]
    )
    return (inner + carried).reshape(head_count, length, value_width)


def head_norm(retained):
    return retained * lax.rsqrt(jnp.mean(retained * retained, axis=-1, keepdims=True) + 1e-06)


def causal_taps(values_in, taps):
    length = values_in.shape[-2]
    padded = jnp.pad(values_in.astype(jnp.float32), ((taps.shape[0] - 1, 0), (0, 0)))
    result = padded[0:length] * taps[0]
    for tap_index in range(1, taps.shape[0]):
        result = result + padded[tap_index : tap_index + length] * taps[tap_index]
    return result


def fold_single(source, weight_piece):
    return jnp.dot(source, weight_piece, preferred_element_type=jnp.float32)


def collect_single(source, weight):
    return fold_single(source, lax.all_gather(weight, "fs", axis=0, tiled=True))


def plain_body(
    tokens,
    norm_gain,
    w_query,
    w_key,
    w_value,
    w_gate,
    mixer_gain,
    w_out,
    channel_gain,
    w_left,
    w_right,
    taps_left,
    taps_right,
    w_down,
):
    length = tokens.shape[0]
    normed = scale_rows(tokens, norm_gain)
    queries = collect_single(normed, w_query)
    keys_proj = collect_single(normed, w_key)
    values_proj = collect_single(normed, w_value)
    gates = collect_single(normed, w_gate)
    queries = queries.astype(jnp.bfloat16)
    keys_proj = keys_proj.astype(jnp.bfloat16)
    values_proj = values_proj.astype(jnp.bfloat16)
    gates = gates.astype(jnp.bfloat16)
    heads_here = w_query.shape[1] // DK
    first_head = (lax.axis_index("tp") * heads_here).astype(jnp.float32)
    log_gamma = decays(first_head, heads_here)
    positions = jnp.arange(length, dtype=jnp.float32)

    def split_heads(rows_in, width):
        return rows_in.astype(jnp.float32).reshape(length, heads_here, width).transpose(1, 0, 2)

    retained = head_norm(
        retention(
            rotate(split_heads(queries, DK), positions),
            rotate(split_heads(keys_proj, DK), positions),
            split_heads(values_proj, DV),
            log_gamma,
        )
    )
    retained = retained.transpose(1, 0, 2).reshape(length, heads_here * DV)
    hidden = (retained * mixer_gain * jax.nn.silu(gates.astype(jnp.float32))).astype(jnp.bfloat16)
    rows_own = length // lax.axis_size("tp")
    first_row = lax.axis_index("tp") * rows_own
    out_whole = lax.all_gather(w_out, "fs", axis=1, tiled=True)
    mixer_total = lax.psum_scatter(
        jnp.dot(hidden, out_whole, preferred_element_type=jnp.float32).astype(jnp.bfloat16),
        "tp",
        scatter_dimension=0,
        tiled=True,
    ).astype(jnp.float32)
    residual = lax.dynamic_slice_in_dim(tokens, first_row, rows_own, 0)
    middle_own = (residual.astype(jnp.float32) + mixer_total).astype(jnp.bfloat16)
    middle = lax.all_gather(middle_own, "tp", axis=0, tiled=True)
    normed_mid = scale_rows(middle, channel_gain)
    left = collect_single(normed_mid, w_left)
    right = collect_single(normed_mid, w_right)
    left = left.astype(jnp.bfloat16)
    right = right.astype(jnp.bfloat16)
    gated = (jax.nn.silu(causal_taps(left, taps_left)) * causal_taps(right, taps_right)).astype(
        jnp.bfloat16
    )
    down_whole = lax.all_gather(w_down, "fs", axis=1, tiled=True)
    channel_part = jnp.dot(gated, down_whole, preferred_element_type=jnp.float32)
    channel_total = lax.psum(channel_part.astype(jnp.bfloat16), "tp").astype(jnp.float32)
    return (middle.astype(jnp.float32) + channel_total).astype(jnp.bfloat16)


def log_gammas(head_count):
    table = np.log(1.0 - 2.0 ** (-5.0 - np.arange(head_count, dtype=np.float64)))
    return np.repeat(table[:, None], BLOCK, axis=1).astype(np.float32)


def turning(length, width):
    half = width // 2
    freqs = np.float32(10000.0) ** (-np.arange(half, dtype=np.float32) / np.float32(half))
    angles = (np.arange(length, dtype=np.float32)[:, None] * freqs[None, :]).astype(np.float64)
    cosine, sine = np.cos(angles), np.sin(angles)
    return (
        np.concatenate([cosine, cosine], axis=1).astype(np.float32),
        np.concatenate([-sine, sine], axis=1).astype(np.float32),
    )


def silu(v):
    return v / (1.0 + jnp.exp(-v))


def normed_rows(floats, gain):
    factor = lax.rsqrt(jnp.mean(floats * floats, axis=-1, keepdims=True) + 1e-06)
    return (floats * factor * gain).astype(jnp.bfloat16)


HOP, SUM, SWAP, WEIGHTS, HOPS, CORES = 3, 4, 5, 6, 7, 8
CHUNKS = 4
NT_PARTS = 2
CLASS_OF = (0, 0, 0, 1, 2, 3, 4, 5)
STAGES = (
    (7, 0),
    (0, 0),
    (0, 1),
    (1, 0),
    (1, 1),
    (2, 0),
    (2, 1),
    (2, 2),
    (2, 3),
    (3, 0),
    (3, 1),
    (3, 2),
    (3, 3),
    (4, 0),
    (5, 0),
    (4, 1),
    (5, 1),
    (4, 2),
    (5, 2),
    (4, 3),
    (5, 3),
    (6, 0),
    (6, 1),
    (6, 2),
    (6, 3),
)
PLAN = (
    (
        (
            (1, 3, 1, 0, 0), (1, 3, 1, 0, 3), (1, 3, 1, 0, 2), (1, 3, 1, 0, 1), (1, 3, 0, 0, 0), (1, 3, 0, 0, 1),
        ),
        (
            (1, 2, 2, 3), (1, 3, 0, 0, 3), (1, 0, 0, 0, 0, 0), (1, 3, 4, 0, 0), (1, 3, 4, 0, 1), (0, 3, 0, 0, 0),
            (0, 3, 1, 0, 1), (1, 3, 1, 0, 5), (0, 3, 0, 0, 1), (1, 0, 0, 1, 0, 0), (1, 3, 0, 0, 2), (1, 3, 4, 0, 3),
            (1, 3, 0, 0, 4), (0, 3, 1, 0, 0), (1, 3, 1, 0, 4), (1, 3, 2, 0, 0), (1, 3, 3, 0, 0), (0, 0, 0, 0, 1, 1),
            (1, 3, 2, 0, 1), (1, 1, 0, 0, 0, 0), (1, 3, 2, 0, 3), (1, 3, 3, 0, 1), (1, 3, 4, 0, 2),
            (1, 1, 0, 0, 1, 1), (0, 3, 2, 0, 0), (1, 2, 2, 1), (0, 3, 2, 0, 1), (1, 1, 0, 1, 0, 0), (1, 3, 5, 0, 0),
            (1, 2, 2, 2), (1, 3, 5, 0, 2), (0, 3, 4, 0, 1), (1, 3, 3, 0, 3), (1, 2, 1, 3), (0, 0, 0, 0, 1, 2),
            (0, 3, 3, 0, 1), (1, 3, 2, 0, 4), (1, 2, 3, 3), (1, 1, 0, 0, 1, 2), (0, 3, 3, 0, 0), (0, 3, 4, 0, 0),
            (1, 3, 0, 0, 5), (1, 2, 0, 3), (0, 0, 0, 1, 1, 1), (0, 3, 5, 0, 0), (1, 3, 5, 0, 1), (1, 3, 3, 0, 5),
            (0, 3, 5, 0, 1), (1, 3, 3, 0, 4), (1, 3, 5, 0, 3), (0, 0, 0, 1, 1, 2), (1, 3, 4, 0, 5),
            (1, 1, 0, 1, 1, 1), (1, 3, 5, 0, 5), (1, 2, 3, 1), (1, 3, 5, 0, 4), (1, 3, 4, 0, 4), (0, 6, 1, 3),
            (1, 3, 1, 3, 1), (1, 3, 1, 3, 2), (1, 2, 4, 3), (1, 3, 1, 3, 3), (1, 3, 1, 3, 0), (1, 1, 0, 1, 1, 2),
            (0, 6, 0, 3), (1, 3, 0, 3, 0), (1, 2, 1, 1), (1, 3, 3, 0, 2), (1, 3, 0, 3, 2), (1, 3, 0, 3, 1),
            (0, 0, 0, 0, 1, 3), (0, 3, 1, 3, 0), (0, 3, 1, 3, 1), (1, 3, 1, 3, 5), (1, 3, 0, 3, 3), (1, 3, 1, 3, 4),
            (1, 2, 0, 1), (1, 1, 0, 0, 1, 3), (1, 2, 4, 1), (0, 3, 0, 3, 0), (1, 3, 0, 3, 4), (1, 2, 1, 2),
            (1, 2, 3, 2), (0, 3, 0, 3, 1), (1, 3, 0, 3, 5), (0, 6, 2, 3), (1, 3, 2, 3, 1), (1, 3, 2, 3, 0),
            (0, 0, 0, 1, 1, 3), (1, 1, 0, 1, 1, 3), (1, 3, 2, 3, 2), (1, 3, 2, 0, 2), (1, 3, 2, 3, 3), (0, 6, 1, 1),
            (1, 3, 1, 1, 2), (1, 3, 1, 1, 1), (1, 3, 1, 1, 3), (1, 3, 1, 1, 0), (0, 3, 2, 3, 1), (1, 3, 2, 3, 5),
            (1, 2, 0, 2), (0, 6, 0, 1), (1, 3, 0, 1, 0), (1, 2, 4, 2), (1, 3, 0, 1, 2), (1, 3, 0, 1, 1),
            (1, 3, 0, 1, 3), (0, 3, 1, 1, 1), (0, 3, 1, 1, 0), (1, 3, 1, 1, 4), (1, 3, 1, 1, 5), (0, 6, 2, 1),
            (0, 3, 0, 1, 0), (0, 6, 1, 2), (1, 2, 7, 3), (0, 3, 0, 1, 1), (1, 2, 5, 3), (0, 3, 2, 3, 0),
            (1, 3, 0, 1, 5), (1, 3, 0, 1, 4), (0, 6, 0, 2), (1, 3, 0, 2, 0), (1, 3, 0, 2, 1), (1, 3, 0, 2, 3),
            (1, 3, 0, 2, 2), (1, 2, 5, 1), (1, 3, 1, 2, 0), (1, 3, 1, 2, 1), (0, 6, 2, 2), (0, 6, 5, 1),
            (0, 3, 0, 2, 1), (1, 3, 1, 2, 3), (0, 3, 0, 2, 0), (1, 3, 0, 2, 5), (1, 3, 0, 2, 4), (1, 3, 1, 2, 2),
            (0, 3, 1, 2, 0), (0, 3, 1, 2, 1), (1, 3, 1, 2, 5), (1, 3, 1, 2, 4), (1, 3, 2, 1, 1), (0, 6, 5, 3),
            (1, 3, 2, 1, 0), (1, 3, 2, 0, 5), (1, 3, 2, 3, 4), (1, 3, 2, 2, 1), (1, 3, 2, 2, 0), (1, 2, 7, 1),
            (0, 6, 3, 1), (1, 3, 2, 1, 3), (1, 3, 3, 1, 0), (1, 3, 2, 2, 3), (0, 8, 0, 0), (0, 7, 0), (0, 7, 1),
        ),
        (
            (0, 3, 2, 1, 0), (1, 3, 2, 2, 2), (1, 3, 3, 1, 1), (0, 3, 2, 1, 1), (1, 3, 2, 1, 5),
        ),
        (
            (1, 3, 2, 1, 4), (1, 2, 5, 2),
        ),
        (
            (0, 6, 3, 2), (0, 6, 3, 3), (0, 3, 2, 2, 1), (1, 2, 7, 2), (1, 3, 2, 1, 2), (1, 3, 2, 2, 5),
            (0, 3, 2, 2, 0), (1, 3, 3, 3, 0), (1, 3, 2, 2, 4), (1, 3, 3, 3, 1), (1, 3, 3, 1, 3), (1, 3, 5, 3, 2),
        ),
        (
            (0, 6, 5, 2), (0, 3, 3, 1, 1), (0, 3, 3, 1, 0), (1, 3, 3, 2, 3), (1, 3, 3, 2, 0), (1, 3, 3, 2, 1),
            (1, 3, 3, 1, 4), (1, 3, 5, 2, 2), (1, 3, 3, 1, 5), (1, 2, 6, 3), (0, 7, 2),
        ),
        (
            (1, 3, 3, 3, 3), (0, 3, 3, 3, 0),
        ),
        (
        ),
        (
            (1, 3, 3, 3, 4),
        ),
        (
            (0, 5, 0, 0), (1, 3, 5, 1, 1), (0, 3, 3, 3, 1), (1, 3, 3, 3, 5), (1, 4, 0, 0, 0, 3), (1, 4, 0, 0, 0, 2),
            (0, 3, 3, 2, 1), (1, 3, 5, 1, 0), (0, 5, 0, 3), (1, 3, 5, 1, 3), (0, 3, 3, 2, 0), (1, 4, 0, 0, 0, 1),
            (0, 6, 4, 3), (1, 3, 4, 3, 2), (1, 3, 4, 3, 0), (1, 3, 4, 3, 1), (1, 4, 0, 3, 0, 3), (1, 3, 4, 3, 3),
            (0, 3, 5, 1, 1), (1, 4, 0, 3, 0, 2), (0, 6, 4, 1), (1, 3, 4, 1, 2), (1, 3, 4, 1, 1), (1, 3, 4, 1, 0),
            (1, 4, 0, 3, 0, 1), (0, 3, 4, 3, 0), (0, 6, 4, 2), (1, 3, 4, 2, 2), (1, 3, 4, 2, 1), (1, 3, 4, 2, 3),
            (1, 3, 4, 2, 0), (1, 3, 4, 1, 3), (1, 3, 5, 3, 1), (1, 3, 5, 3, 0), (0, 5, 0, 1), (1, 3, 5, 2, 1),
            (1, 4, 0, 1, 0, 3), (1, 3, 3, 3, 2), (0, 5, 0, 2), (0, 3, 4, 3, 1), (1, 3, 5, 1, 2), (0, 3, 4, 1, 0),
            (1, 3, 4, 1, 4), (1, 4, 0, 1, 0, 2), (0, 3, 4, 1, 1), (1, 4, 0, 1, 0, 1), (1, 3, 4, 3, 5),
            (1, 3, 4, 1, 5), (0, 3, 4, 2, 1), (1, 3, 4, 2, 5), (1, 3, 3, 1, 2), (1, 4, 0, 2, 0, 3), (0, 3, 4, 2, 0),
            (1, 3, 4, 2, 4), (1, 3, 5, 2, 0), (0, 4, 0, 0, 1, 0),
        ),
        (
            (0, 0, 1, 0, 1, 1), (1, 3, 4, 3, 4), (1, 4, 0, 2, 0, 2), (1, 3, 3, 2, 2), (1, 3, 5, 1, 5),
            (1, 3, 3, 2, 5), (1, 4, 0, 2, 0, 1), (1, 3, 3, 2, 4), (1, 1, 1, 0, 1, 1), (1, 0, 1, 0, 0, 0),
            (0, 0, 1, 0, 1, 2), (1, 2, 6, 1), (0, 3, 5, 3, 1), (1, 3, 5, 3, 5), (0, 4, 0, 1, 1, 0), (1, 3, 5, 3, 3),
        ),
        (
            (0, 3, 5, 2, 1), (1, 0, 1, 1, 0, 0), (0, 3, 5, 1, 0), (1, 3, 5, 1, 4), (1, 3, 5, 2, 3), (0, 3, 5, 2, 0),
            (1, 1, 1, 0, 1, 2), (1, 3, 5, 2, 5), (0, 0, 1, 1, 1, 1), (1, 2, 6, 2), (0, 4, 0, 2, 1, 0),
            (1, 1, 1, 0, 0, 0), (0, 4, 0, 3, 1, 0),
        ),
        (
            (1, 1, 1, 1, 0, 0), (1, 1, 1, 1, 1, 1),
        ),
        (
            (0, 0, 1, 1, 1, 2), (1, 0, 1, 2, 0, 0), (1, 1, 1, 2, 0, 0), (1, 3, 5, 2, 4), (0, 3, 5, 3, 0),
            (1, 1, 1, 1, 1, 2), (0, 0, 1, 2, 1, 1), (1, 3, 5, 3, 4), (1, 0, 1, 3, 0, 0), (1, 1, 1, 2, 1, 1),
            (0, 0, 1, 0, 1, 3), (1, 1, 1, 0, 1, 3), (0, 0, 1, 3, 1, 1), (0, 8, 1, 0), (0, 7, 3), (0, 7, 4),
        ),
        (
            (0, 0, 1, 2, 1, 2), (1, 1, 1, 3, 0, 0), (0, 7, 5),
        ),
        (
            (0, 0, 1, 1, 1, 3), (1, 1, 1, 1, 1, 3), (0, 5, 1, 0), (1, 1, 1, 2, 1, 2), (1, 4, 1, 0, 0, 3),
            (0, 0, 1, 3, 1, 2), (0, 8, 1, 1),
        ),
        (
        ),
        (
            (1, 4, 1, 0, 0, 2), (0, 0, 1, 2, 1, 3), (1, 1, 1, 2, 1, 3), (1, 1, 1, 3, 1, 2), (1, 4, 1, 0, 0, 1),
            (1, 1, 1, 3, 1, 1), (0, 5, 1, 1), (0, 8, 1, 2),
        ),
        (
            (0, 0, 1, 3, 1, 3), (1, 4, 1, 1, 0, 3), (1, 1, 1, 3, 1, 3),
        ),
        (
            (1, 4, 1, 1, 0, 2), (0, 8, 1, 3),
        ),
        (
        ),
        (
            (0, 5, 1, 2), (1, 4, 1, 2, 0, 3), (0, 5, 1, 3), (1, 4, 1, 3, 0, 3), (1, 4, 1, 2, 0, 2),
            (0, 4, 1, 0, 1, 0), (1, 4, 1, 3, 0, 2), (1, 4, 1, 1, 0, 1),
        ),
        (
            (1, 4, 1, 2, 0, 1), (0, 4, 1, 1, 1, 0),
        ),
        (
            (1, 4, 1, 3, 0, 1), (0, 4, 1, 2, 1, 0),
        ),
        (
            (0, 4, 1, 3, 1, 0),
        ),
        (
        ),
    ),
    (
        (
            (1, 3, 0, 1, 0), (1, 2, 2, 0), (1, 3, 0, 1, 2), (1, 3, 0, 1, 3), (1, 3, 0, 1, 1), (1, 2, 2, 2),
            (1, 3, 1, 1, 0),
        ),
        (
            (1, 3, 1, 1, 2), (1, 1, 0, 0, 0, 0), (1, 3, 1, 1, 1), (1, 0, 0, 0, 1, 0), (1, 0, 0, 1, 1, 0),
            (1, 0, 0, 0, 0, 0), (0, 3, 0, 1, 0), (1, 3, 0, 1, 4), (0, 3, 0, 1, 1), (1, 3, 2, 1, 0), (1, 3, 0, 1, 5),
            (0, 3, 1, 1, 0), (1, 0, 0, 1, 0, 0), (1, 3, 2, 1, 2), (1, 3, 2, 1, 1), (1, 1, 0, 1, 0, 0),
            (1, 3, 2, 1, 3), (0, 0, 0, 0, 1, 1), (0, 3, 2, 1, 0), (0, 0, 0, 0, 0, 1), (1, 3, 3, 1, 0),
            (1, 0, 0, 0, 1, 1), (1, 3, 3, 1, 1), (1, 3, 5, 1, 0), (1, 3, 4, 1, 0), (1, 3, 4, 1, 2), (1, 3, 3, 1, 3),
            (1, 1, 0, 0, 0, 1), (0, 3, 1, 1, 1), (1, 0, 0, 0, 0, 1), (1, 1, 0, 0, 1, 1), (1, 3, 4, 1, 1),
            (0, 3, 2, 1, 1), (1, 3, 2, 1, 4), (1, 3, 4, 1, 3), (0, 0, 0, 1, 0, 1), (1, 1, 0, 1, 0, 1),
            (0, 3, 3, 1, 1), (0, 0, 0, 1, 1, 1), (1, 0, 0, 1, 1, 1), (0, 3, 4, 1, 1), (1, 3, 5, 1, 1),
            (1, 3, 5, 1, 2), (0, 0, 0, 0, 1, 2), (1, 3, 1, 1, 5), (1, 1, 0, 1, 1, 1), (1, 0, 0, 1, 0, 1),
            (0, 3, 3, 1, 0), (1, 2, 2, 3), (1, 3, 2, 1, 5), (1, 3, 1, 1, 4), (0, 3, 5, 1, 0), (1, 0, 0, 0, 1, 2),
            (1, 3, 4, 1, 5), (1, 3, 1, 1, 3), (0, 3, 5, 1, 1), (1, 3, 3, 1, 5), (1, 3, 3, 1, 2), (0, 3, 4, 1, 0),
            (0, 0, 0, 1, 1, 2), (1, 1, 0, 1, 1, 2), (1, 3, 5, 1, 5), (1, 3, 3, 1, 4), (1, 2, 3, 2), (1, 2, 1, 2),
            (1, 2, 0, 2), (1, 1, 0, 0, 1, 2), (1, 3, 4, 1, 4), (1, 3, 5, 1, 4), (1, 2, 4, 2), (1, 0, 0, 1, 1, 2),
            (1, 2, 1, 0), (1, 2, 3, 0), (0, 6, 1, 0), (1, 3, 1, 0, 1), (1, 2, 1, 3), (1, 3, 1, 0, 0), (0, 6, 0, 0),
            (1, 3, 0, 0, 0), (1, 3, 0, 0, 1), (0, 6, 0, 2), (1, 3, 0, 2, 3), (1, 3, 0, 2, 1), (1, 3, 0, 2, 2),
            (1, 3, 0, 2, 0), (1, 3, 0, 0, 3), (1, 3, 0, 0, 2), (1, 2, 0, 0), (1, 2, 3, 3), (0, 3, 1, 0, 1),
            (1, 2, 4, 0), (0, 3, 0, 0, 0), (0, 3, 0, 0, 1), (0, 3, 1, 0, 0), (1, 3, 0, 0, 5), (1, 2, 0, 3),
            (1, 2, 7, 0), (1, 2, 4, 3), (1, 3, 0, 0, 4), (0, 3, 0, 2, 0), (1, 3, 0, 2, 4), (0, 3, 0, 2, 1),
            (1, 3, 0, 2, 5), (0, 6, 2, 0), (1, 2, 5, 0), (1, 2, 7, 2), (0, 6, 1, 2), (0, 6, 0, 3), (1, 3, 0, 3, 1),
            (1, 2, 5, 2), (1, 3, 0, 3, 0), (1, 3, 0, 3, 2), (0, 6, 1, 3), (1, 3, 0, 3, 3), (0, 6, 2, 3),
            (1, 3, 1, 0, 5), (1, 3, 1, 0, 4), (0, 3, 0, 3, 1), (0, 3, 0, 3, 0), (1, 3, 0, 3, 4), (1, 3, 0, 3, 5),
            (1, 3, 1, 0, 3), (1, 3, 1, 0, 2), (1, 3, 1, 2, 0), (1, 3, 1, 2, 1), (1, 3, 1, 2, 2), (1, 3, 1, 2, 3),
            (1, 3, 1, 3, 0), (1, 2, 5, 3), (1, 3, 1, 3, 1), (1, 3, 1, 3, 3), (0, 6, 5, 2), (1, 3, 1, 3, 2),
            (1, 2, 7, 3), (0, 3, 1, 2, 0), (0, 3, 1, 2, 1), (1, 3, 1, 2, 4), (1, 3, 1, 2, 5), (1, 3, 2, 0, 0),
            (1, 3, 2, 0, 1), (0, 3, 1, 3, 0), (0, 6, 3, 2), (0, 3, 1, 3, 1), (1, 3, 1, 3, 5), (1, 3, 1, 3, 4),
            (1, 3, 2, 0, 3), (0, 6, 2, 2), (1, 3, 2, 2, 1), (1, 3, 2, 2, 2), (1, 3, 2, 2, 0), (1, 3, 5, 1, 3),
            (1, 3, 2, 0, 2), (1, 3, 2, 3, 0), (0, 3, 2, 0, 0), (0, 3, 2, 0, 1), (1, 3, 2, 3, 1), (1, 3, 2, 0, 4),
            (1, 3, 2, 3, 3), (1, 3, 2, 2, 3), (0, 8, 0, 0), (0, 7, 0), (0, 7, 1),
        ),
        (
        ),
        (
            (1, 3, 2, 0, 5), (0, 3, 2, 2, 1), (0, 3, 2, 2, 0), (1, 3, 2, 2, 4), (1, 3, 2, 3, 2), (1, 3, 2, 2, 5),
        ),
        (
            (1, 3, 3, 2, 0), (0, 3, 2, 3, 0), (0, 3, 2, 3, 1), (1, 3, 3, 2, 1),
        ),
        (
            (1, 3, 2, 3, 5), (1, 3, 2, 3, 4), (1, 3, 5, 2, 2), (1, 3, 3, 2, 3), (0, 6, 3, 0), (1, 3, 3, 0, 0),
            (1, 3, 3, 0, 1), (1, 3, 5, 2, 1), (1, 3, 5, 2, 0), (1, 2, 6, 2), (0, 3, 3, 2, 1), (0, 6, 3, 3),
            (1, 2, 6, 0), (0, 7, 2),
        ),
        (
            (1, 3, 3, 3, 1), (1, 3, 3, 3, 0),
        ),
        (
            (0, 3, 3, 2, 0),
        ),
        (
        ),
        (
            (1, 3, 3, 2, 5), (1, 2, 6, 3), (1, 3, 3, 3, 3), (0, 4, 0, 0, 0, 2), (1, 3, 3, 0, 2), (1, 3, 3, 0, 3),
            (0, 3, 3, 3, 1), (1, 3, 3, 3, 2), (1, 3, 5, 2, 3), (0, 5, 0, 0), (0, 5, 0, 3), (0, 3, 3, 0, 0),
            (0, 6, 4, 2), (0, 4, 0, 0, 0, 1), (1, 4, 0, 0, 0, 2), (1, 3, 4, 2, 0), (1, 4, 0, 0, 0, 1),
            (0, 4, 0, 0, 0, 0), (1, 3, 4, 2, 1), (0, 4, 0, 3, 0, 2), (1, 3, 4, 2, 2), (1, 4, 0, 3, 0, 2),
            (0, 3, 3, 3, 0), (0, 4, 0, 0, 1, 1), (1, 4, 0, 0, 1, 1), (0, 3, 5, 2, 1), (0, 4, 0, 3, 0, 1),
            (0, 5, 0, 1), (0, 3, 4, 2, 1), (0, 6, 5, 0), (0, 3, 4, 2, 0), (1, 3, 4, 2, 5), (1, 4, 0, 3, 0, 1),
            (1, 3, 5, 0, 0), (1, 3, 3, 2, 4), (0, 3, 3, 0, 1), (1, 3, 3, 0, 5), (0, 4, 0, 0, 1, 0),
        ),
        (
            (1, 0, 1, 0, 1, 0), (0, 4, 0, 3, 1, 1), (1, 3, 4, 2, 4), (1, 0, 1, 0, 0, 0), (1, 3, 5, 0, 1),
            (0, 4, 0, 1, 0, 2), (1, 4, 0, 1, 0, 2), (1, 3, 3, 2, 2), (0, 4, 0, 3, 0, 0), (1, 3, 5, 2, 5),
            (0, 6, 5, 3), (1, 3, 5, 3, 3), (1, 3, 5, 3, 0), (1, 3, 5, 3, 1), (1, 3, 3, 3, 5), (1, 4, 0, 3, 1, 1),
            (1, 3, 4, 2, 3), (0, 4, 0, 1, 0, 1), (1, 3, 5, 3, 2), (1, 3, 5, 0, 3), (0, 3, 5, 2, 0), (1, 3, 5, 2, 4),
            (1, 1, 1, 0, 0, 0), (1, 3, 3, 0, 4), (1, 4, 0, 1, 0, 1), (0, 0, 1, 0, 1, 1), (0, 5, 0, 2),
            (1, 0, 1, 0, 1, 1), (0, 3, 5, 0, 1), (0, 3, 5, 0, 0), (1, 3, 5, 0, 5), (0, 4, 0, 2, 0, 2),
            (0, 4, 0, 1, 1, 1), (0, 4, 0, 1, 0, 0), (1, 4, 0, 1, 1, 1), (1, 4, 0, 2, 0, 2), (0, 4, 0, 3, 1, 0),
            (1, 1, 1, 0, 1, 1), (0, 4, 0, 2, 0, 1), (0, 4, 0, 1, 1, 0),
        ),
        (
            (1, 0, 1, 1, 0, 0), (0, 3, 5, 3, 0), (1, 0, 1, 1, 1, 0), (0, 4, 0, 2, 0, 0), (1, 4, 0, 2, 0, 1),
            (0, 4, 0, 2, 1, 1), (0, 3, 5, 3, 1), (1, 3, 5, 3, 5), (1, 3, 5, 0, 4), (0, 0, 1, 0, 0, 1),
            (1, 0, 1, 0, 0, 1), (1, 4, 0, 2, 1, 1), (1, 3, 3, 3, 4), (0, 0, 1, 1, 1, 1), (1, 0, 1, 1, 1, 1),
            (0, 6, 4, 0), (1, 3, 4, 0, 1), (1, 3, 5, 0, 2), (1, 3, 4, 0, 0), (0, 4, 0, 2, 1, 0), (1, 1, 1, 0, 0, 1),
            (1, 3, 4, 0, 2),
        ),
        (
            (1, 3, 4, 0, 3),
        ),
        (
            (1, 1, 1, 1, 1, 1), (1, 1, 1, 3, 0, 0), (1, 0, 1, 2, 1, 0), (1, 0, 1, 2, 0, 0), (1, 0, 1, 3, 1, 0),
            (0, 0, 1, 0, 1, 2), (1, 1, 1, 0, 1, 2), (1, 3, 5, 3, 4), (0, 0, 1, 1, 0, 1), (1, 1, 1, 1, 0, 0),
            (1, 0, 1, 1, 0, 1), (1, 0, 1, 0, 1, 2), (0, 3, 4, 0, 1), (1, 3, 4, 0, 5), (1, 0, 1, 3, 0, 0),
            (0, 3, 4, 0, 0), (1, 3, 4, 0, 4), (0, 0, 1, 2, 1, 1), (1, 1, 1, 2, 0, 0), (1, 0, 1, 2, 1, 1),
            (0, 6, 4, 3), (1, 3, 4, 3, 1), (1, 3, 4, 3, 0), (1, 1, 1, 1, 0, 1), (0, 0, 1, 2, 0, 1),
            (1, 1, 1, 2, 1, 1), (0, 0, 1, 1, 1, 2), (1, 0, 1, 2, 0, 1), (1, 3, 4, 3, 2), (1, 3, 4, 3, 3),
            (1, 0, 1, 1, 1, 2), (0, 0, 1, 3, 1, 1), (0, 0, 1, 3, 0, 1), (1, 0, 1, 3, 0, 1), (1, 0, 1, 3, 1, 1),
            (0, 3, 4, 3, 0), (1, 1, 1, 3, 0, 1), (0, 3, 4, 3, 1), (1, 3, 4, 3, 4), (1, 3, 4, 3, 5),
            (0, 0, 1, 2, 1, 2), (1, 1, 1, 1, 1, 2), (1, 0, 1, 2, 1, 2), (0, 0, 1, 3, 1, 2), (1, 0, 1, 3, 1, 2),
            (1, 1, 1, 3, 1, 1), (1, 1, 1, 3, 1, 2), (0, 8, 1, 0), (0, 7, 3), (0, 7, 4),
        ),
        (
            (1, 1, 1, 2, 1, 2), (1, 1, 1, 2, 0, 1), (0, 7, 5),
        ),
        (
            (0, 8, 1, 1),
        ),
        (
        ),
        (
            (0, 5, 1, 0), (0, 4, 1, 0, 0, 2), (0, 8, 1, 2),
        ),
        (
            (1, 4, 1, 0, 0, 2), (0, 4, 1, 0, 0, 1),
        ),
        (
            (1, 4, 1, 0, 0, 1), (0, 8, 1, 3),
        ),
        (
            (0, 5, 1, 1),
        ),
        (
            (0, 4, 1, 0, 0, 0), (0, 4, 1, 0, 1, 1), (0, 4, 1, 1, 0, 2), (1, 4, 1, 0, 1, 1), (1, 4, 1, 1, 0, 2),
            (0, 4, 1, 0, 1, 0),
        ),
        (
            (0, 4, 1, 1, 0, 1), (1, 4, 1, 1, 0, 1), (0, 4, 1, 2, 0, 2), (0, 5, 1, 2), (0, 5, 1, 3),
            (1, 4, 1, 2, 0, 2), (0, 4, 1, 1, 1, 1), (1, 4, 1, 1, 1, 1), (0, 4, 1, 3, 0, 2), (1, 4, 1, 3, 0, 2),
            (0, 4, 1, 2, 0, 1), (0, 4, 1, 1, 1, 0), (1, 4, 1, 2, 0, 1), (0, 4, 1, 2, 1, 1), (1, 4, 1, 2, 1, 1),
            (0, 4, 1, 3, 0, 1), (1, 4, 1, 3, 0, 1), (0, 4, 1, 3, 1, 1), (1, 4, 1, 3, 1, 1), (0, 4, 1, 2, 0, 0),
            (0, 4, 1, 1, 0, 0), (0, 4, 1, 2, 1, 0),
        ),
        (
        ),
        (
            (0, 4, 1, 3, 0, 0), (0, 4, 1, 3, 1, 0),
        ),
        (
        ),
    ),
)

OWN_FIRST = {}
for at, ops in enumerate(PLAN):
    for op in (op for stage in ops for op in stage):
        if op[:2] == (1, HOP) and op[3] == at:
            OWN_FIRST.setdefault((op[2], at), op[4])


def layer_kernel(
    n_fs,
    groups,
    tokens_in,
    norm_gain_in,
    wq,
    wk,
    wv,
    wg,
    mixer_gain_in,
    wo,
    channel_gain_in,
    wl,
    wr,
    taps_left_in,
    taps_right_in,
    wd,
    cos_in,
    sin_in,
    gammas_in,
    out,
    tokens,
    norm_gain,
    mixer_gain,
    channel_gain,
    taps_left,
    taps_right,
    cos_t,
    sin_t,
    gammas,
    w1,
    wout,
    wlr,
    wdown,
    nt,
    nm,
    qkvg,
    hid,
    gated,
    part1,
    part2,
    xb1,
    xb2,
    sb1,
    sb2,
    rb1,
    rb2,
    mid,
    acc,
    both,
    fin,
    w_send,
    w_recv,
    self_sem,
    h_send,
    h_recv,
    h_rest,
    a_send,
    a_recv,
    f_send,
    f_recv,
    x_send,
    x_recv,
    r_send,
    r_recv,
    o_send,
    o_recv,
    load_sem,
    store_sem,
):
    fs, tp = lax.axis_index("fs"), lax.axis_index("tp")
    planes = n_fs // groups
    z, q = fs // planes, lax.rem(fs, planes)
    other = 1 - tp
    length, width = tokens_in.shape
    own = length // 2
    part_rows = own // NT_PARTS
    span_c = length // CHUNKS
    few = span_c // 2
    kb = wq.shape[0]
    nb = wo.shape[1]
    cq, cv, cf = wq.shape[1] // groups, wv.shape[1] // groups, wl.shape[1] // groups
    upper = z * 2 >= groups
    place_z = jnp.where(upper, groups - 1 - z, z)

    def real(plane):
        return jnp.where(upper, groups - 1 - plane, plane)

    def flip(side):
        return jnp.where(upper, 1 - side, side)

    def zdev(target):
        return {"fs": target * planes + q, "tp": tp}

    partner = {"fs": fs, "tp": other}

    def lanes(index, size):
        return pl.ds(pl.multiple_of(index * size, 128), size)

    def rows(index, size):
        return pl.ds(pl.multiple_of(index * size, size), size)

    pieces = (
        (lambda c: wq.at[:, lanes(c, cq)], lambda f: w1.at[rows(f, kb), pl.ds(0, cq)]),
        (lambda c: wk.at[:, lanes(c, cq)], lambda f: w1.at[rows(f, kb), pl.ds(cq, cq)]),
        (lambda c: wv.at[:, lanes(c, cv)], lambda f: w1.at[rows(f, kb), pl.ds(2 * cq, cv)]),
        (lambda c: wg.at[:, lanes(c, cv)], lambda f: w1.at[rows(f, kb), pl.ds(2 * cq + cv, cv)]),
        (lambda c: wo.at[rows(c, cv), :], lambda f: wout.at[:, lanes(f, nb)]),
        (lambda c: wl.at[:, lanes(c, cf)], lambda f: wlr.at[rows(f, kb), pl.ds(0, cf)]),
        (lambda c: wr.at[:, lanes(c, cf)], lambda f: wlr.at[rows(f, kb), pl.ds(cf, cf)]),
        (lambda c: wd.at[rows(c, cf), :], lambda f: wdown.at[:, lanes(f, nb)]),
    )
    starts = (0, cq, 2 * cq, 2 * cq + cv, 0, 0, cf, 0)
    widths = (cq, cq, cv, cv, 0, cf, cf, 0)

    def stretch(cls, first, count, half=None):
        members = [i for i in range(len(pieces)) if CLASS_OF[i] == cls]
        low = starts[members[0]]
        wide = sum(widths[i] for i in members)
        if members[0] == 4 or members[0] == 7:
            buf, size = (wout, cv) if members[0] == 4 else (wdown, cf)
            across = pl.ds(pl.multiple_of(first * nb, 128), count * nb)
            if half is None:
                return buf.at[:, across]
            return buf.at[pl.ds(half * (size // 2), size // 2), across]
        buf = w1 if members[0] < 4 else wlr
        if half is None:
            return buf.at[pl.ds(pl.multiple_of(first * kb, kb), count * kb), pl.ds(low, wide)]
        start = pl.multiple_of(first * kb + half * (kb // 2), kb // 2)
        return buf.at[pl.ds(start, kb // 2), pl.ds(low, wide)]

    barrier = pltpu.get_barrier_semaphore()
    for step in range(1, groups):
        pl.semaphore_signal(barrier, inc=1, device_id=zdev(lax.rem(z + step, groups)), device_id_type=MESH)
    qx = q + 1 - 2 * lax.rem(q, 2)
    qy = q + 2 - 4 * (q // 2)
    diagonal = planes - 1 - q
    to_x = {"fs": z * planes + qx, "tp": tp}
    to_y = {"fs": z * planes + qy, "tp": tp}
    for device in (to_x, to_y):
        pl.semaphore_signal(barrier, inc=1, device_id=device, device_id_type=MESH)
    pl.semaphore_signal(barrier, inc=1, device_id=partner, device_id_type=MESH)

    loads = []
    for i, (source, held_here) in enumerate((
        (tokens_in, tokens), (norm_gain_in, norm_gain), (mixer_gain_in, mixer_gain),
        (channel_gain_in, channel_gain), (taps_left_in, taps_left), (taps_right_in, taps_right),
        (cos_in, cos_t), (sin_in, sin_t), (gammas_in, gammas),
    )):
        load = pltpu.make_async_copy(source, held_here, load_sem.at[i])
        load.start()
        loads.append(load)
    keeps = []
    for i, (src, dst) in enumerate(pieces):
        keep = pltpu.make_async_copy(src(z), dst(fs), self_sem.at[i])
        keep.start()
        keeps.append(keep)

    def prepare(_):
        for load in loads:
            load.wait()
        my_half = pl.ds(pl.multiple_of(tp * own, own), own)
        nt[pl.ds(pl.multiple_of(z * length + tp * own, own), own), :] = normed_rows(
            tokens[my_half, :].astype(jnp.float32), norm_gain[...]
        )

    pl.semaphore_wait(barrier, groups - 1 + 2 + 1)

    def remote(src, dst, ssem, rsem, device):
        return pltpu.make_async_remote_copy(
            src_ref=src, dst_ref=dst, send_sem=ssem, recv_sem=rsem,
            device_id=device, device_id_type=MESH,
        )

    def block(key, c, seq, core):
        if key:
            first = c * groups * span_c + seq * span_c + core * few
            return nm.at[pl.ds(pl.multiple_of(first, few), few), :]
        first = seq * length + core * own + c * part_rows
        return nt.at[pl.ds(pl.multiple_of(first, part_rows), part_rows), :]

    part, xb, sb, rb = (part1, part2), (xb1, xb2), (sb1, sb2), (rb1, rb2)

    def pair(which, c, g):
        return part[which][c, tp, g].astype(jnp.float32) + xb[which][c, g].astype(jnp.float32)

    def exchange(which, c):
        return remote(part[which].at[c, other], xb[which].at[c], x_send.at[which], x_recv.at[which, c], partner)

    def gather_copy(me, key, c, side, d, landing=False):
        move = 1 - 2 * side
        source = real(me - move * d)
        ref = block(key, c, source, tp)
        at = c + key * NT_PARTS
        device = partner if landing else zdev(real(me + move))
        return remote(ref, ref, a_send.at[key], a_recv.at[at, source], device)

    def core_copy(me, key, c, side, d):
        move = 1 - 2 * side
        ref = block(key, c, real(me - move * d), tp)
        return remote(ref, ref, f_send.at[key], f_recv.at[key * (1 + c)], partner)

    def weight_copy(me, i, plane):
        src, dst = pieces[i]
        far = real(plane)
        return remote(src(far), dst(fs), w_send.at[i], w_recv.at[CLASS_OF[i], z], zdev(far))

    def hop_copy(me, cls, plane, slot, landing=False):
        origin = (qx, qy)[slot] if landing else (q, q, q, q, qx, qy)[slot]
        source = real(plane)
        ref = stretch(cls, source * planes + origin, 1, (0, 1, 1, 0, 0, 1)[slot])
        device = (to_x, to_y, to_x, to_y, to_y, to_x)[slot]
        landed = h_recv.at[cls, source, slot] if slot < 2 else h_rest.at[cls]
        return remote(ref, ref, h_send.at[cls], landed, device)

    def sum_copy(me, which, c, side, d, landing=False):
        ref = sb[which].at[c, flip(side), d]
        at = d if landing else d - 1
        device = partner if landing else zdev(real(me + 1 - 2 * side))
        return remote(ref, rb[which].at[c, flip(side), at], r_send.at[which], r_recv.at[which, c, flip(side), at], device)

    makers = (gather_copy, core_copy, weight_copy, hop_copy, sum_copy)

    def await_bytes(ref, sem):
        remote(ref, ref, sem, sem, partner).wait_recv()

    def act(me, op):
        sends, kind, args = op[0], op[1], op[2:]
        if not sends:
            if kind == SWAP:
                exchange(*args).wait_recv()
            elif kind == WEIGHTS:
                cls, far = args[0], real(args[1])
                await_bytes(stretch(cls, far * planes + q, 1), w_recv.at[cls, far])
            elif kind == HOPS:
                await_bytes(stretch(args[0], 0, 2 * groups), h_rest.at[args[0]])
            elif kind == CORES:
                key, c = args
                if key:
                    await_bytes(nm.at[pl.ds(0, groups * few), :], f_recv.at[1 + c])
                else:
                    await_bytes(nt.at[pl.ds(0, groups * own), :], f_recv.at[0])
            else:
                makers[kind](me, *args, True).wait_recv()
            return
        if kind == HOP and args[1] == me and args[2] == OWN_FIRST[args[0], me]:
            for i, keep in enumerate(keeps):
                if CLASS_OF[i] == args[0]:
                    keep.wait()
        if kind == SUM:
            which, c, side, d = args
            move = 1 - 2 * side
            value = pair(which, c, real(me + move * d))
            if 0 <= me - move < groups:
                value = value + rb[which][c, flip(side), d].astype(jnp.float32)
            sb[which][c, flip(side), d] = value.astype(jnp.bfloat16)
        makers[kind](me, *args).start()

    def perform(stage):
        for me, ops in enumerate(PLAN):
            @pl.when(place_z == me)
            def _():
                for op in ops[stage]:
                    act(me, op)

    def multiply(left, weight, which, c):
        value = jnp.dot(
            left[rows(c, groups * span_c), :], weight[...], preferred_element_type=jnp.float32
        ).astype(jnp.bfloat16)
        for g in range(groups):
            part[which][c, 0, g] = value[g * span_c : g * span_c + few]
            part[which][c, 1, g] = value[g * span_c + few : (g + 1) * span_c]
        exchange(which, c).start()

    def collect(which, c):
        acc[c] = pair(which, c, z)
        for side, has in ((0, z > 0), (1, z < groups - 1)):
            @pl.when(has)
            def _():
                acc[c] = acc[c] + rb[which][c, side, 0].astype(jnp.float32)
        return acc[c]

    def natural(c, core):
        return pl.ds(pl.multiple_of(c * span_c + core * few, few), few)

    head = tp * groups + z
    chunk = groups * length // 2

    def project(at):
        span = rows(at, chunk)
        qkvg[span, :] = jnp.dot(
            nt[span, :], w1[...], preferred_element_type=jnp.float32
        ).astype(jnp.bfloat16)

    def retain(first):
        log_gamma = gammas[pl.ds(head, 1), :]
        distance = (
            lax.broadcasted_iota(jnp.int32, (length, length), 0)
            - lax.broadcasted_iota(jnp.int32, (length, length), 1)
        ).astype(jnp.float32)
        decay = jnp.where(distance >= 0, jnp.exp(log_gamma * jnp.maximum(distance, 0.0)), 0.0)

        @pl.loop(first * groups // 2, (first + 1) * groups // 2)
        def _(at):
            span = rows(at, length)
            held = qkvg[span, :].astype(jnp.float32)

            def turn(x):
                return x * cos_t[...] + pltpu.roll(x, cq // 2, 1) * sin_t[...]

            rq = turn(held[:, :cq])
            rk = turn(held[:, cq : 2 * cq])
            scores = lax.dot_general(
                rq, rk, (((1,), (1,)), ((), ())), precision=highest, preferred_element_type=jnp.float32
            ) * decay
            kept = jnp.dot(
                scores, held[:, 2 * cq : 2 * cq + cv], precision=highest,
                preferred_element_type=jnp.float32,
            )
            kept = kept * lax.rsqrt(jnp.mean(kept * kept, axis=-1, keepdims=True) + 1e-06)
            gain = mixer_gain[:, lanes(z, cv)]
            whole = (kept * gain * silu(held[:, 2 * cq + cv :])).astype(jnp.bfloat16)
            for c in range(CHUNKS):
                hid[rows(at + c * groups, span_c), :] = whole[c * span_c : (c + 1) * span_c]

    def renorm(c):
        middle = (
            tokens[natural(c, tp), :].astype(jnp.float32) + collect(0, c)
        ).astype(jnp.bfloat16).astype(jnp.float32)
        mid[c] = middle
        first = c * groups * span_c + z * span_c + tp * few
        nm[pl.ds(pl.multiple_of(first, few), few), :] = normed_rows(middle, channel_gain[...])

    place = lax.rem(lax.broadcasted_iota(jnp.int32, (groups * span_c, 1), 0), span_c)

    def convolve(c, low, taps):
        x = both[c, :, low : low + cf].astype(jnp.float32)
        count = taps.shape[0]
        weights = taps[:, lanes(z, cf)]
        result = x * weights[count - 1 :, :]
        for back in range(1, count):
            if c:
                before = both[c - 1, :, low : low + cf].astype(jnp.float32)
                before = pltpu.roll(before, back + (groups - 1) * span_c, 0)
            else:
                before = 0.0
            moved = jnp.where(place >= back, pltpu.roll(x, back, 0), before)
            result = result + moved * weights[count - 1 - back : count - back, :]
        return result

    def mix(c):
        both[c] = jnp.dot(
            nm[rows(c, groups * span_c), :], wlr[...], preferred_element_type=jnp.float32
        ).astype(jnp.bfloat16)
        gated[rows(c, groups * span_c), :] = (
            silu(convolve(c, 0, taps_left)) * convolve(c, cf, taps_right)
        ).astype(jnp.bfloat16)

    def finish(c):
        mine = natural(c, tp)
        fin[c] = (mid[c] + collect(1, c)).astype(jnp.bfloat16)
        remote(fin.at[c], out.at[mine, :], o_send.at[0], o_recv.at[0], partner).start()
        pltpu.make_async_copy(fin.at[c], out.at[mine, :], store_sem.at[0]).start()

    steps = (
        project,
        retain,
        lambda c: multiply(hid, wout, 0, c),
        renorm,
        mix,
        lambda c: multiply(gated, wdown, 1, c),
        finish,
        prepare,
    )
    perform(0)
    for stage, (name, index) in enumerate(STAGES):
        steps[name](index)
        perform(stage + 1)
    await_bytes(fin, o_recv.at[0])
    await_bytes(fin, o_send.at[0])
    for key, buf in ((0, nt), (1, nm)):
        await_bytes(buf.at[pl.ds(0, groups * own), :], f_send.at[key])
        await_bytes(part[key].at[:, 0], x_send.at[key])
        await_bytes(sb[key].at[:, 0, pl.ds(0, groups - 1)], r_send.at[key])
    for cls in range(max(CLASS_OF) + 1):
        await_bytes(stretch(cls, 0, 3 * groups), h_send.at[cls])
    for i, (_, dst) in enumerate(pieces):
        if i == 4 or i == 7:
            ref = (wout if i == 4 else wdown).at[:, pl.ds(0, (groups - 1) * nb)]
        else:
            ref = (w1 if i < 4 else wlr).at[pl.ds(0, (groups - 1) * kb), pl.ds(starts[i], widths[i])]
        await_bytes(ref, w_send.at[i])
    for me, ops in enumerate(PLAN):
        @pl.when(place_z == me)
        def _():
            for key, buf, size in ((0, nt, part_rows), (1, nm, few)):
                count = sum(op[:3] == (1, 0, key) for stage in ops for op in stage)
                await_bytes(buf.at[pl.ds(0, count * size), :], a_send.at[key])
    pltpu.make_async_copy(fin, fin, store_sem.at[0]).wait()


def body(n_fs, *args):
    (tokens, norm_gain, w_query, w_key, w_value, w_gate, mixer_gain, w_out, channel_gain,
     w_left, w_right, taps_left, taps_right, w_down) = args
    groups = w_query.shape[1] // DK
    if (
        groups != 2 * len(PLAN)
        or n_fs % groups
        or n_fs != 4 * groups
        or lax.axis_size("tp") != 2
        or tokens.shape[0] != BLOCK
        or (w_left.shape[1] // groups) % 128
        or w_left.shape[1] % groups
        or w_out.shape[1] % 128
        or w_query.shape[0] % 32
        or tokens.shape[0] % (32 * CHUNKS)
    ):
        return plain_body(*args)
    length, width = tokens.shape
    heads = groups * lax.axis_size("tp")
    cq, cv, cf = w_query.shape[1] // groups, w_value.shape[1] // groups, w_left.shape[1] // groups
    planes = n_fs // groups
    span_c = length // CHUNKS
    few = span_c // 2
    classes = max(CLASS_OF) + 1
    cos_t, sin_t = turning(length, DK)
    gammas = log_gammas(heads)
    held = pl.BlockSpec(memory_space=pl.ANY)
    bf, f32, dma = jnp.bfloat16, jnp.float32, pltpu.SemaphoreType.DMA
    return pl.pallas_call(
        functools.partial(layer_kernel, n_fs, groups),
        out_shape=jax.ShapeDtypeStruct(tokens.shape, bf),
        in_specs=[held] * 17,
        out_specs=held,
        scratch_shapes=[
            pltpu.VMEM(tokens.shape, bf),
            pltpu.VMEM((1, width), f32),
            pltpu.VMEM((1, w_value.shape[1]), f32),
            pltpu.VMEM((1, width), f32),
            pltpu.VMEM(taps_left.shape, f32),
            pltpu.VMEM(taps_right.shape, f32),
            pltpu.VMEM(cos_t.shape, f32),
            pltpu.VMEM(sin_t.shape, f32),
            pltpu.VMEM(gammas.shape, f32),
            pltpu.VMEM((width, 2 * cq + 2 * cv), bf),
            pltpu.VMEM((cv, width), bf),
            pltpu.VMEM((width, 2 * cf), bf),
            pltpu.VMEM((cf, width), bf),
            pltpu.VMEM((groups * length, width), bf),
            pltpu.VMEM((groups * length, width), bf),
            pltpu.VMEM((groups * length, 2 * cq + 2 * cv), bf),
            pltpu.VMEM((groups * length, cv), bf),
            pltpu.VMEM((groups * length, cf), bf),
            pltpu.VMEM((CHUNKS, 2, groups, few, width), bf),
            pltpu.VMEM((CHUNKS, 2, groups, few, width), bf),
            pltpu.VMEM((CHUNKS, groups, few, width), bf),
            pltpu.VMEM((CHUNKS, groups, few, width), bf),
            pltpu.VMEM((CHUNKS, 2, groups, few, width), bf),
            pltpu.VMEM((CHUNKS, 2, groups, few, width), bf),
            pltpu.VMEM((CHUNKS, 2, groups, few, width), bf),
            pltpu.VMEM((CHUNKS, 2, groups, few, width), bf),
            pltpu.VMEM((CHUNKS, few, width), f32),
            pltpu.VMEM((CHUNKS, few, width), f32),
            pltpu.VMEM((CHUNKS, groups * span_c, 2 * cf), bf),
            pltpu.VMEM((CHUNKS, few, width), bf),
            dma((8,)),
            dma((classes, groups)),
            dma((8,)),
            dma((classes,)),
            dma((classes, groups, 2)),
            dma((classes,)),
            dma((2,)),
            dma((NT_PARTS + CHUNKS, groups)),
            dma((2,)),
            dma((1 + CHUNKS,)),
            dma((2,)),
            dma((2, CHUNKS)),
            dma((2,)),
            dma((2, CHUNKS, 2, groups - 1)),
            dma((1,)),
            dma((1,)),
            dma((9,)),
            dma((1,)),
        ],
        compiler_params=pltpu.CompilerParams(
            collective_id=0, has_side_effects=True, vmem_limit_bytes=60 * 1024 * 1024
        ),
    )(
        tokens, norm_gain[None], w_query, w_key, w_value, w_gate, mixer_gain[None], w_out,
        channel_gain[None], w_left, w_right, taps_left, taps_right, w_down,
        cos_t, sin_t, gammas,
    )


def solution(mesh):
    placed = (
        P("fs", None),
        P(),
        P("fs", "tp"),
        P("fs", "tp"),
        P("fs", "tp"),
        P("fs", "tp"),
        P("tp"),
        P("tp", "fs"),
        P(),
        P("fs", "tp"),
        P("fs", "tp"),
        P(None, "tp"),
        P(None, "tp"),
        P("tp", "fs"),
    )
    return jax.shard_map(
        functools.partial(body, mesh.shape["fs"]), mesh=mesh, in_specs=placed, out_specs=P("fs", None), check_vma=False)
```

```python
import functools

import jax
import jax.numpy as jnp
import numpy as np
from jax import lax
from jax.experimental import pallas as pl
from jax.experimental.pallas import tpu as pltpu
from jax.sharding import PartitionSpec as P

DK = 128
DV = 256
BLOCK = 128
MESH = pl.DeviceIdType.MESH


highest = lax.Precision.HIGHEST


def scale_rows(rows_in, gain_vec):
    floats = rows_in.astype(jnp.float32)
    factor = lax.rsqrt(jnp.mean(floats * floats, axis=-1, keepdims=True) + 1e-06)
    return (floats * factor * gain_vec).astype(jnp.bfloat16)


def decays(first_head, count):
    head_ids = first_head + jnp.arange(count, dtype=jnp.float32)
    return jnp.log(1.0 - 2.0 ** (-5.0 - head_ids))


def rotate(heads_in, positions):
    width = heads_in.shape[-1]
    half = width // 2
    freqs = 10000.0 ** (-jnp.arange(half, dtype=jnp.float32) / half)
    angles = positions[:, None] * freqs[None, :]
    cosine = jnp.cos(angles)
    sine = jnp.sin(angles)
    first_half = heads_in[..., :half]
    second_half = heads_in[..., half:]
    return jnp.concatenate(
        [first_half * cosine - second_half * sine, first_half * sine + second_half * cosine],
        axis=-1,
    )


def retention(queries, keys_in, values_in, log_gamma):
    head_count, length, key_width = queries.shape
    value_width = values_in.shape[-1]
    blocks = length // BLOCK
    queries = queries.reshape(head_count, blocks, BLOCK, key_width)
    keys_in = keys_in.reshape(head_count, blocks, BLOCK, key_width)
    values_in = values_in.reshape(head_count, blocks, BLOCK, value_width)
    offsets = jnp.arange(BLOCK, dtype=jnp.float32)
    distance = offsets[:, None] - offsets[None, :]
    weights = jnp.where(
        distance >= 0, jnp.exp(log_gamma[:, None, None] * jnp.maximum(distance, 0.0)), 0.0
    )
    scores = jnp.einsum("hbnd,hbmd->hbnm", queries, keys_in, precision=highest) * weights[:, None]
    inner = jnp.einsum("hbnm,hbme->hbne", scores, values_in, precision=highest)
    key_weight = jnp.exp(log_gamma[:, None] * (BLOCK - 1 - offsets)[None, :])
    contrib = jnp.einsum(
        "hbjd,hbje->hbde", keys_in * key_weight[:, None, :, None], values_in, precision=highest
    )
    block_decay = jnp.exp(log_gamma * BLOCK)[:, None, None]

    def advance(state, contrib_block):
        return (state * block_decay + contrib_block, state)

    _, states = lax.scan(
        advance,
        jnp.zeros((head_count, key_width, value_width), jnp.float32),
        jnp.moveaxis(contrib, 1, 0),
    )
    states = jnp.moveaxis(states, 0, 1)
    query_weight = jnp.exp(log_gamma[:, None] * (offsets + 1.0)[None, :])
    carried = (
        jnp.einsum("hbnd,hbde->hbne", queries, states, precision=highest)
        * query_weight[:, None, :, None]
    )
    return (inner + carried).reshape(head_count, length, value_width)


def head_norm(retained):
    return retained * lax.rsqrt(jnp.mean(retained * retained, axis=-1, keepdims=True) + 1e-06)


def causal_taps(values_in, taps):
    length = values_in.shape[-2]
    padded = jnp.pad(values_in.astype(jnp.float32), ((taps.shape[0] - 1, 0), (0, 0)))
    result = padded[0:length] * taps[0]
    for tap_index in range(1, taps.shape[0]):
        result = result + padded[tap_index : tap_index + length] * taps[tap_index]
    return result


def fold_single(source, weight_piece):
    return jnp.dot(source, weight_piece, preferred_element_type=jnp.float32)


def collect_single(source, weight):
    return fold_single(source, lax.all_gather(weight, "fs", axis=0, tiled=True))


def plain_body(
    tokens,
    norm_gain,
    w_query,
    w_key,
    w_value,
    w_gate,
    mixer_gain,
    w_out,
    channel_gain,
    w_left,
    w_right,
    taps_left,
    taps_right,
    w_down,
):
    length = tokens.shape[0]
    normed = scale_rows(tokens, norm_gain)
    queries = collect_single(normed, w_query)
    keys_proj = collect_single(normed, w_key)
    values_proj = collect_single(normed, w_value)
    gates = collect_single(normed, w_gate)
    queries = queries.astype(jnp.bfloat16)
    keys_proj = keys_proj.astype(jnp.bfloat16)
    values_proj = values_proj.astype(jnp.bfloat16)
    gates = gates.astype(jnp.bfloat16)
    heads_here = w_query.shape[1] // DK
    first_head = (lax.axis_index("tp") * heads_here).astype(jnp.float32)
    log_gamma = decays(first_head, heads_here)
    positions = jnp.arange(length, dtype=jnp.float32)

    def split_heads(rows_in, width):
        return rows_in.astype(jnp.float32).reshape(length, heads_here, width).transpose(1, 0, 2)

    retained = head_norm(
        retention(
            rotate(split_heads(queries, DK), positions),
            rotate(split_heads(keys_proj, DK), positions),
            split_heads(values_proj, DV),
            log_gamma,
        )
    )
    retained = retained.transpose(1, 0, 2).reshape(length, heads_here * DV)
    hidden = (retained * mixer_gain * jax.nn.silu(gates.astype(jnp.float32))).astype(jnp.bfloat16)
    rows_own = length // lax.axis_size("tp")
    first_row = lax.axis_index("tp") * rows_own
    out_whole = lax.all_gather(w_out, "fs", axis=1, tiled=True)
    mixer_total = lax.psum_scatter(
        jnp.dot(hidden, out_whole, preferred_element_type=jnp.float32).astype(jnp.bfloat16),
        "tp",
        scatter_dimension=0,
        tiled=True,
    ).astype(jnp.float32)
    residual = lax.dynamic_slice_in_dim(tokens, first_row, rows_own, 0)
    middle_own = (residual.astype(jnp.float32) + mixer_total).astype(jnp.bfloat16)
    middle = lax.all_gather(middle_own, "tp", axis=0, tiled=True)
    normed_mid = scale_rows(middle, channel_gain)
    left = collect_single(normed_mid, w_left)
    right = collect_single(normed_mid, w_right)
    left = left.astype(jnp.bfloat16)
    right = right.astype(jnp.bfloat16)
    gated = (jax.nn.silu(causal_taps(left, taps_left)) * causal_taps(right, taps_right)).astype(
        jnp.bfloat16
    )
    down_whole = lax.all_gather(w_down, "fs", axis=1, tiled=True)
    channel_part = jnp.dot(gated, down_whole, preferred_element_type=jnp.float32)
    channel_total = lax.psum(channel_part.astype(jnp.bfloat16), "tp").astype(jnp.float32)
    return (middle.astype(jnp.float32) + channel_total).astype(jnp.bfloat16)


def log_gammas(head_count):
    table = np.log(1.0 - 2.0 ** (-5.0 - np.arange(head_count, dtype=np.float64)))
    return np.repeat(table[:, None], BLOCK, axis=1).astype(np.float32)


def turning(length, width):
    half = width // 2
    freqs = np.float32(10000.0) ** (-np.arange(half, dtype=np.float32) / np.float32(half))
    angles = (np.arange(length, dtype=np.float32)[:, None] * freqs[None, :]).astype(np.float64)
    cosine, sine = np.cos(angles), np.sin(angles)
    return (
        np.concatenate([cosine, cosine], axis=1).astype(np.float32),
        np.concatenate([-sine, sine], axis=1).astype(np.float32),
    )


def silu(v):
    return v / (1.0 + jnp.exp(-v))


def normed_rows(floats, gain):
    factor = lax.rsqrt(jnp.mean(floats * floats, axis=-1, keepdims=True) + 1e-06)
    return (floats * factor * gain).astype(jnp.bfloat16)


HOP, SUM, SWAP, WEIGHTS, HOPS, CORES = 3, 4, 5, 6, 7, 8
CHUNKS = 4
NT_PARTS = 2
CLASS_OF = (0, 0, 0, 1, 2, 3, 4, 5)
STAGES = (
    (7, 0),
    (0, 0),
    (0, 1),
    (1, 0),
    (1, 1),
    (2, 0),
    (2, 1),
    (2, 2),
    (2, 3),
    (3, 0),
    (3, 1),
    (3, 2),
    (3, 3),
    (4, 0),
    (5, 0),
    (4, 1),
    (5, 1),
    (4, 2),
    (5, 2),
    (4, 3),
    (5, 3),
    (6, 0),
    (6, 1),
    (6, 2),
    (6, 3),
)
PLAN = (
    (
        (
            (1, 2, 0, 3), (1, 2, 3, 1), (1, 2, 3, 3), (1, 3, 4, 0, 0),
        ),
        (
            (1, 3, 0, 0, 0), (0, 6, 1, 1), (1, 3, 1, 1, 1), (1, 3, 1, 1, 3), (1, 3, 1, 1, 2), (1, 3, 3, 0, 0),
            (1, 3, 1, 1, 0), (1, 2, 2, 3), (1, 2, 1, 3), (1, 3, 3, 0, 1), (1, 3, 0, 0, 2), (1, 3, 1, 0, 0),
            (1, 3, 1, 0, 1), (1, 3, 1, 0, 3), (0, 6, 1, 3), (1, 3, 1, 3, 3), (1, 3, 1, 3, 2), (1, 3, 0, 0, 1),
            (1, 0, 0, 0, 0, 0), (1, 0, 0, 1, 0, 0), (0, 3, 0, 0, 0), (1, 3, 5, 0, 0), (1, 3, 5, 0, 1),
            (1, 3, 1, 3, 0), (1, 3, 4, 0, 1), (0, 6, 0, 1), (1, 3, 0, 1, 2), (1, 3, 0, 1, 0), (1, 3, 0, 1, 3),
            (1, 3, 0, 1, 1), (1, 2, 0, 1), (1, 3, 0, 0, 3), (1, 3, 1, 3, 1), (0, 3, 1, 1, 1), (1, 3, 1, 1, 5),
            (0, 6, 2, 1), (0, 3, 3, 0, 1), (1, 3, 2, 1, 0), (1, 3, 2, 1, 3), (1, 3, 2, 1, 2), (1, 3, 1, 0, 2),
            (0, 6, 0, 3), (1, 3, 2, 0, 0), (1, 3, 0, 3, 3), (1, 3, 0, 3, 1), (1, 3, 2, 1, 1), (1, 2, 1, 1),
            (1, 2, 4, 3), (1, 3, 0, 3, 0), (0, 3, 0, 0, 1), (1, 3, 0, 3, 2), (1, 3, 2, 0, 2), (1, 2, 2, 1),
            (1, 3, 0, 0, 5), (0, 3, 0, 1, 0), (1, 3, 0, 1, 4), (1, 2, 3, 2), (1, 2, 4, 1), (0, 6, 2, 3),
            (0, 3, 1, 3, 1), (1, 3, 1, 3, 5), (1, 3, 2, 3, 1), (1, 2, 0, 2), (0, 6, 1, 2), (1, 3, 1, 2, 2),
            (1, 3, 0, 0, 4), (1, 3, 2, 3, 3), (0, 6, 5, 1), (1, 3, 2, 3, 0), (1, 3, 1, 2, 1), (1, 3, 1, 2, 3),
            (0, 3, 0, 1, 1), (1, 3, 0, 1, 5), (0, 3, 0, 3, 1), (1, 3, 1, 2, 0), (0, 0, 0, 0, 1, 1),
            (1, 1, 0, 0, 1, 1), (0, 3, 1, 3, 0), (0, 3, 0, 3, 0), (1, 3, 2, 0, 1), (1, 2, 1, 2), (1, 1, 0, 1, 0, 0),
            (0, 6, 3, 1), (1, 3, 3, 1, 2), (1, 3, 3, 1, 1), (1, 3, 3, 0, 3), (1, 3, 1, 3, 4), (1, 3, 0, 3, 4),
            (1, 3, 0, 3, 5), (1, 1, 0, 0, 0, 0), (0, 3, 5, 0, 1), (1, 3, 5, 0, 5), (0, 6, 4, 1), (1, 3, 4, 1, 0),
            (1, 3, 4, 1, 1), (1, 2, 2, 2), (1, 3, 3, 0, 2), (1, 2, 4, 2), (1, 2, 5, 2), (0, 3, 1, 2, 0),
            (0, 3, 2, 0, 0), (1, 3, 3, 1, 0), (0, 3, 1, 1, 0), (1, 3, 1, 1, 4), (1, 3, 5, 1, 1), (0, 3, 1, 0, 1),
            (1, 3, 1, 2, 4), (0, 6, 0, 2), (1, 3, 1, 0, 5), (1, 3, 0, 2, 1), (1, 2, 6, 1), (1, 3, 0, 2, 0),
            (0, 6, 2, 2), (1, 3, 2, 2, 0), (1, 3, 2, 2, 1), (0, 3, 1, 2, 1), (0, 3, 1, 0, 0), (0, 3, 4, 0, 0),
            (1, 3, 1, 2, 5), (0, 0, 0, 0, 1, 3), (1, 1, 0, 0, 1, 3), (1, 3, 1, 0, 4), (1, 2, 7, 1), (1, 3, 0, 2, 3),
            (1, 3, 0, 2, 2), (0, 0, 0, 1, 1, 2), (1, 1, 0, 1, 1, 2), (0, 3, 0, 2, 1), (1, 3, 0, 2, 5),
            (0, 3, 0, 2, 0), (1, 3, 0, 2, 4), (1, 3, 2, 2, 3), (1, 2, 5, 1), (0, 0, 0, 1, 1, 1), (1, 1, 0, 1, 1, 1),
            (1, 3, 3, 1, 3), (0, 0, 0, 0, 1, 2), (1, 1, 0, 0, 1, 2), (0, 3, 2, 0, 1), (1, 2, 5, 3), (0, 3, 4, 1, 1),
            (0, 3, 2, 2, 0), (1, 2, 7, 3), (1, 3, 2, 2, 4), (0, 3, 2, 2, 1), (0, 3, 2, 1, 0), (0, 3, 2, 1, 1),
            (1, 3, 2, 3, 2), (1, 3, 2, 2, 5), (1, 3, 2, 0, 3), (0, 7, 1), (0, 0, 0, 1, 1, 3), (1, 1, 0, 1, 1, 3),
            (0, 3, 2, 3, 1), (1, 3, 2, 3, 5), (1, 3, 2, 1, 5), (1, 3, 5, 1, 3), (1, 3, 5, 1, 0), (1, 3, 2, 0, 5),
            (0, 3, 2, 3, 0), (1, 3, 2, 3, 4), (1, 2, 7, 2), (1, 3, 2, 2, 2), (1, 3, 2, 0, 4), (1, 3, 2, 1, 4),
            (0, 8, 0, 0), (0, 7, 0),
        ),
        (
            (0, 3, 5, 1, 1),
        ),
        (
        ),
        (
            (1, 2, 6, 3), (1, 3, 4, 1, 2), (0, 3, 4, 0, 1), (1, 3, 4, 0, 5),
        ),
        (
            (0, 3, 5, 1, 0), (1, 3, 4, 1, 5), (0, 3, 5, 0, 0), (1, 3, 4, 0, 3), (0, 6, 5, 2), (1, 3, 5, 2, 3),
            (1, 3, 5, 1, 5), (0, 6, 3, 3), (1, 3, 5, 2, 2), (0, 7, 2),
        ),
        (
            (0, 6, 3, 2), (1, 3, 3, 2, 3), (1, 3, 5, 2, 1), (1, 3, 3, 3, 0),
        ),
        (
            (1, 3, 5, 2, 0),
        ),
        (
            (0, 6, 5, 3), (1, 3, 5, 3, 1), (1, 3, 5, 3, 3), (1, 3, 5, 3, 0), (0, 5, 0, 0), (1, 4, 0, 0, 0, 2),
        ),
        (
            (1, 4, 0, 0, 0, 3), (0, 5, 0, 3), (1, 4, 0, 3, 0, 3), (0, 3, 3, 1, 1), (1, 3, 4, 0, 4),
            (1, 4, 0, 0, 0, 1), (1, 3, 5, 1, 2), (1, 3, 3, 2, 0), (1, 3, 3, 2, 1), (0, 6, 4, 3), (1, 3, 3, 2, 2),
            (1, 3, 4, 3, 2), (0, 5, 0, 1), (1, 4, 0, 1, 0, 3), (1, 3, 4, 3, 1), (1, 3, 4, 3, 0), (0, 5, 0, 2),
            (1, 3, 3, 3, 3), (1, 4, 0, 1, 0, 2), (1, 4, 0, 2, 0, 3), (0, 3, 5, 2, 1), (1, 3, 5, 0, 2), (0, 6, 4, 2),
            (1, 3, 4, 2, 0), (1, 3, 3, 3, 2), (1, 3, 3, 3, 1), (1, 3, 4, 0, 2), (1, 3, 4, 2, 3), (1, 4, 0, 3, 0, 2),
            (1, 3, 5, 3, 2), (1, 3, 3, 1, 5), (0, 3, 3, 2, 0), (1, 3, 3, 2, 4), (1, 3, 4, 2, 1), (1, 3, 5, 1, 4),
            (0, 3, 3, 0, 0), (1, 4, 0, 1, 0, 1), (1, 4, 0, 2, 0, 2), (0, 4, 0, 0, 1, 0), (1, 3, 3, 0, 4),
        ),
        (
            (0, 3, 4, 3, 0), (0, 0, 1, 0, 1, 1), (1, 0, 1, 0, 0, 0), (1, 3, 4, 2, 2), (0, 3, 3, 1, 0),
            (0, 3, 3, 3, 0), (1, 3, 3, 1, 4), (1, 3, 5, 0, 3), (0, 3, 4, 2, 0), (0, 3, 4, 2, 1), (1, 3, 3, 3, 4),
            (1, 4, 0, 3, 0, 1), (0, 3, 4, 1, 0), (1, 3, 5, 2, 5), (0, 3, 5, 3, 1), (1, 4, 0, 2, 0, 1),
            (0, 4, 0, 1, 1, 0),
        ),
        (
            (1, 1, 1, 1, 0, 0), (1, 3, 4, 2, 4), (0, 3, 3, 3, 1), (1, 0, 1, 1, 0, 0), (1, 2, 6, 2),
            (1, 1, 1, 0, 0, 0), (1, 3, 4, 3, 4), (1, 3, 4, 2, 5), (0, 3, 4, 3, 1), (1, 3, 4, 3, 5), (1, 3, 5, 3, 5),
            (1, 3, 3, 3, 5), (1, 3, 4, 3, 3), (0, 3, 5, 2, 0), (1, 3, 5, 2, 4), (0, 3, 3, 2, 1), (0, 3, 5, 3, 0),
            (1, 3, 3, 2, 5), (0, 4, 0, 2, 1, 0),
        ),
        (
            (1, 3, 4, 1, 4), (1, 0, 1, 2, 0, 0), (0, 4, 0, 3, 1, 0), (1, 3, 4, 1, 3), (1, 3, 5, 3, 4),
        ),
        (
            (1, 0, 1, 3, 0, 0), (1, 1, 1, 3, 0, 0), (1, 3, 3, 0, 5), (1, 1, 1, 0, 1, 1), (0, 0, 1, 1, 1, 1),
            (1, 3, 5, 0, 4), (0, 0, 1, 1, 1, 2), (0, 0, 1, 0, 1, 2), (1, 1, 1, 1, 1, 2), (1, 1, 1, 0, 1, 2),
            (0, 0, 1, 0, 1, 3), (1, 1, 1, 0, 1, 3), (0, 8, 1, 0), (0, 7, 3), (0, 7, 4),
        ),
        (
            (0, 7, 5), (1, 1, 1, 1, 1, 1),
        ),
        (
            (0, 0, 1, 1, 1, 3), (1, 1, 1, 1, 1, 3), (1, 1, 1, 2, 0, 0), (0, 5, 1, 0), (1, 4, 1, 0, 0, 2),
            (1, 4, 1, 0, 0, 1), (0, 8, 1, 1),
        ),
        (
        ),
        (
            (1, 4, 1, 0, 0, 3), (0, 0, 1, 2, 1, 3), (1, 1, 1, 2, 1, 3), (0, 0, 1, 2, 1, 2), (0, 0, 1, 3, 1, 1),
            (1, 1, 1, 3, 1, 1), (1, 1, 1, 2, 1, 2), (0, 0, 1, 2, 1, 1), (1, 1, 1, 2, 1, 1), (0, 5, 1, 1),
            (1, 4, 1, 1, 0, 2), (0, 0, 1, 3, 1, 2), (1, 1, 1, 3, 1, 2), (1, 4, 1, 1, 0, 3), (1, 4, 1, 1, 0, 1),
            (0, 0, 1, 3, 1, 3), (1, 1, 1, 3, 1, 3), (0, 8, 1, 2),
        ),
        (
        ),
        (
            (0, 8, 1, 3),
        ),
        (
        ),
        (
            (0, 5, 1, 2), (1, 4, 1, 2, 0, 3), (0, 5, 1, 3), (1, 4, 1, 3, 0, 3), (1, 4, 1, 2, 0, 2),
            (1, 4, 1, 3, 0, 2), (0, 4, 1, 0, 1, 0),
        ),
        (
            (1, 4, 1, 2, 0, 1), (1, 4, 1, 3, 0, 1), (0, 4, 1, 1, 1, 0),
        ),
        (
            (0, 4, 1, 2, 1, 0),
        ),
        (
            (0, 4, 1, 3, 1, 0),
        ),
        (
        ),
    ),
    (
        (
            (1, 3, 4, 1, 0), (1, 2, 1, 2), (1, 2, 1, 0), (1, 2, 3, 0), (1, 3, 0, 1, 0), (1, 2, 3, 2), (1, 2, 2, 0),
            (1, 3, 0, 1, 1), (1, 2, 0, 0), (1, 3, 1, 1, 0), (1, 3, 2, 1, 0), (1, 3, 1, 1, 1), (1, 2, 0, 2),
            (1, 2, 4, 2),
        ),
        (
            (1, 3, 4, 1, 1), (1, 3, 2, 1, 1), (1, 0, 0, 1, 0, 0), (0, 6, 1, 0), (1, 2, 4, 0), (0, 6, 1, 2),
            (1, 3, 1, 2, 0), (1, 3, 1, 0, 3), (1, 2, 2, 2), (1, 3, 1, 1, 3), (0, 3, 4, 1, 0), (1, 1, 0, 1, 0, 0),
            (1, 3, 3, 1, 0), (1, 0, 0, 1, 1, 0), (0, 6, 2, 2), (1, 3, 2, 2, 1), (1, 3, 2, 2, 3), (1, 0, 0, 0, 1, 0),
            (1, 0, 0, 0, 0, 0), (1, 3, 2, 2, 2), (1, 3, 2, 2, 0), (1, 3, 1, 2, 1), (1, 3, 1, 0, 1), (0, 3, 0, 1, 1),
            (1, 3, 0, 1, 5), (0, 6, 0, 2), (1, 3, 0, 2, 0), (1, 3, 0, 2, 2), (1, 3, 0, 1, 3), (1, 2, 3, 3),
            (1, 3, 1, 0, 0), (1, 3, 3, 1, 1), (1, 3, 4, 1, 3), (0, 0, 0, 1, 0, 1), (1, 1, 0, 0, 0, 0),
            (1, 3, 1, 2, 3), (1, 0, 0, 1, 0, 1), (1, 2, 7, 0), (0, 3, 2, 1, 1), (1, 3, 0, 2, 1), (1, 3, 1, 0, 2),
            (1, 3, 4, 1, 4), (1, 1, 0, 1, 0, 1), (0, 0, 0, 0, 0, 1), (1, 0, 0, 0, 0, 1), (0, 3, 2, 1, 0),
            (1, 3, 2, 1, 5), (0, 3, 1, 1, 1), (1, 3, 1, 1, 5), (0, 3, 2, 2, 0), (1, 2, 6, 0), (1, 3, 0, 1, 2),
            (1, 2, 2, 3), (0, 3, 1, 2, 1), (1, 3, 0, 2, 3), (1, 3, 2, 2, 4), (1, 2, 5, 0), (0, 3, 1, 2, 0),
            (0, 0, 0, 1, 1, 1), (1, 0, 0, 1, 1, 1), (0, 3, 1, 1, 0), (1, 3, 1, 1, 4), (0, 6, 0, 0), (1, 3, 0, 0, 0),
            (0, 3, 1, 0, 0), (1, 3, 0, 0, 3), (0, 6, 1, 3), (1, 3, 1, 3, 1), (0, 6, 2, 0), (1, 3, 2, 0, 0),
            (1, 3, 1, 2, 5), (1, 3, 1, 3, 0), (1, 3, 0, 0, 2), (0, 3, 2, 2, 1), (1, 3, 2, 2, 5), (0, 3, 0, 2, 0),
            (1, 3, 0, 2, 4), (0, 3, 0, 1, 0), (0, 3, 3, 1, 1), (0, 3, 0, 2, 1), (1, 3, 1, 2, 4), (1, 3, 1, 2, 2),
            (1, 3, 0, 1, 4), (1, 3, 1, 3, 2), (1, 1, 0, 0, 0, 1), (1, 2, 1, 3), (0, 3, 0, 0, 0), (1, 2, 0, 3),
            (1, 3, 2, 0, 1), (1, 2, 4, 3), (0, 0, 0, 1, 1, 2), (1, 1, 0, 1, 1, 2), (0, 0, 0, 0, 1, 1),
            (0, 0, 0, 0, 1, 2), (1, 3, 2, 1, 3), (1, 3, 3, 1, 2), (1, 1, 0, 0, 1, 2), (1, 1, 0, 0, 1, 1),
            (1, 0, 0, 0, 1, 2), (1, 3, 0, 0, 1), (0, 3, 3, 1, 0), (1, 3, 0, 2, 5), (0, 3, 2, 0, 0), (0, 6, 0, 3),
            (1, 3, 0, 3, 3), (0, 3, 1, 3, 0), (1, 0, 0, 1, 1, 2), (1, 3, 0, 3, 0), (1, 3, 0, 3, 1), (1, 3, 0, 3, 2),
            (0, 3, 1, 0, 1), (1, 1, 0, 1, 1, 1), (0, 3, 0, 0, 1), (1, 3, 1, 0, 5), (1, 3, 1, 0, 4), (1, 2, 6, 2),
            (0, 6, 2, 3), (1, 3, 2, 3, 0), (1, 3, 2, 1, 4), (0, 3, 4, 1, 1), (1, 3, 1, 1, 2), (1, 3, 1, 3, 3),
            (1, 3, 2, 1, 2), (1, 3, 4, 1, 2), (0, 3, 2, 0, 1), (1, 3, 0, 0, 4), (1, 0, 0, 0, 1, 1), (1, 3, 2, 3, 1),
            (1, 2, 5, 2), (0, 3, 0, 3, 0), (1, 3, 0, 0, 5), (1, 3, 0, 3, 4), (0, 8, 0, 0), (1, 2, 7, 3), (0, 6, 4, 0),
            (0, 6, 3, 3), (1, 3, 4, 0, 0), (0, 3, 1, 3, 1), (1, 3, 1, 3, 5), (1, 3, 1, 3, 4), (1, 2, 5, 3),
            (0, 3, 2, 3, 0), (1, 3, 5, 1, 0), (1, 3, 5, 1, 1), (0, 3, 0, 3, 1), (1, 3, 0, 3, 5), (1, 3, 4, 0, 2),
            (1, 3, 2, 0, 5), (0, 6, 3, 0), (1, 3, 3, 0, 1), (1, 3, 2, 3, 2), (1, 3, 4, 1, 5), (0, 6, 4, 2),
            (1, 3, 4, 2, 3), (1, 3, 4, 2, 1), (0, 3, 5, 1, 1), (0, 6, 5, 0), (1, 3, 5, 0, 1), (1, 3, 2, 0, 3),
            (1, 3, 3, 1, 3), (0, 7, 0), (1, 3, 3, 0, 0), (1, 3, 2, 0, 2), (1, 3, 2, 0, 4), (0, 3, 2, 3, 1),
            (1, 3, 2, 3, 5), (0, 7, 1), (1, 3, 2, 3, 3),
        ),
        (
            (1, 3, 2, 3, 4),
        ),
        (
            (0, 6, 3, 2), (1, 3, 3, 2, 0), (1, 2, 7, 2), (0, 3, 5, 1, 0), (1, 2, 6, 3),
        ),
        (
        ),
        (
            (0, 7, 2),
        ),
        (
        ),
        (
        ),
        (
            (1, 3, 3, 2, 1), (1, 3, 5, 1, 5), (0, 6, 5, 3), (1, 3, 5, 3, 1), (1, 3, 5, 0, 2), (0, 6, 5, 2),
            (1, 3, 5, 2, 1), (1, 3, 3, 3, 0), (1, 3, 5, 3, 0), (1, 3, 5, 0, 0),
        ),
        (
            (1, 3, 5, 2, 3), (0, 5, 0, 0), (0, 4, 0, 0, 0, 1), (1, 4, 0, 0, 0, 1), (1, 3, 3, 3, 3), (1, 3, 4, 2, 0),
            (0, 3, 3, 0, 1), (0, 4, 0, 0, 0, 2), (1, 4, 0, 0, 0, 2), (1, 3, 3, 3, 1), (0, 5, 0, 3), (0, 3, 4, 0, 0),
            (0, 4, 0, 3, 0, 2), (1, 4, 0, 3, 0, 2), (0, 4, 0, 0, 1, 0), (0, 4, 0, 0, 0, 0),
        ),
        (
            (1, 0, 1, 0, 1, 0), (1, 0, 1, 0, 0, 0), (0, 3, 4, 2, 1), (1, 3, 5, 2, 0), (1, 3, 4, 0, 1), (0, 5, 0, 1),
            (1, 3, 4, 0, 4), (1, 3, 3, 0, 3), (1, 3, 5, 3, 2), (0, 5, 0, 2), (0, 4, 0, 0, 1, 1), (1, 3, 3, 1, 4),
            (1, 3, 3, 1, 5), (1, 4, 0, 0, 1, 1), (0, 4, 0, 1, 0, 2), (1, 4, 0, 1, 0, 2), (0, 3, 3, 0, 0),
            (0, 4, 0, 1, 0, 1), (1, 4, 0, 1, 0, 1), (1, 3, 4, 2, 2), (0, 3, 3, 3, 1), (0, 4, 0, 2, 0, 2),
            (1, 4, 0, 2, 0, 2), (0, 3, 5, 2, 0), (1, 3, 3, 2, 3), (0, 3, 3, 2, 1), (0, 4, 0, 1, 1, 1),
            (1, 4, 0, 1, 1, 1), (1, 3, 3, 2, 5), (1, 3, 3, 0, 2), (1, 3, 5, 1, 3), (0, 4, 0, 3, 0, 1),
            (1, 4, 0, 3, 0, 1), (0, 4, 0, 1, 1, 0), (0, 3, 4, 2, 0), (1, 3, 5, 3, 3), (0, 3, 5, 3, 1),
            (1, 3, 5, 3, 5), (0, 4, 0, 1, 0, 0),
        ),
        (
            (1, 0, 1, 1, 1, 0), (0, 3, 5, 2, 1), (1, 3, 5, 2, 5), (1, 0, 1, 1, 0, 0), (0, 4, 0, 2, 0, 1),
            (1, 4, 0, 2, 0, 1), (0, 4, 0, 2, 1, 1), (1, 4, 0, 2, 1, 1), (1, 3, 4, 0, 3), (0, 4, 0, 3, 1, 1),
            (1, 3, 3, 3, 2), (0, 0, 1, 0, 0, 1), (1, 0, 1, 0, 0, 1), (1, 4, 0, 3, 1, 1), (1, 3, 5, 1, 2),
            (1, 3, 5, 2, 2), (1, 3, 4, 2, 5), (1, 3, 5, 0, 3), (0, 0, 1, 1, 1, 1), (1, 0, 1, 1, 1, 1),
            (0, 3, 5, 0, 0), (1, 3, 5, 0, 4), (1, 3, 3, 0, 4), (0, 0, 1, 0, 1, 1), (1, 1, 1, 0, 1, 1),
            (1, 0, 1, 0, 1, 1), (0, 4, 0, 2, 1, 0), (0, 4, 0, 2, 0, 0),
        ),
        (
            (1, 3, 5, 1, 4), (0, 0, 1, 1, 0, 1), (1, 1, 1, 1, 0, 1), (1, 1, 1, 2, 0, 0), (1, 1, 1, 0, 0, 0),
            (0, 0, 1, 0, 1, 2), (1, 1, 1, 0, 1, 2), (1, 0, 1, 0, 1, 2), (1, 1, 1, 1, 1, 1), (0, 3, 5, 3, 0),
            (1, 3, 5, 3, 4), (1, 0, 1, 1, 0, 1), (1, 0, 1, 2, 0, 0), (0, 4, 0, 3, 1, 0), (0, 4, 0, 3, 0, 0),
        ),
        (
            (1, 1, 1, 3, 0, 0), (1, 3, 4, 2, 4), (0, 3, 4, 0, 1), (0, 3, 3, 2, 0), (1, 3, 3, 0, 5),
            (1, 0, 1, 3, 1, 0), (1, 3, 3, 3, 5), (1, 0, 1, 2, 1, 0), (0, 6, 4, 3), (1, 3, 4, 3, 0), (1, 3, 4, 3, 1),
            (1, 3, 4, 3, 2), (1, 3, 4, 3, 3), (1, 3, 4, 0, 5), (0, 0, 1, 2, 0, 1), (1, 0, 1, 2, 0, 1),
            (1, 3, 3, 2, 4), (1, 0, 1, 3, 0, 0), (0, 3, 3, 3, 0), (0, 0, 1, 1, 1, 2), (1, 0, 1, 1, 1, 2),
            (0, 0, 1, 3, 0, 1), (1, 0, 1, 3, 0, 1), (0, 0, 1, 2, 1, 1), (1, 0, 1, 2, 1, 1), (1, 1, 1, 2, 1, 1),
            (0, 3, 5, 0, 1), (1, 3, 3, 2, 2), (1, 3, 5, 0, 5), (1, 1, 1, 2, 0, 1), (1, 1, 1, 1, 0, 0),
            (1, 1, 1, 3, 0, 1), (1, 3, 3, 3, 4), (1, 3, 5, 2, 4), (1, 1, 1, 1, 1, 2), (0, 0, 1, 2, 1, 2),
            (1, 0, 1, 2, 1, 2), (1, 1, 1, 0, 0, 1), (1, 1, 1, 2, 1, 2), (0, 3, 4, 3, 0), (1, 3, 4, 3, 4),
            (0, 0, 1, 3, 1, 1), (1, 0, 1, 3, 1, 1), (0, 3, 4, 3, 1), (1, 3, 4, 3, 5), (1, 1, 1, 3, 1, 1),
            (0, 0, 1, 3, 1, 2), (1, 0, 1, 3, 1, 2), (1, 1, 1, 3, 1, 2), (0, 7, 4), (0, 7, 3), (0, 8, 1, 0),
        ),
        (
            (0, 7, 5),
        ),
        (
            (0, 8, 1, 1),
        ),
        (
            (0, 5, 1, 0), (0, 4, 1, 0, 0, 2), (0, 8, 1, 2), (1, 4, 1, 0, 0, 2), (0, 4, 1, 0, 0, 1),
            (1, 4, 1, 0, 0, 1),
        ),
        (
        ),
        (
        ),
        (
            (0, 5, 1, 1), (0, 4, 1, 1, 0, 1), (1, 4, 1, 1, 0, 1), (0, 8, 1, 3), (0, 4, 1, 0, 0, 0),
        ),
        (
            (0, 4, 1, 1, 0, 2), (0, 4, 1, 0, 1, 1), (1, 4, 1, 0, 1, 1), (1, 4, 1, 1, 0, 2), (0, 5, 1, 2),
        ),
        (
            (0, 4, 1, 2, 0, 2), (1, 4, 1, 2, 0, 2), (0, 5, 1, 3), (0, 4, 1, 3, 0, 2), (1, 4, 1, 3, 0, 2),
            (0, 4, 1, 1, 1, 1), (1, 4, 1, 1, 1, 1), (0, 4, 1, 2, 0, 1), (1, 4, 1, 2, 0, 1), (0, 4, 1, 2, 1, 1),
            (1, 4, 1, 2, 1, 1), (0, 4, 1, 3, 0, 1), (1, 4, 1, 3, 0, 1), (0, 4, 1, 0, 1, 0),
        ),
        (
            (0, 4, 1, 3, 1, 1), (1, 4, 1, 3, 1, 1), (0, 4, 1, 1, 0, 0), (0, 4, 1, 3, 0, 0), (0, 4, 1, 1, 1, 0),
        ),
        (
            (0, 4, 1, 2, 1, 0), (0, 4, 1, 2, 0, 0),
        ),
        (
            (0, 4, 1, 3, 1, 0),
        ),
        (
        ),
    ),
)

OWN_FIRST = {}
for at, ops in enumerate(PLAN):
    for op in (op for stage in ops for op in stage):
        if op[:2] == (1, HOP) and op[3] == at:
            OWN_FIRST.setdefault((op[2], at), op[4])


def layer_kernel(
    n_fs,
    groups,
    tokens_in,
    norm_gain_in,
    wq,
    wk,
    wv,
    wg,
    mixer_gain_in,
    wo,
    channel_gain_in,
    wl,
    wr,
    taps_left_in,
    taps_right_in,
    wd,
    cos_in,
    sin_in,
    gammas_in,
    out,
    tokens,
    norm_gain,
    mixer_gain,
    channel_gain,
    taps_left,
    taps_right,
    cos_t,
    sin_t,
    gammas,
    w1,
    wout,
    wlr,
    wdown,
    nt,
    nm,
    qkvg,
    hid,
    gated,
    part1,
    part2,
    xb1,
    xb2,
    sb1,
    sb2,
    rb1,
    rb2,
    mid,
    acc,
    both,
    fin,
    w_send,
    w_recv,
    self_sem,
    h_send,
    h_recv,
    h_rest,
    a_send,
    a_recv,
    f_send,
    f_recv,
    x_send,
    x_recv,
    r_send,
    r_recv,
    o_send,
    o_recv,
    load_sem,
    store_sem,
):
    fs, tp = lax.axis_index("fs"), lax.axis_index("tp")
    planes = n_fs // groups
    z, q = fs // planes, lax.rem(fs, planes)
    other = 1 - tp
    length, width = tokens_in.shape
    own = length // 2
    part_rows = own // NT_PARTS
    span_c = length // CHUNKS
    few = span_c // 2
    kb = wq.shape[0]
    nb = wo.shape[1]
    cq, cv, cf = wq.shape[1] // groups, wv.shape[1] // groups, wl.shape[1] // groups
    upper = z * 2 >= groups
    place_z = jnp.where(upper, groups - 1 - z, z)

    def real(plane):
        return jnp.where(upper, groups - 1 - plane, plane)

    def flip(side):
        return jnp.where(upper, 1 - side, side)

    def zdev(target):
        return {"fs": target * planes + q, "tp": tp}

    partner = {"fs": fs, "tp": other}

    def lanes(index, size):
        return pl.ds(pl.multiple_of(index * size, 128), size)

    def rows(index, size):
        return pl.ds(pl.multiple_of(index * size, size), size)

    pieces = (
        (lambda c: wq.at[:, lanes(c, cq)], lambda f: w1.at[rows(f, kb), pl.ds(0, cq)]),
        (lambda c: wk.at[:, lanes(c, cq)], lambda f: w1.at[rows(f, kb), pl.ds(cq, cq)]),
        (lambda c: wv.at[:, lanes(c, cv)], lambda f: w1.at[rows(f, kb), pl.ds(2 * cq, cv)]),
        (lambda c: wg.at[:, lanes(c, cv)], lambda f: w1.at[rows(f, kb), pl.ds(2 * cq + cv, cv)]),
        (lambda c: wo.at[rows(c, cv), :], lambda f: wout.at[:, lanes(f, nb)]),
        (lambda c: wl.at[:, lanes(c, cf)], lambda f: wlr.at[rows(f, kb), pl.ds(0, cf)]),
        (lambda c: wr.at[:, lanes(c, cf)], lambda f: wlr.at[rows(f, kb), pl.ds(cf, cf)]),
        (lambda c: wd.at[rows(c, cf), :], lambda f: wdown.at[:, lanes(f, nb)]),
    )
    starts = (0, cq, 2 * cq, 2 * cq + cv, 0, 0, cf, 0)
    widths = (cq, cq, cv, cv, 0, cf, cf, 0)

    def stretch(cls, first, count, half=None):
        members = [i for i in range(len(pieces)) if CLASS_OF[i] == cls]
        low = starts[members[0]]
        wide = sum(widths[i] for i in members)
        if members[0] == 4 or members[0] == 7:
            buf, size = (wout, cv) if members[0] == 4 else (wdown, cf)
            across = pl.ds(pl.multiple_of(first * nb, 128), count * nb)
            if half is None:
                return buf.at[:, across]
            return buf.at[pl.ds(half * (size // 2), size // 2), across]
        buf = w1 if members[0] < 4 else wlr
        if half is None:
            return buf.at[pl.ds(pl.multiple_of(first * kb, kb), count * kb), pl.ds(low, wide)]
        start = pl.multiple_of(first * kb + half * (kb // 2), kb // 2)
        return buf.at[pl.ds(start, kb // 2), pl.ds(low, wide)]

    barrier = pltpu.get_barrier_semaphore()
    for step in range(1, groups):
        pl.semaphore_signal(barrier, inc=1, device_id=zdev(lax.rem(z + step, groups)), device_id_type=MESH)
    qx = q + 1 - 2 * lax.rem(q, 2)
    qy = q + 2 - 4 * (q // 2)
    diagonal = planes - 1 - q
    to_x = {"fs": z * planes + qx, "tp": tp}
    to_y = {"fs": z * planes + qy, "tp": tp}
    for device in (to_x, to_y):
        pl.semaphore_signal(barrier, inc=1, device_id=device, device_id_type=MESH)
    pl.semaphore_signal(barrier, inc=1, device_id=partner, device_id_type=MESH)

    loads = []
    for i, (source, held_here) in enumerate((
        (tokens_in, tokens), (norm_gain_in, norm_gain), (mixer_gain_in, mixer_gain),
        (channel_gain_in, channel_gain), (taps_left_in, taps_left), (taps_right_in, taps_right),
        (cos_in, cos_t), (sin_in, sin_t), (gammas_in, gammas),
    )):
        load = pltpu.make_async_copy(source, held_here, load_sem.at[i])
        load.start()
        loads.append(load)
    keeps = []
    for i, (src, dst) in enumerate(pieces):
        keep = pltpu.make_async_copy(src(z), dst(fs), self_sem.at[i])
        keep.start()
        keeps.append(keep)

    def prepare(_):
        for load in loads:
            load.wait()
        my_half = pl.ds(pl.multiple_of(tp * own, own), own)
        nt[pl.ds(pl.multiple_of(z * length + tp * own, own), own), :] = normed_rows(
            tokens[my_half, :].astype(jnp.float32), norm_gain[...]
        )

    pl.semaphore_wait(barrier, groups - 1 + 2 + 1)

    def remote(src, dst, ssem, rsem, device):
        return pltpu.make_async_remote_copy(
            src_ref=src, dst_ref=dst, send_sem=ssem, recv_sem=rsem,
            device_id=device, device_id_type=MESH,
        )

    def block(key, c, seq, core):
        if key:
            first = c * groups * span_c + seq * span_c + core * few
            return nm.at[pl.ds(pl.multiple_of(first, few), few), :]
        first = seq * length + core * own + c * part_rows
        return nt.at[pl.ds(pl.multiple_of(first, part_rows), part_rows), :]

    part, xb, sb, rb = (part1, part2), (xb1, xb2), (sb1, sb2), (rb1, rb2)

    def pair(which, c, g):
        return part[which][c, tp, g].astype(jnp.float32) + xb[which][c, g].astype(jnp.float32)

    def exchange(which, c):
        return remote(part[which].at[c, other], xb[which].at[c], x_send.at[which], x_recv.at[which, c], partner)

    def gather_copy(me, key, c, side, d, landing=False):
        move = 1 - 2 * side
        source = real(me - move * d)
        ref = block(key, c, source, tp)
        at = c + key * NT_PARTS
        device = partner if landing else zdev(real(me + move))
        return remote(ref, ref, a_send.at[key], a_recv.at[at, source], device)

    def core_copy(me, key, c, side, d):
        move = 1 - 2 * side
        ref = block(key, c, real(me - move * d), tp)
        return remote(ref, ref, f_send.at[key], f_recv.at[key * (1 + c)], partner)

    def weight_copy(me, i, plane):
        src, dst = pieces[i]
        far = real(plane)
        return remote(src(far), dst(fs), w_send.at[i], w_recv.at[CLASS_OF[i], z], zdev(far))

    def hop_copy(me, cls, plane, slot, landing=False):
        origin = (qx, qy)[slot] if landing else (q, q, q, q, qx, qy)[slot]
        source = real(plane)
        ref = stretch(cls, source * planes + origin, 1, (0, 1, 1, 0, 0, 1)[slot])
        device = (to_x, to_y, to_x, to_y, to_y, to_x)[slot]
        landed = h_recv.at[cls, source, slot] if slot < 2 else h_rest.at[cls]
        return remote(ref, ref, h_send.at[cls], landed, device)

    def sum_copy(me, which, c, side, d, landing=False):
        ref = sb[which].at[c, flip(side), d]
        at = d if landing else d - 1
        device = partner if landing else zdev(real(me + 1 - 2 * side))
        return remote(ref, rb[which].at[c, flip(side), at], r_send.at[which], r_recv.at[which, c, flip(side), at], device)

    makers = (gather_copy, core_copy, weight_copy, hop_copy, sum_copy)

    def await_bytes(ref, sem):
        remote(ref, ref, sem, sem, partner).wait_recv()

    def act(me, op):
        sends, kind, args = op[0], op[1], op[2:]
        if not sends:
            if kind == SWAP:
                exchange(*args).wait_recv()
            elif kind == WEIGHTS:
                cls, far = args[0], real(args[1])
                await_bytes(stretch(cls, far * planes + q, 1), w_recv.at[cls, far])
            elif kind == HOPS:
                await_bytes(stretch(args[0], 0, 2 * groups), h_rest.at[args[0]])
            elif kind == CORES:
                key, c = args
                if key:
                    await_bytes(nm.at[pl.ds(0, groups * few), :], f_recv.at[1 + c])
                else:
                    await_bytes(nt.at[pl.ds(0, groups * own), :], f_recv.at[0])
            else:
                makers[kind](me, *args, True).wait_recv()
            return
        if kind == HOP and args[1] == me and args[2] == OWN_FIRST[args[0], me]:
            for i, keep in enumerate(keeps):
                if CLASS_OF[i] == args[0]:
                    keep.wait()
        if kind == SUM:
            which, c, side, d = args
            move = 1 - 2 * side
            value = pair(which, c, real(me + move * d))
            if 0 <= me - move < groups:
                value = value + rb[which][c, flip(side), d].astype(jnp.float32)
            sb[which][c, flip(side), d] = value.astype(jnp.bfloat16)
        makers[kind](me, *args).start()

    def perform(stage):
        for me, ops in enumerate(PLAN):
            @pl.when(place_z == me)
            def _():
                for op in ops[stage]:
                    act(me, op)

    def multiply(left, weight, which, c):
        value = jnp.dot(
            left[rows(c, groups * span_c), :], weight[...], preferred_element_type=jnp.float32
        ).astype(jnp.bfloat16)
        for g in range(groups):
            part[which][c, 0, g] = value[g * span_c : g * span_c + few]
            part[which][c, 1, g] = value[g * span_c + few : (g + 1) * span_c]
        exchange(which, c).start()

    def collect(which, c):
        acc[c] = pair(which, c, z)
        for side, has in ((0, z > 0), (1, z < groups - 1)):
            @pl.when(has)
            def _():
                acc[c] = acc[c] + rb[which][c, side, 0].astype(jnp.float32)
        return acc[c]

    def natural(c, core):
        return pl.ds(pl.multiple_of(c * span_c + core * few, few), few)

    head = tp * groups + z
    chunk = groups * length // 2

    def project(at):
        span = rows(at, chunk)
        qkvg[span, :] = jnp.dot(
            nt[span, :], w1[...], preferred_element_type=jnp.float32
        ).astype(jnp.bfloat16)

    def retain(first):
        log_gamma = gammas[pl.ds(head, 1), :]
        distance = (
            lax.broadcasted_iota(jnp.int32, (length, length), 0)
            - lax.broadcasted_iota(jnp.int32, (length, length), 1)
        ).astype(jnp.float32)
        decay = jnp.where(distance >= 0, jnp.exp(log_gamma * jnp.maximum(distance, 0.0)), 0.0)

        @pl.loop(first * groups // 2, (first + 1) * groups // 2)
        def _(at):
            span = rows(at, length)
            held = qkvg[span, :].astype(jnp.float32)

            def turn(x):
                return x * cos_t[...] + pltpu.roll(x, cq // 2, 1) * sin_t[...]

            rq = turn(held[:, :cq])
            rk = turn(held[:, cq : 2 * cq])
            scores = lax.dot_general(
                rq, rk, (((1,), (1,)), ((), ())), precision=highest, preferred_element_type=jnp.float32
            ) * decay
            kept = jnp.dot(
                scores, held[:, 2 * cq : 2 * cq + cv], precision=highest,
                preferred_element_type=jnp.float32,
            )
            kept = kept * lax.rsqrt(jnp.mean(kept * kept, axis=-1, keepdims=True) + 1e-06)
            gain = mixer_gain[:, lanes(z, cv)]
            whole = (kept * gain * silu(held[:, 2 * cq + cv :])).astype(jnp.bfloat16)
            for c in range(CHUNKS):
                hid[rows(at + c * groups, span_c), :] = whole[c * span_c : (c + 1) * span_c]

    def renorm(c):
        middle = (
            tokens[natural(c, tp), :].astype(jnp.float32) + collect(0, c)
        ).astype(jnp.bfloat16).astype(jnp.float32)
        mid[c] = middle
        first = c * groups * span_c + z * span_c + tp * few
        nm[pl.ds(pl.multiple_of(first, few), few), :] = normed_rows(middle, channel_gain[...])

    place = lax.rem(lax.broadcasted_iota(jnp.int32, (groups * span_c, 1), 0), span_c)

    def convolve(c, low, taps):
        x = both[c, :, low : low + cf].astype(jnp.float32)
        count = taps.shape[0]
        weights = taps[:, lanes(z, cf)]
        result = x * weights[count - 1 :, :]
        for back in range(1, count):
            if c:
                before = both[c - 1, :, low : low + cf].astype(jnp.float32)
                before = pltpu.roll(before, back + (groups - 1) * span_c, 0)
            else:
                before = 0.0
            moved = jnp.where(place >= back, pltpu.roll(x, back, 0), before)
            result = result + moved * weights[count - 1 - back : count - back, :]
        return result

    def mix(c):
        both[c] = jnp.dot(
            nm[rows(c, groups * span_c), :], wlr[...], preferred_element_type=jnp.float32
        ).astype(jnp.bfloat16)
        gated[rows(c, groups * span_c), :] = (
            silu(convolve(c, 0, taps_left)) * convolve(c, cf, taps_right)
        ).astype(jnp.bfloat16)

    def finish(c):
        mine = natural(c, tp)
        fin[c] = (mid[c] + collect(1, c)).astype(jnp.bfloat16)
        remote(fin.at[c], out.at[mine, :], o_send.at[0], o_recv.at[0], partner).start()
        pltpu.make_async_copy(fin.at[c], out.at[mine, :], store_sem.at[0]).start()

    steps = (
        project,
        retain,
        lambda c: multiply(hid, wout, 0, c),
        renorm,
        mix,
        lambda c: multiply(gated, wdown, 1, c),
        finish,
        prepare,
    )
    perform(0)
    for stage, (name, index) in enumerate(STAGES):
        steps[name](index)
        perform(stage + 1)
    await_bytes(fin, o_recv.at[0])
    await_bytes(fin, o_send.at[0])
    for key, buf in ((0, nt), (1, nm)):
        await_bytes(buf.at[pl.ds(0, groups * own), :], f_send.at[key])
        await_bytes(part[key].at[:, 0], x_send.at[key])
        await_bytes(sb[key].at[:, 0, pl.ds(0, groups - 1)], r_send.at[key])
    for cls in range(max(CLASS_OF) + 1):
        await_bytes(stretch(cls, 0, 3 * groups), h_send.at[cls])
    for i, (_, dst) in enumerate(pieces):
        if i == 4 or i == 7:
            ref = (wout if i == 4 else wdown).at[:, pl.ds(0, (groups - 1) * nb)]
        else:
            ref = (w1 if i < 4 else wlr).at[pl.ds(0, (groups - 1) * kb), pl.ds(starts[i], widths[i])]
        await_bytes(ref, w_send.at[i])
    for me, ops in enumerate(PLAN):
        @pl.when(place_z == me)
        def _():
            for key, buf, size in ((0, nt, part_rows), (1, nm, few)):
                count = sum(op[:3] == (1, 0, key) for stage in ops for op in stage)
                await_bytes(buf.at[pl.ds(0, count * size), :], a_send.at[key])
    pltpu.make_async_copy(fin, fin, store_sem.at[0]).wait()


def body(n_fs, *args):
    (tokens, norm_gain, w_query, w_key, w_value, w_gate, mixer_gain, w_out, channel_gain,
     w_left, w_right, taps_left, taps_right, w_down) = args
    groups = w_query.shape[1] // DK
    if (
        groups != 2 * len(PLAN)
        or n_fs % groups
        or n_fs != 4 * groups
        or lax.axis_size("tp") != 2
        or tokens.shape[0] != BLOCK
        or (w_left.shape[1] // groups) % 128
        or w_left.shape[1] % groups
        or w_out.shape[1] % 128
        or w_query.shape[0] % 32
        or tokens.shape[0] % (32 * CHUNKS)
    ):
        return plain_body(*args)
    length, width = tokens.shape
    heads = groups * lax.axis_size("tp")
    cq, cv, cf = w_query.shape[1] // groups, w_value.shape[1] // groups, w_left.shape[1] // groups
    planes = n_fs // groups
    span_c = length // CHUNKS
    few = span_c // 2
    classes = max(CLASS_OF) + 1
    cos_t, sin_t = turning(length, DK)
    gammas = log_gammas(heads)
    held = pl.BlockSpec(memory_space=pl.ANY)
    bf, f32, dma = jnp.bfloat16, jnp.float32, pltpu.SemaphoreType.DMA
    return pl.pallas_call(
        functools.partial(layer_kernel, n_fs, groups),
        out_shape=jax.ShapeDtypeStruct(tokens.shape, bf),
        in_specs=[held] * 17,
        out_specs=held,
        scratch_shapes=[
            pltpu.VMEM(tokens.shape, bf),
            pltpu.VMEM((1, width), f32),
            pltpu.VMEM((1, w_value.shape[1]), f32),
            pltpu.VMEM((1, width), f32),
            pltpu.VMEM(taps_left.shape, f32),
            pltpu.VMEM(taps_right.shape, f32),
            pltpu.VMEM(cos_t.shape, f32),
            pltpu.VMEM(sin_t.shape, f32),
            pltpu.VMEM(gammas.shape, f32),
            pltpu.VMEM((width, 2 * cq + 2 * cv), bf),
            pltpu.VMEM((cv, width), bf),
            pltpu.VMEM((width, 2 * cf), bf),
            pltpu.VMEM((cf, width), bf),
            pltpu.VMEM((groups * length, width), bf),
            pltpu.VMEM((groups * length, width), bf),
            pltpu.VMEM((groups * length, 2 * cq + 2 * cv), bf),
            pltpu.VMEM((groups * length, cv), bf),
            pltpu.VMEM((groups * length, cf), bf),
            pltpu.VMEM((CHUNKS, 2, groups, few, width), bf),
            pltpu.VMEM((CHUNKS, 2, groups, few, width), bf),
            pltpu.VMEM((CHUNKS, groups, few, width), bf),
            pltpu.VMEM((CHUNKS, groups, few, width), bf),
            pltpu.VMEM((CHUNKS, 2, groups, few, width), bf),
            pltpu.VMEM((CHUNKS, 2, groups, few, width), bf),
            pltpu.VMEM((CHUNKS, 2, groups, few, width), bf),
            pltpu.VMEM((CHUNKS, 2, groups, few, width), bf),
            pltpu.VMEM((CHUNKS, few, width), f32),
            pltpu.VMEM((CHUNKS, few, width), f32),
            pltpu.VMEM((CHUNKS, groups * span_c, 2 * cf), bf),
            pltpu.VMEM((CHUNKS, few, width), bf),
            dma((8,)),
            dma((classes, groups)),
            dma((8,)),
            dma((classes,)),
            dma((classes, groups, 2)),
            dma((classes,)),
            dma((2,)),
            dma((NT_PARTS + CHUNKS, groups)),
            dma((2,)),
            dma((1 + CHUNKS,)),
            dma((2,)),
            dma((2, CHUNKS)),
            dma((2,)),
            dma((2, CHUNKS, 2, groups - 1)),
            dma((1,)),
            dma((1,)),
            dma((9,)),
            dma((1,)),
        ],
        compiler_params=pltpu.CompilerParams(
            collective_id=0, has_side_effects=True, vmem_limit_bytes=60 * 1024 * 1024
        ),
    )(
        tokens, norm_gain[None], w_query, w_key, w_value, w_gate, mixer_gain[None], w_out,
        channel_gain[None], w_left, w_right, taps_left, taps_right, w_down,
        cos_t, sin_t, gammas,
    )


def solution(mesh):
    placed = (
        P("fs", None),
        P(),
        P("fs", "tp"),
        P("fs", "tp"),
        P("fs", "tp"),
        P("fs", "tp"),
        P("tp"),
        P("tp", "fs"),
        P(),
        P("fs", "tp"),
        P("fs", "tp"),
        P(None, "tp"),
        P(None, "tp"),
        P("tp", "fs"),
    )
    return jax.shard_map(
        functools.partial(body, mesh.shape["fs"]), mesh=mesh, in_specs=placed, out_specs=P("fs", None), check_vma=False)
```

```python
import functools

import jax
import jax.numpy as jnp
import numpy as np
from jax import lax
from jax.experimental import pallas as pl
from jax.experimental.pallas import tpu as pltpu
from jax.sharding import PartitionSpec as P

DK = 128
DV = 256
BLOCK = 128
MESH = pl.DeviceIdType.MESH


highest = lax.Precision.HIGHEST


def scale_rows(rows_in, gain_vec):
    floats = rows_in.astype(jnp.float32)
    factor = lax.rsqrt(jnp.mean(floats * floats, axis=-1, keepdims=True) + 1e-06)
    return (floats * factor * gain_vec).astype(jnp.bfloat16)


def decays(first_head, count):
    head_ids = first_head + jnp.arange(count, dtype=jnp.float32)
    return jnp.log(1.0 - 2.0 ** (-5.0 - head_ids))


def rotate(heads_in, positions):
    width = heads_in.shape[-1]
    half = width // 2
    freqs = 10000.0 ** (-jnp.arange(half, dtype=jnp.float32) / half)
    angles = positions[:, None] * freqs[None, :]
    cosine = jnp.cos(angles)
    sine = jnp.sin(angles)
    first_half = heads_in[..., :half]
    second_half = heads_in[..., half:]
    return jnp.concatenate(
        [first_half * cosine - second_half * sine, first_half * sine + second_half * cosine],
        axis=-1,
    )


def retention(queries, keys_in, values_in, log_gamma):
    head_count, length, key_width = queries.shape
    value_width = values_in.shape[-1]
    blocks = length // BLOCK
    queries = queries.reshape(head_count, blocks, BLOCK, key_width)
    keys_in = keys_in.reshape(head_count, blocks, BLOCK, key_width)
    values_in = values_in.reshape(head_count, blocks, BLOCK, value_width)
    offsets = jnp.arange(BLOCK, dtype=jnp.float32)
    distance = offsets[:, None] - offsets[None, :]
    weights = jnp.where(
        distance >= 0, jnp.exp(log_gamma[:, None, None] * jnp.maximum(distance, 0.0)), 0.0
    )
    scores = jnp.einsum("hbnd,hbmd->hbnm", queries, keys_in, precision=highest) * weights[:, None]
    inner = jnp.einsum("hbnm,hbme->hbne", scores, values_in, precision=highest)
    key_weight = jnp.exp(log_gamma[:, None] * (BLOCK - 1 - offsets)[None, :])
    contrib = jnp.einsum(
        "hbjd,hbje->hbde", keys_in * key_weight[:, None, :, None], values_in, precision=highest
    )
    block_decay = jnp.exp(log_gamma * BLOCK)[:, None, None]

    def advance(state, contrib_block):
        return (state * block_decay + contrib_block, state)

    _, states = lax.scan(
        advance,
        jnp.zeros((head_count, key_width, value_width), jnp.float32),
        jnp.moveaxis(contrib, 1, 0),
    )
    states = jnp.moveaxis(states, 0, 1)
    query_weight = jnp.exp(log_gamma[:, None] * (offsets + 1.0)[None, :])
    carried = (
        jnp.einsum("hbnd,hbde->hbne", queries, states, precision=highest)
        * query_weight[:, None, :, None]
    )
    return (inner + carried).reshape(head_count, length, value_width)


def head_norm(retained):
    return retained * lax.rsqrt(jnp.mean(retained * retained, axis=-1, keepdims=True) + 1e-06)


def causal_taps(values_in, taps):
    length = values_in.shape[-2]
    padded = jnp.pad(values_in.astype(jnp.float32), ((taps.shape[0] - 1, 0), (0, 0)))
    result = padded[0:length] * taps[0]
    for tap_index in range(1, taps.shape[0]):
        result = result + padded[tap_index : tap_index + length] * taps[tap_index]
    return result


def fold_single(source, weight_piece):
    return jnp.dot(source, weight_piece, preferred_element_type=jnp.float32)


def collect_single(source, weight):
    return fold_single(source, lax.all_gather(weight, "fs", axis=0, tiled=True))


def plain_body(
    tokens,
    norm_gain,
    w_query,
    w_key,
    w_value,
    w_gate,
    mixer_gain,
    w_out,
    channel_gain,
    w_left,
    w_right,
    taps_left,
    taps_right,
    w_down,
):
    length = tokens.shape[0]
    normed = scale_rows(tokens, norm_gain)
    queries = collect_single(normed, w_query)
    keys_proj = collect_single(normed, w_key)
    values_proj = collect_single(normed, w_value)
    gates = collect_single(normed, w_gate)
    queries = queries.astype(jnp.bfloat16)
    keys_proj = keys_proj.astype(jnp.bfloat16)
    values_proj = values_proj.astype(jnp.bfloat16)
    gates = gates.astype(jnp.bfloat16)
    heads_here = w_query.shape[1] // DK
    first_head = (lax.axis_index("tp") * heads_here).astype(jnp.float32)
    log_gamma = decays(first_head, heads_here)
    positions = jnp.arange(length, dtype=jnp.float32)

    def split_heads(rows_in, width):
        return rows_in.astype(jnp.float32).reshape(length, heads_here, width).transpose(1, 0, 2)

    retained = head_norm(
        retention(
            rotate(split_heads(queries, DK), positions),
            rotate(split_heads(keys_proj, DK), positions),
            split_heads(values_proj, DV),
            log_gamma,
        )
    )
    retained = retained.transpose(1, 0, 2).reshape(length, heads_here * DV)
    hidden = (retained * mixer_gain * jax.nn.silu(gates.astype(jnp.float32))).astype(jnp.bfloat16)
    rows_own = length // lax.axis_size("tp")
    first_row = lax.axis_index("tp") * rows_own
    out_whole = lax.all_gather(w_out, "fs", axis=1, tiled=True)
    mixer_total = lax.psum_scatter(
        jnp.dot(hidden, out_whole, preferred_element_type=jnp.float32).astype(jnp.bfloat16),
        "tp",
        scatter_dimension=0,
        tiled=True,
    ).astype(jnp.float32)
    residual = lax.dynamic_slice_in_dim(tokens, first_row, rows_own, 0)
    middle_own = (residual.astype(jnp.float32) + mixer_total).astype(jnp.bfloat16)
    middle = lax.all_gather(middle_own, "tp", axis=0, tiled=True)
    normed_mid = scale_rows(middle, channel_gain)
    left = collect_single(normed_mid, w_left)
    right = collect_single(normed_mid, w_right)
    left = left.astype(jnp.bfloat16)
    right = right.astype(jnp.bfloat16)
    gated = (jax.nn.silu(causal_taps(left, taps_left)) * causal_taps(right, taps_right)).astype(
        jnp.bfloat16
    )
    down_whole = lax.all_gather(w_down, "fs", axis=1, tiled=True)
    channel_part = jnp.dot(gated, down_whole, preferred_element_type=jnp.float32)
    channel_total = lax.psum(channel_part.astype(jnp.bfloat16), "tp").astype(jnp.float32)
    return (middle.astype(jnp.float32) + channel_total).astype(jnp.bfloat16)


def log_gammas(head_count):
    table = np.log(1.0 - 2.0 ** (-5.0 - np.arange(head_count, dtype=np.float64)))
    return np.repeat(table[:, None], BLOCK, axis=1).astype(np.float32)


def turning(length, width):
    half = width // 2
    freqs = np.float32(10000.0) ** (-np.arange(half, dtype=np.float32) / np.float32(half))
    angles = (np.arange(length, dtype=np.float32)[:, None] * freqs[None, :]).astype(np.float64)
    cosine, sine = np.cos(angles), np.sin(angles)
    return (
        np.concatenate([cosine, cosine], axis=1).astype(np.float32),
        np.concatenate([-sine, sine], axis=1).astype(np.float32),
    )


def silu(v):
    return v / (1.0 + jnp.exp(-v))


def normed_rows(floats, gain):
    factor = lax.rsqrt(jnp.mean(floats * floats, axis=-1, keepdims=True) + 1e-06)
    return (floats * factor * gain).astype(jnp.bfloat16)


HOP, SUM, SWAP, WEIGHTS, HOPS, CORES = 3, 4, 5, 6, 7, 8
CHUNKS = 4
NT_PARTS = 2
CLASS_OF = (0, 0, 0, 1, 2, 3, 4, 5)
STAGES = (
    (7, 0),
    (0, 0),
    (0, 1),
    (1, 0),
    (1, 1),
    (8, 0),
    (8, 1),
    (2, 0),
    (2, 1),
    (2, 2),
    (2, 3),
    (3, 0),
    (3, 1),
    (3, 2),
    (3, 3),
    (4, 0),
    (5, 0),
    (4, 1),
    (5, 1),
    (4, 2),
    (5, 2),
    (4, 3),
    (5, 3),
    (6, 0),
    (6, 1),
    (6, 2),
    (6, 3),
)
PLAN = (
    (
        (
            (1, 2, 1, 3), (1, 2, 2, 3), (1, 2, 0, 3), (1, 2, 3, 3), (1, 3, 3, 0, 0), (1, 3, 3, 0, 3), (1, 3, 0, 0, 0),
            (1, 3, 2, 0, 0), (1, 3, 2, 0, 1), (1, 3, 4, 0, 0), (0, 6, 1, 1), (1, 3, 1, 1, 3), (1, 3, 1, 1, 1),
            (1, 3, 0, 0, 2), (1, 2, 3, 1),
        ),
        (
            (1, 0, 0, 1, 0, 0), (1, 1, 0, 0, 0, 0), (1, 1, 0, 1, 0, 0), (1, 3, 5, 0, 0), (1, 2, 1, 1), (0, 6, 0, 3),
            (1, 3, 0, 3, 1), (1, 3, 0, 3, 0), (1, 3, 0, 3, 2), (1, 3, 2, 0, 2), (1, 3, 2, 0, 3), (1, 0, 0, 0, 0, 0),
            (1, 3, 0, 0, 1), (0, 6, 2, 1), (1, 3, 2, 1, 1), (1, 3, 0, 3, 3), (0, 3, 1, 1, 1), (0, 3, 2, 0, 1),
            (0, 6, 1, 3), (1, 2, 0, 1), (1, 3, 1, 3, 1), (0, 3, 3, 0, 0), (0, 6, 0, 1), (1, 3, 0, 1, 1),
            (1, 3, 3, 0, 4), (1, 3, 2, 1, 0), (1, 3, 1, 3, 0), (1, 3, 0, 1, 3), (1, 3, 1, 1, 0), (1, 3, 4, 0, 1),
            (1, 3, 2, 1, 2), (0, 3, 0, 3, 1), (1, 3, 0, 3, 5), (1, 3, 0, 1, 0), (0, 3, 2, 0, 0), (1, 2, 4, 3),
            (0, 3, 1, 3, 1), (1, 2, 2, 1), (1, 2, 4, 1), (1, 3, 1, 0, 0), (1, 2, 5, 1), (1, 3, 1, 1, 5),
            (0, 3, 0, 0, 1), (1, 3, 2, 1, 3), (1, 3, 0, 0, 3), (0, 6, 1, 2), (1, 3, 1, 2, 2), (1, 3, 1, 0, 3),
            (1, 3, 1, 0, 1), (0, 3, 0, 0, 0), (1, 3, 1, 2, 0), (0, 3, 2, 1, 0), (1, 3, 2, 1, 4), (1, 3, 1, 2, 3),
            (1, 3, 1, 2, 1), (1, 3, 5, 0, 3), (1, 2, 3, 2), (1, 3, 0, 1, 2), (1, 3, 1, 3, 2), (0, 6, 4, 1),
            (0, 6, 2, 3), (1, 3, 2, 3, 3), (1, 3, 2, 3, 1), (1, 3, 2, 3, 0), (1, 3, 0, 0, 5), (0, 0, 0, 0, 1, 1),
            (0, 3, 1, 1, 0), (1, 3, 2, 3, 2), (1, 3, 4, 1, 2), (0, 6, 3, 1), (1, 3, 3, 1, 2), (1, 3, 2, 0, 4),
            (1, 3, 5, 0, 2), (1, 2, 1, 2), (1, 2, 0, 2), (1, 3, 1, 3, 3), (0, 3, 0, 3, 0), (1, 3, 4, 1, 3),
            (1, 3, 0, 3, 4), (1, 3, 4, 1, 0), (1, 3, 0, 0, 4), (1, 2, 2, 2), (1, 3, 1, 0, 2), (1, 3, 1, 3, 5),
            (1, 2, 4, 2), (0, 6, 0, 2), (1, 3, 0, 2, 1), (1, 3, 0, 2, 0), (1, 3, 0, 2, 3), (0, 3, 0, 1, 0),
            (1, 3, 2, 0, 5), (1, 3, 0, 1, 4), (0, 3, 1, 2, 1), (1, 3, 1, 2, 5), (1, 2, 5, 2), (1, 3, 0, 2, 2),
            (0, 6, 2, 2), (1, 3, 2, 2, 1), (1, 2, 7, 1), (1, 2, 6, 1), (0, 0, 0, 0, 1, 2), (1, 1, 0, 0, 1, 2),
            (1, 1, 0, 0, 1, 1), (1, 3, 2, 2, 3), (1, 3, 2, 2, 0), (0, 3, 0, 1, 1), (1, 3, 0, 1, 5), (0, 3, 0, 2, 1),
            (0, 3, 0, 2, 0), (1, 3, 0, 2, 4), (1, 3, 0, 2, 5), (0, 3, 1, 3, 0), (1, 3, 1, 3, 4), (0, 0, 0, 0, 1, 3),
            (0, 3, 2, 3, 1), (0, 3, 2, 2, 0), (1, 2, 7, 3), (1, 2, 6, 3), (0, 3, 1, 0, 0), (1, 3, 1, 0, 4),
            (1, 3, 2, 2, 4), (0, 0, 0, 1, 1, 1), (1, 3, 2, 3, 5), (1, 1, 0, 1, 1, 1), (1, 3, 1, 1, 4),
            (0, 3, 1, 0, 1), (1, 3, 1, 0, 5), (0, 3, 2, 2, 1), (1, 3, 2, 2, 5), (0, 3, 2, 3, 0), (1, 3, 2, 3, 4),
            (0, 0, 0, 1, 1, 2), (1, 1, 0, 1, 1, 2), (1, 3, 1, 1, 2), (0, 3, 2, 1, 1), (1, 3, 2, 1, 5),
            (1, 3, 2, 2, 2), (0, 3, 1, 2, 0), (1, 3, 1, 2, 4), (1, 3, 4, 0, 3), (1, 1, 0, 0, 1, 3), (1, 2, 7, 2),
            (1, 2, 5, 3), (0, 6, 5, 1), (1, 3, 5, 1, 0), (1, 3, 5, 1, 1), (1, 3, 3, 1, 1), (0, 3, 4, 0, 1),
            (1, 3, 4, 0, 5), (1, 3, 3, 0, 1), (0, 0, 0, 1, 1, 3), (1, 1, 0, 1, 1, 3), (0, 8, 0, 0), (0, 7, 0),
        ),
        (
        ),
        (
        ),
        (
        ),
        (
            (0, 7, 1),
        ),
        (
            (0, 7, 2),
        ),
        (
        ),
        (
            (0, 6, 5, 3), (1, 3, 5, 3, 0), (1, 3, 5, 3, 1),
        ),
        (
            (1, 3, 3, 1, 0), (0, 6, 3, 2), (0, 6, 4, 3), (1, 3, 4, 3, 2), (1, 3, 3, 2, 1), (1, 3, 4, 3, 0),
            (1, 3, 4, 3, 3),
        ),
        (
            (0, 3, 5, 0, 0), (1, 3, 5, 0, 4), (1, 3, 3, 0, 2), (1, 3, 5, 1, 2), (0, 5, 0, 0), (1, 4, 0, 0, 0, 2),
            (0, 3, 5, 1, 0),
        ),
        (
            (1, 4, 0, 0, 0, 3), (1, 3, 3, 2, 3), (0, 5, 0, 3), (1, 4, 0, 3, 0, 3), (1, 4, 0, 0, 0, 1),
            (1, 3, 3, 2, 0), (1, 3, 3, 1, 3), (1, 3, 5, 3, 2), (0, 5, 0, 1), (0, 3, 4, 1, 0), (1, 3, 4, 1, 4),
            (0, 3, 3, 2, 1), (1, 3, 3, 2, 5), (0, 6, 3, 3), (1, 3, 3, 3, 0), (1, 3, 3, 3, 3), (1, 4, 0, 1, 0, 3),
            (1, 3, 3, 3, 2), (1, 4, 0, 1, 0, 2), (0, 6, 4, 2), (1, 3, 4, 2, 1), (0, 3, 4, 3, 0), (1, 3, 4, 3, 4),
            (1, 3, 4, 2, 0), (1, 3, 4, 3, 1), (1, 3, 4, 1, 1), (1, 3, 4, 2, 3), (0, 3, 3, 0, 1), (0, 6, 5, 2),
            (1, 3, 5, 2, 3), (0, 5, 0, 2), (1, 4, 0, 2, 0, 3), (1, 4, 0, 3, 0, 2), (1, 3, 3, 3, 1), (1, 3, 5, 2, 1),
            (1, 3, 5, 0, 1), (1, 3, 5, 2, 0), (1, 4, 0, 1, 0, 1), (0, 3, 5, 3, 1), (1, 3, 5, 3, 5), (0, 3, 5, 1, 1),
            (1, 3, 5, 1, 5), (1, 3, 5, 1, 3), (0, 3, 3, 1, 0), (1, 3, 3, 2, 2), (1, 4, 0, 2, 0, 2),
            (0, 4, 0, 0, 1, 0),
        ),
        (
            (1, 0, 1, 0, 0, 0), (0, 3, 4, 1, 1), (1, 3, 5, 3, 3), (0, 3, 5, 3, 0), (1, 3, 5, 3, 4), (0, 3, 4, 2, 0),
            (1, 1, 1, 0, 0, 0), (1, 3, 4, 1, 5), (1, 3, 4, 0, 2), (1, 4, 0, 3, 0, 1), (0, 3, 5, 2, 0),
            (1, 3, 4, 2, 4), (1, 3, 5, 2, 4), (0, 3, 3, 1, 1), (1, 3, 3, 1, 5), (1, 4, 0, 2, 0, 1),
            (0, 4, 0, 1, 1, 0),
        ),
        (
            (1, 0, 1, 1, 0, 0), (1, 2, 6, 2), (1, 1, 1, 1, 0, 0), (1, 3, 5, 2, 2), (1, 3, 3, 0, 5), (0, 3, 4, 0, 0),
            (1, 3, 4, 0, 4), (0, 3, 4, 3, 1), (0, 3, 3, 3, 0), (1, 3, 4, 3, 5), (0, 3, 4, 2, 1), (0, 4, 0, 2, 1, 0),
        ),
        (
            (1, 0, 1, 2, 0, 0), (1, 3, 4, 2, 2), (0, 3, 5, 2, 1), (1, 3, 5, 2, 5), (0, 0, 1, 1, 1, 1),
            (1, 1, 1, 1, 1, 1), (0, 3, 3, 2, 0), (1, 3, 4, 2, 5), (1, 3, 3, 1, 4), (0, 3, 3, 3, 1), (1, 3, 3, 3, 5),
            (0, 4, 0, 3, 1, 0), (1, 3, 3, 3, 4),
        ),
        (
            (1, 0, 1, 3, 0, 0), (1, 3, 3, 2, 4), (0, 3, 5, 0, 1), (1, 3, 5, 0, 5), (0, 0, 1, 0, 1, 2),
            (1, 1, 1, 0, 1, 2), (1, 3, 5, 1, 4), (0, 0, 1, 0, 1, 1), (1, 1, 1, 0, 1, 1), (0, 0, 1, 0, 1, 3),
            (1, 1, 1, 0, 1, 3), (0, 0, 1, 1, 1, 2), (1, 1, 1, 1, 1, 2), (0, 0, 1, 3, 1, 1), (1, 1, 1, 3, 1, 1),
            (1, 1, 1, 3, 0, 0), (0, 8, 1, 0), (0, 7, 3), (0, 7, 4),
        ),
        (
            (0, 7, 5),
        ),
        (
            (0, 0, 1, 1, 1, 3), (1, 1, 1, 1, 1, 3), (1, 1, 1, 2, 0, 0), (0, 0, 1, 2, 1, 2), (1, 1, 1, 2, 1, 2),
            (0, 5, 1, 0), (1, 4, 1, 0, 0, 2), (0, 8, 1, 1),
        ),
        (
            (0, 0, 1, 2, 1, 1),
        ),
        (
            (1, 4, 1, 0, 0, 3), (1, 1, 1, 2, 1, 1), (1, 4, 1, 0, 0, 1), (0, 0, 1, 2, 1, 3), (1, 1, 1, 2, 1, 3),
            (0, 0, 1, 3, 1, 2), (1, 1, 1, 3, 1, 2), (0, 5, 1, 1), (1, 4, 1, 1, 0, 3), (1, 4, 1, 1, 0, 2),
            (0, 0, 1, 3, 1, 3), (1, 1, 1, 3, 1, 3), (0, 8, 1, 2),
        ),
        (
        ),
        (
            (0, 8, 1, 3),
        ),
        (
        ),
        (
            (0, 5, 1, 2), (1, 4, 1, 2, 0, 3), (0, 5, 1, 3), (1, 4, 1, 3, 0, 3), (1, 4, 1, 2, 0, 2),
            (1, 4, 1, 3, 0, 2), (0, 4, 1, 0, 1, 0),
        ),
        (
            (1, 4, 1, 3, 0, 1), (1, 4, 1, 1, 0, 1), (1, 4, 1, 2, 0, 1), (0, 4, 1, 1, 1, 0),
        ),
        (
            (0, 4, 1, 2, 1, 0),
        ),
        (
            (0, 4, 1, 3, 1, 0),
        ),
        (
        ),
    ),
    (
        (
            (1, 3, 5, 1, 0), (1, 3, 5, 1, 1), (1, 3, 5, 1, 3), (1, 3, 1, 1, 0), (1, 3, 1, 1, 1), (1, 3, 2, 1, 0),
            (1, 3, 2, 1, 3), (1, 3, 0, 1, 0), (1, 3, 0, 1, 3), (1, 3, 2, 1, 2), (1, 3, 5, 1, 2), (1, 3, 1, 1, 3),
            (1, 2, 4, 2), (1, 2, 3, 0), (1, 2, 0, 0), (1, 3, 4, 1, 0), (1, 2, 2, 2), (1, 3, 2, 1, 1),
        ),
        (
            (1, 2, 4, 0), (1, 2, 2, 0), (1, 0, 0, 1, 0, 0), (1, 3, 3, 1, 0), (0, 6, 2, 2), (1, 3, 2, 2, 2),
            (1, 3, 2, 2, 1), (1, 3, 3, 1, 1), (1, 2, 0, 2), (1, 3, 0, 1, 2), (1, 2, 1, 0), (1, 2, 3, 2),
            (1, 3, 2, 2, 3), (1, 2, 1, 2), (1, 3, 0, 1, 1), (1, 0, 0, 1, 1, 0), (0, 6, 1, 0), (1, 3, 1, 0, 2),
            (1, 3, 1, 0, 0), (1, 0, 0, 0, 0, 0), (0, 3, 2, 1, 0), (1, 3, 2, 2, 0), (1, 3, 1, 1, 2),
            (1, 0, 0, 0, 1, 0), (1, 2, 3, 3), (0, 3, 2, 1, 1), (0, 6, 0, 2), (1, 3, 0, 2, 3), (1, 3, 1, 0, 1),
            (1, 3, 0, 2, 1), (1, 3, 0, 2, 2), (1, 3, 2, 1, 4), (1, 3, 0, 2, 0), (0, 0, 0, 0, 0, 1), (1, 2, 5, 0),
            (0, 0, 0, 1, 0, 1), (1, 0, 0, 1, 0, 1), (1, 0, 0, 0, 0, 1), (0, 6, 1, 2), (1, 3, 1, 2, 2), (1, 2, 6, 0),
            (0, 3, 0, 1, 1), (1, 3, 1, 2, 3), (0, 3, 4, 1, 0), (0, 3, 0, 1, 0), (0, 3, 5, 1, 1), (0, 3, 1, 0, 0),
            (1, 3, 2, 1, 5), (1, 3, 0, 1, 5), (0, 0, 0, 1, 1, 1), (1, 0, 0, 1, 1, 1), (1, 1, 0, 1, 1, 1),
            (0, 0, 0, 0, 1, 1), (0, 6, 0, 0), (1, 0, 0, 0, 1, 1), (1, 3, 0, 0, 2), (1, 3, 0, 0, 0), (1, 3, 4, 1, 1),
            (0, 6, 2, 0), (0, 3, 0, 2, 1), (1, 3, 0, 2, 5), (0, 3, 2, 2, 0), (1, 3, 0, 0, 1), (1, 3, 2, 0, 0),
            (1, 2, 0, 3), (1, 3, 2, 2, 4), (1, 2, 2, 3), (0, 3, 4, 1, 1), (0, 3, 0, 2, 0), (1, 3, 0, 2, 4),
            (1, 2, 1, 3), (1, 3, 0, 1, 4), (1, 3, 1, 2, 1), (1, 3, 1, 2, 0), (1, 2, 4, 3), (0, 3, 0, 0, 1),
            (0, 6, 1, 3), (1, 3, 1, 3, 1), (1, 3, 4, 1, 3), (1, 3, 4, 1, 2), (1, 3, 1, 3, 0), (1, 3, 1, 0, 4),
            (1, 3, 1, 3, 3), (1, 3, 0, 0, 3), (0, 0, 0, 0, 1, 2), (1, 0, 0, 0, 1, 2), (1, 3, 1, 3, 2),
            (0, 3, 1, 2, 0), (0, 6, 0, 3), (1, 3, 0, 3, 0), (1, 3, 0, 3, 3), (0, 0, 0, 1, 1, 2), (1, 3, 0, 3, 1),
            (0, 3, 1, 0, 1), (1, 3, 1, 0, 5), (1, 1, 0, 1, 0, 0), (1, 2, 7, 0), (1, 0, 0, 1, 1, 2), (1, 3, 0, 3, 2),
            (1, 3, 2, 0, 1), (1, 2, 5, 2), (0, 3, 0, 0, 0), (0, 6, 2, 3), (1, 3, 2, 3, 1), (1, 3, 2, 3, 0),
            (1, 3, 2, 0, 3), (1, 2, 6, 2), (1, 2, 5, 3), (0, 3, 1, 1, 1), (1, 3, 1, 1, 5), (0, 3, 2, 2, 1),
            (1, 3, 0, 0, 4), (1, 3, 2, 2, 5), (1, 3, 0, 0, 5), (0, 6, 3, 3), (0, 3, 0, 3, 1), (1, 3, 0, 3, 5),
            (0, 6, 3, 0), (0, 6, 3, 2), (1, 3, 3, 3, 0), (1, 3, 5, 1, 5), (0, 3, 2, 3, 1), (0, 3, 2, 0, 1),
            (1, 3, 2, 0, 5), (0, 3, 1, 3, 0), (1, 3, 2, 3, 3), (0, 3, 2, 3, 0), (1, 3, 2, 3, 4), (0, 3, 2, 0, 0),
            (1, 3, 2, 0, 4), (1, 3, 1, 0, 3), (0, 3, 0, 3, 0), (1, 3, 0, 3, 4), (0, 3, 1, 2, 1), (0, 3, 1, 3, 1),
            (1, 3, 1, 3, 5), (1, 3, 1, 2, 5), (0, 6, 5, 0), (1, 3, 1, 3, 4), (1, 3, 5, 0, 0), (1, 3, 2, 0, 2),
            (1, 3, 1, 2, 4), (1, 1, 0, 1, 1, 2), (1, 3, 3, 0, 1), (1, 3, 2, 3, 2), (0, 3, 1, 1, 0), (1, 3, 1, 1, 4),
            (1, 1, 0, 0, 0, 0), (1, 1, 0, 0, 1, 2), (1, 1, 0, 1, 0, 1), (1, 1, 0, 0, 1, 1), (1, 1, 0, 0, 0, 1),
            (0, 8, 0, 0), (1, 3, 2, 3, 5), (1, 3, 3, 0, 2), (0, 7, 0), (0, 6, 4, 0), (1, 3, 4, 0, 2), (1, 3, 5, 0, 2),
        ),
        (
        ),
        (
            (1, 2, 7, 2), (1, 2, 6, 3), (1, 3, 3, 2, 1), (1, 3, 4, 0, 3), (1, 3, 4, 0, 1), (1, 3, 4, 0, 0),
            (0, 6, 4, 2),
        ),
        (
            (1, 3, 4, 2, 1), (1, 3, 4, 2, 2), (0, 3, 3, 1, 1), (1, 3, 5, 0, 3), (0, 3, 5, 0, 0),
        ),
        (
            (0, 6, 5, 3), (1, 3, 5, 3, 0), (1, 3, 5, 3, 2), (1, 3, 5, 3, 1), (0, 7, 1), (1, 3, 4, 2, 0),
            (1, 3, 3, 3, 1),
        ),
        (
        ),
        (
            (1, 3, 3, 2, 0), (0, 7, 2),
        ),
        (
            (1, 2, 7, 3), (1, 3, 3, 0, 3), (1, 3, 5, 0, 1), (0, 6, 5, 2), (1, 3, 5, 2, 1),
        ),
        (
        ),
        (
            (0, 4, 0, 0, 0, 1), (0, 5, 0, 0), (1, 4, 0, 0, 0, 1), (0, 5, 0, 1), (1, 3, 3, 0, 0),
        ),
        (
            (0, 4, 0, 0, 0, 2), (1, 4, 0, 0, 0, 2), (1, 3, 5, 2, 2), (1, 3, 3, 3, 2), (0, 5, 0, 3), (0, 5, 0, 2),
            (1, 3, 5, 2, 0), (1, 3, 5, 3, 3), (0, 4, 0, 3, 0, 2), (0, 3, 5, 3, 0), (1, 4, 0, 3, 0, 2),
            (0, 4, 0, 0, 0, 0), (0, 4, 0, 0, 1, 0),
        ),
        (
            (1, 0, 1, 0, 0, 0), (0, 4, 0, 0, 1, 1), (1, 4, 0, 0, 1, 1), (1, 0, 1, 0, 1, 0), (0, 4, 0, 1, 0, 2),
            (1, 3, 3, 2, 2), (1, 4, 0, 1, 0, 2), (1, 3, 5, 3, 4), (0, 3, 3, 1, 0), (1, 3, 3, 1, 4), (0, 3, 3, 0, 0),
            (0, 3, 4, 2, 0), (0, 3, 3, 0, 1), (0, 3, 5, 1, 0), (1, 3, 5, 2, 3), (0, 4, 0, 3, 1, 1), (0, 3, 4, 2, 1),
            (0, 4, 0, 1, 0, 1), (1, 4, 0, 1, 0, 1), (1, 3, 5, 1, 4), (1, 4, 0, 3, 1, 1), (0, 4, 0, 2, 0, 2),
            (1, 4, 0, 2, 0, 2), (1, 3, 4, 1, 5), (1, 3, 4, 2, 3), (0, 4, 0, 3, 0, 1), (1, 4, 0, 3, 0, 1),
            (0, 4, 0, 1, 1, 1), (1, 4, 0, 1, 1, 1), (0, 4, 0, 1, 1, 0), (0, 3, 3, 3, 0), (0, 4, 0, 1, 0, 0),
        ),
        (
            (1, 0, 1, 1, 0, 0), (1, 0, 1, 1, 1, 0), (0, 3, 5, 2, 0), (1, 3, 3, 2, 3), (0, 3, 3, 3, 1),
            (0, 3, 5, 2, 1), (1, 3, 5, 2, 5), (1, 3, 4, 2, 5), (1, 3, 4, 1, 4), (0, 4, 0, 2, 0, 1),
            (1, 4, 0, 2, 0, 1), (1, 3, 4, 2, 4), (0, 3, 3, 2, 1), (1, 3, 3, 2, 5), (0, 4, 0, 2, 1, 1),
            (1, 4, 0, 2, 1, 1), (1, 3, 3, 3, 5), (0, 3, 3, 2, 0), (1, 3, 5, 2, 4), (0, 0, 1, 0, 0, 1),
            (1, 0, 1, 0, 0, 1), (1, 3, 3, 2, 4), (1, 3, 3, 1, 5), (1, 3, 3, 3, 4), (0, 0, 1, 0, 1, 1),
            (1, 0, 1, 0, 1, 1), (0, 0, 1, 1, 1, 1), (1, 0, 1, 1, 1, 1), (1, 1, 1, 0, 1, 1), (1, 3, 5, 0, 4),
            (0, 4, 0, 2, 1, 0), (1, 3, 3, 0, 5), (0, 3, 5, 3, 1), (1, 3, 5, 3, 5), (0, 3, 4, 0, 0), (1, 3, 4, 0, 4),
            (1, 1, 1, 0, 0, 0), (0, 4, 0, 2, 0, 0),
        ),
        (
            (1, 0, 1, 2, 1, 0), (1, 1, 1, 2, 0, 0), (0, 0, 1, 1, 0, 1), (1, 0, 1, 1, 0, 1), (0, 0, 1, 0, 1, 2),
            (1, 0, 1, 0, 1, 2), (1, 1, 1, 0, 0, 1), (1, 1, 1, 1, 0, 1), (0, 4, 0, 3, 0, 0), (0, 4, 0, 3, 1, 0),
        ),
        (
            (1, 1, 1, 1, 1, 1), (1, 0, 1, 2, 0, 0), (1, 3, 3, 0, 4), (1, 0, 1, 3, 0, 0), (1, 0, 1, 3, 1, 0),
            (0, 6, 4, 3), (1, 3, 4, 3, 1), (1, 3, 4, 3, 0), (1, 1, 1, 3, 0, 0), (1, 3, 3, 1, 2), (1, 3, 4, 3, 2),
            (1, 3, 3, 1, 3), (0, 3, 4, 0, 1), (1, 3, 4, 0, 5), (0, 0, 1, 2, 0, 1), (1, 1, 1, 2, 0, 1),
            (1, 0, 1, 2, 0, 1), (0, 0, 1, 1, 1, 2), (1, 0, 1, 1, 1, 2), (1, 3, 3, 3, 3), (0, 0, 1, 3, 0, 1),
            (1, 1, 1, 3, 0, 1), (1, 0, 1, 3, 0, 1), (0, 0, 1, 2, 1, 1), (1, 0, 1, 2, 1, 1), (1, 1, 1, 2, 1, 1),
            (1, 3, 4, 3, 3), (0, 3, 4, 3, 0), (1, 3, 4, 3, 4), (1, 1, 1, 1, 0, 0), (0, 0, 1, 3, 1, 1),
            (1, 0, 1, 3, 1, 1), (0, 3, 4, 3, 1), (1, 3, 4, 3, 5), (0, 3, 5, 0, 1), (1, 3, 5, 0, 5),
            (1, 1, 1, 1, 1, 2), (1, 1, 1, 3, 1, 1), (0, 0, 1, 2, 1, 2), (1, 1, 1, 2, 1, 2), (1, 0, 1, 2, 1, 2),
            (0, 0, 1, 3, 1, 2), (1, 1, 1, 3, 1, 2), (1, 0, 1, 3, 1, 2), (0, 7, 3), (1, 1, 1, 0, 1, 2), (0, 8, 1, 0),
            (0, 7, 4),
        ),
        (
            (0, 7, 5),
        ),
        (
            (0, 8, 1, 1),
        ),
        (
            (0, 5, 1, 0), (0, 4, 1, 0, 0, 1), (0, 4, 1, 0, 0, 2), (1, 4, 1, 0, 0, 2),
        ),
        (
            (1, 4, 1, 0, 0, 1), (0, 8, 1, 2),
        ),
        (
        ),
        (
            (0, 5, 1, 1), (0, 4, 1, 1, 0, 2), (1, 4, 1, 1, 0, 2), (0, 8, 1, 3),
        ),
        (
            (0, 4, 1, 0, 1, 1), (1, 4, 1, 0, 1, 1), (0, 4, 1, 1, 0, 1), (1, 4, 1, 1, 0, 1),
        ),
        (
            (0, 4, 1, 2, 0, 2), (0, 5, 1, 2), (1, 4, 1, 2, 0, 2), (0, 4, 1, 1, 1, 1), (1, 4, 1, 1, 1, 1),
            (0, 5, 1, 3), (0, 4, 1, 3, 0, 2), (1, 4, 1, 3, 0, 2), (0, 4, 1, 2, 0, 1), (1, 4, 1, 2, 0, 1),
            (0, 4, 1, 0, 0, 0), (0, 4, 1, 2, 1, 1), (1, 4, 1, 2, 1, 1), (0, 4, 1, 1, 1, 0), (0, 4, 1, 3, 1, 1),
            (1, 4, 1, 3, 1, 1), (0, 4, 1, 3, 0, 1), (1, 4, 1, 3, 0, 1), (0, 4, 1, 0, 1, 0),
        ),
        (
            (0, 4, 1, 1, 0, 0),
        ),
        (
            (0, 4, 1, 2, 1, 0), (0, 4, 1, 2, 0, 0),
        ),
        (
            (0, 4, 1, 3, 0, 0), (0, 4, 1, 3, 1, 0),
        ),
        (
        ),
    ),
)

OWN_FIRST = {}
for at, ops in enumerate(PLAN):
    for op in (op for stage in ops for op in stage):
        if op[:2] == (1, HOP) and op[3] == at:
            OWN_FIRST.setdefault((op[2], at), op[4])


def layer_kernel(
    n_fs,
    groups,
    tokens_in,
    norm_gain_in,
    wq,
    wk,
    wv,
    wg,
    mixer_gain_in,
    wo,
    channel_gain_in,
    wl,
    wr,
    taps_left_in,
    taps_right_in,
    wd,
    cos_in,
    sin_in,
    gammas_in,
    out,
    tokens,
    norm_gain,
    mixer_gain,
    channel_gain,
    taps_left,
    taps_right,
    cos_t,
    sin_t,
    gammas,
    w1,
    wout,
    wlr,
    wdown,
    nt,
    nm,
    qkvg,
    held_kept,
    hid,
    gated,
    part1,
    part2,
    xb1,
    xb2,
    sb1,
    sb2,
    rb1,
    rb2,
    mid,
    acc,
    both,
    fin,
    w_send,
    w_recv,
    self_sem,
    h_send,
    h_recv,
    h_rest,
    a_send,
    a_recv,
    f_send,
    f_recv,
    x_send,
    x_recv,
    r_send,
    r_recv,
    o_send,
    o_recv,
    load_sem,
    store_sem,
):
    fs, tp = lax.axis_index("fs"), lax.axis_index("tp")
    planes = n_fs // groups
    z, q = fs // planes, lax.rem(fs, planes)
    other = 1 - tp
    length, width = tokens_in.shape
    own = length // 2
    part_rows = own // NT_PARTS
    span_c = length // CHUNKS
    few = span_c // 2
    kb = wq.shape[0]
    nb = wo.shape[1]
    cq, cv, cf = wq.shape[1] // groups, wv.shape[1] // groups, wl.shape[1] // groups
    upper = z * 2 >= groups
    place_z = jnp.where(upper, groups - 1 - z, z)

    def real(plane):
        return jnp.where(upper, groups - 1 - plane, plane)

    def flip(side):
        return jnp.where(upper, 1 - side, side)

    def zdev(target):
        return {"fs": target * planes + q, "tp": tp}

    partner = {"fs": fs, "tp": other}

    def lanes(index, size):
        return pl.ds(pl.multiple_of(index * size, 128), size)

    def rows(index, size):
        return pl.ds(pl.multiple_of(index * size, size), size)

    pieces = (
        (lambda c: wq.at[:, lanes(c, cq)], lambda f: w1.at[rows(f, kb), pl.ds(0, cq)]),
        (lambda c: wk.at[:, lanes(c, cq)], lambda f: w1.at[rows(f, kb), pl.ds(cq, cq)]),
        (lambda c: wv.at[:, lanes(c, cv)], lambda f: w1.at[rows(f, kb), pl.ds(2 * cq, cv)]),
        (lambda c: wg.at[:, lanes(c, cv)], lambda f: w1.at[rows(f, kb), pl.ds(2 * cq + cv, cv)]),
        (lambda c: wo.at[rows(c, cv), :], lambda f: wout.at[:, lanes(f, nb)]),
        (lambda c: wl.at[:, lanes(c, cf)], lambda f: wlr.at[rows(f, kb), pl.ds(0, cf)]),
        (lambda c: wr.at[:, lanes(c, cf)], lambda f: wlr.at[rows(f, kb), pl.ds(cf, cf)]),
        (lambda c: wd.at[rows(c, cf), :], lambda f: wdown.at[:, lanes(f, nb)]),
    )
    starts = (0, cq, 2 * cq, 2 * cq + cv, 0, 0, cf, 0)
    widths = (cq, cq, cv, cv, 0, cf, cf, 0)

    def stretch(cls, first, count, half=None):
        members = [i for i in range(len(pieces)) if CLASS_OF[i] == cls]
        low = starts[members[0]]
        wide = sum(widths[i] for i in members)
        if members[0] == 4 or members[0] == 7:
            buf, size = (wout, cv) if members[0] == 4 else (wdown, cf)
            across = pl.ds(pl.multiple_of(first * nb, 128), count * nb)
            if half is None:
                return buf.at[:, across]
            return buf.at[pl.ds(half * (size // 2), size // 2), across]
        buf = w1 if members[0] < 4 else wlr
        if half is None:
            return buf.at[pl.ds(pl.multiple_of(first * kb, kb), count * kb), pl.ds(low, wide)]
        start = pl.multiple_of(first * kb + half * (kb // 2), kb // 2)
        return buf.at[pl.ds(start, kb // 2), pl.ds(low, wide)]

    barrier = pltpu.get_barrier_semaphore()
    for step in range(1, groups):
        pl.semaphore_signal(barrier, inc=1, device_id=zdev(lax.rem(z + step, groups)), device_id_type=MESH)
    qx = q + 1 - 2 * lax.rem(q, 2)
    qy = q + 2 - 4 * (q // 2)
    diagonal = planes - 1 - q
    to_x = {"fs": z * planes + qx, "tp": tp}
    to_y = {"fs": z * planes + qy, "tp": tp}
    for device in (to_x, to_y):
        pl.semaphore_signal(barrier, inc=1, device_id=device, device_id_type=MESH)
    pl.semaphore_signal(barrier, inc=1, device_id=partner, device_id_type=MESH)

    loads = []
    for i, (source, held_here) in enumerate((
        (tokens_in, tokens), (norm_gain_in, norm_gain), (mixer_gain_in, mixer_gain),
        (channel_gain_in, channel_gain), (taps_left_in, taps_left), (taps_right_in, taps_right),
        (cos_in, cos_t), (sin_in, sin_t), (gammas_in, gammas),
    )):
        load = pltpu.make_async_copy(source, held_here, load_sem.at[i])
        load.start()
        loads.append(load)
    keeps = []
    for i, (src, dst) in enumerate(pieces):
        keep = pltpu.make_async_copy(src(z), dst(fs), self_sem.at[i])
        keep.start()
        keeps.append(keep)

    def prepare(_):
        for load in loads:
            load.wait()
        my_half = pl.ds(pl.multiple_of(tp * own, own), own)
        nt[pl.ds(pl.multiple_of(z * length + tp * own, own), own), :] = normed_rows(
            tokens[my_half, :].astype(jnp.float32), norm_gain[...]
        )

    pl.semaphore_wait(barrier, groups - 1 + 2 + 1)

    def remote(src, dst, ssem, rsem, device):
        return pltpu.make_async_remote_copy(
            src_ref=src, dst_ref=dst, send_sem=ssem, recv_sem=rsem,
            device_id=device, device_id_type=MESH,
        )

    def block(key, c, seq, core):
        if key:
            first = c * groups * span_c + seq * span_c + core * few
            return nm.at[pl.ds(pl.multiple_of(first, few), few), :]
        first = seq * length + core * own + c * part_rows
        return nt.at[pl.ds(pl.multiple_of(first, part_rows), part_rows), :]

    part, xb, sb, rb = (part1, part2), (xb1, xb2), (sb1, sb2), (rb1, rb2)

    def pair(which, c, g):
        return part[which][c, tp, g].astype(jnp.float32) + xb[which][c, g].astype(jnp.float32)

    def exchange(which, c):
        return remote(part[which].at[c, other], xb[which].at[c], x_send.at[which], x_recv.at[which, c], partner)

    def gather_copy(me, key, c, side, d, landing=False):
        move = 1 - 2 * side
        source = real(me - move * d)
        ref = block(key, c, source, tp)
        at = c + key * NT_PARTS
        device = partner if landing else zdev(real(me + move))
        return remote(ref, ref, a_send.at[key], a_recv.at[at, source], device)

    def core_copy(me, key, c, side, d):
        move = 1 - 2 * side
        ref = block(key, c, real(me - move * d), tp)
        return remote(ref, ref, f_send.at[key], f_recv.at[key * (1 + c)], partner)

    def weight_copy(me, i, plane):
        src, dst = pieces[i]
        far = real(plane)
        return remote(src(far), dst(fs), w_send.at[i], w_recv.at[CLASS_OF[i], z], zdev(far))

    def hop_copy(me, cls, plane, slot, landing=False):
        origin = (qx, qy)[slot] if landing else (q, q, q, q, qx, qy)[slot]
        source = real(plane)
        ref = stretch(cls, source * planes + origin, 1, (0, 1, 1, 0, 0, 1)[slot])
        device = (to_x, to_y, to_x, to_y, to_y, to_x)[slot]
        landed = h_recv.at[cls, source, slot] if slot < 2 else h_rest.at[cls]
        return remote(ref, ref, h_send.at[cls], landed, device)

    def sum_copy(me, which, c, side, d, landing=False):
        ref = sb[which].at[c, flip(side), d]
        at = d if landing else d - 1
        device = partner if landing else zdev(real(me + 1 - 2 * side))
        return remote(ref, rb[which].at[c, flip(side), at], r_send.at[which], r_recv.at[which, c, flip(side), at], device)

    makers = (gather_copy, core_copy, weight_copy, hop_copy, sum_copy)

    def await_bytes(ref, sem):
        remote(ref, ref, sem, sem, partner).wait_recv()

    def act(me, op):
        sends, kind, args = op[0], op[1], op[2:]
        if not sends:
            if kind == SWAP:
                exchange(*args).wait_recv()
            elif kind == WEIGHTS:
                cls, far = args[0], real(args[1])
                await_bytes(stretch(cls, far * planes + q, 1), w_recv.at[cls, far])
            elif kind == HOPS:
                await_bytes(stretch(args[0], 0, 2 * groups), h_rest.at[args[0]])
            elif kind == CORES:
                key, c = args
                if key:
                    await_bytes(nm.at[pl.ds(0, groups * few), :], f_recv.at[1 + c])
                else:
                    await_bytes(nt.at[pl.ds(0, groups * own), :], f_recv.at[0])
            else:
                makers[kind](me, *args, True).wait_recv()
            return
        if kind == HOP and args[1] == me and args[2] == OWN_FIRST[args[0], me]:
            for i, keep in enumerate(keeps):
                if CLASS_OF[i] == args[0]:
                    keep.wait()
        if kind == SUM:
            which, c, side, d = args
            move = 1 - 2 * side
            value = pair(which, c, real(me + move * d))
            if 0 <= me - move < groups:
                value = value + rb[which][c, flip(side), d].astype(jnp.float32)
            sb[which][c, flip(side), d] = value.astype(jnp.bfloat16)
        makers[kind](me, *args).start()

    def perform(stage):
        for me, ops in enumerate(PLAN):
            @pl.when(place_z == me)
            def _():
                for op in ops[stage]:
                    act(me, op)

    def multiply(left, weight, which, c):
        value = jnp.dot(
            left[rows(c, groups * span_c), :], weight[...], preferred_element_type=jnp.float32
        ).astype(jnp.bfloat16)
        for g in range(groups):
            part[which][c, 0, g] = value[g * span_c : g * span_c + few]
            part[which][c, 1, g] = value[g * span_c + few : (g + 1) * span_c]
        exchange(which, c).start()

    def collect(which, c):
        acc[c] = pair(which, c, z)
        for side, has in ((0, z > 0), (1, z < groups - 1)):
            @pl.when(has)
            def _():
                acc[c] = acc[c] + rb[which][c, side, 0].astype(jnp.float32)
        return acc[c]

    def natural(c, core):
        return pl.ds(pl.multiple_of(c * span_c + core * few, few), few)

    head = tp * groups + z
    chunk = groups * length // 2

    def project(at):
        span = rows(at, chunk)
        qkvg[span, :] = jnp.dot(
            nt[span, :], w1[:, pl.ds(0, 2 * cq + cv)], preferred_element_type=jnp.float32
        ).astype(jnp.bfloat16)

    def gate(at):
        span = rows(at, chunk)
        gates = jnp.dot(
            nt[span, :], w1[:, pl.ds(2 * cq + cv, cv)], preferred_element_type=jnp.float32
        ).astype(jnp.bfloat16).astype(jnp.float32)
        whole = (held_kept[span, :] * mixer_gain[:, lanes(z, cv)] * silu(gates)).astype(jnp.bfloat16)
        for i in range(chunk // length):
            for c in range(CHUNKS):
                first = i * length + c * span_c
                hid[rows(at * (chunk // length) + i + c * groups, span_c), :] = whole[first : first + span_c]

    def two_parts(x):
        high = x.astype(jnp.bfloat16)
        return high, (x - high.astype(jnp.float32)).astype(jnp.bfloat16)

    def retain(first):
        log_gamma = gammas[pl.ds(head, 1), :]
        distance = (
            lax.broadcasted_iota(jnp.int32, (length, length), 0)
            - lax.broadcasted_iota(jnp.int32, (length, length), 1)
        ).astype(jnp.float32)
        decay = jnp.where(distance >= 0, jnp.exp(log_gamma * jnp.maximum(distance, 0.0)), 0.0)

        @pl.loop(first * groups // 2, (first + 1) * groups // 2)
        def _(at):
            span = rows(at, length)
            held = qkvg[span, pl.ds(0, 2 * cq)].astype(jnp.float32)

            def turn(x):
                return x * cos_t[...] + pltpu.roll(x, cq // 2, 1) * sin_t[...]

            rq = turn(held[:, :cq])
            rk = turn(held[:, cq : 2 * cq])
            q_high, q_low = two_parts(rq)
            k_high, k_low = two_parts(rk)
            scores = lax.dot_general(
                jnp.concatenate([q_high, q_high, q_low], axis=1),
                jnp.concatenate([k_high, k_low, k_high], axis=1),
                (((1,), (1,)), ((), ())), preferred_element_type=jnp.float32,
            ) * decay
            s_high, s_low = two_parts(scores)
            v_exact = qkvg[span, pl.ds(2 * cq, cv)]
            kept = jnp.dot(
                jnp.concatenate([s_high, s_low], axis=1),
                jnp.concatenate([v_exact, v_exact], axis=0), preferred_element_type=jnp.float32,
            )
            kept = kept * lax.rsqrt(jnp.mean(kept * kept, axis=-1, keepdims=True) + 1e-06)
            held_kept[span, :] = kept

    def renorm(c):
        middle = (
            tokens[natural(c, tp), :].astype(jnp.float32) + collect(0, c)
        ).astype(jnp.bfloat16).astype(jnp.float32)
        mid[c] = middle
        first = c * groups * span_c + z * span_c + tp * few
        nm[pl.ds(pl.multiple_of(first, few), few), :] = normed_rows(middle, channel_gain[...])

    place = lax.rem(lax.broadcasted_iota(jnp.int32, (groups * span_c, 1), 0), span_c)

    def convolve(c, low, taps):
        x = both[c, :, low : low + cf].astype(jnp.float32)
        count = taps.shape[0]
        weights = taps[:, lanes(z, cf)]
        result = x * weights[count - 1 :, :]
        for back in range(1, count):
            if c:
                before = both[c - 1, :, low : low + cf].astype(jnp.float32)
                before = pltpu.roll(before, back + (groups - 1) * span_c, 0)
            else:
                before = 0.0
            moved = jnp.where(place >= back, pltpu.roll(x, back, 0), before)
            result = result + moved * weights[count - 1 - back : count - back, :]
        return result

    def mix(c):
        both[c] = jnp.dot(
            nm[rows(c, groups * span_c), :], wlr[...], preferred_element_type=jnp.float32
        ).astype(jnp.bfloat16)
        gated[rows(c, groups * span_c), :] = (
            silu(convolve(c, 0, taps_left)) * convolve(c, cf, taps_right)
        ).astype(jnp.bfloat16)

    def finish(c):
        mine = natural(c, tp)
        fin[c] = (mid[c] + collect(1, c)).astype(jnp.bfloat16)
        remote(fin.at[c], out.at[mine, :], o_send.at[0], o_recv.at[0], partner).start()
        pltpu.make_async_copy(fin.at[c], out.at[mine, :], store_sem.at[0]).start()

    steps = (
        project,
        retain,
        lambda c: multiply(hid, wout, 0, c),
        renorm,
        mix,
        lambda c: multiply(gated, wdown, 1, c),
        finish,
        prepare,
        gate,
    )
    perform(0)
    for stage, (name, index) in enumerate(STAGES):
        steps[name](index)
        perform(stage + 1)
    await_bytes(fin, o_recv.at[0])
    await_bytes(fin, o_send.at[0])
    for key, buf in ((0, nt), (1, nm)):
        await_bytes(buf.at[pl.ds(0, groups * own), :], f_send.at[key])
        await_bytes(part[key].at[:, 0], x_send.at[key])
        await_bytes(sb[key].at[:, 0, pl.ds(0, groups - 1)], r_send.at[key])
    for cls in range(max(CLASS_OF) + 1):
        await_bytes(stretch(cls, 0, 3 * groups), h_send.at[cls])
    for i, (_, dst) in enumerate(pieces):
        if i == 4 or i == 7:
            ref = (wout if i == 4 else wdown).at[:, pl.ds(0, (groups - 1) * nb)]
        else:
            ref = (w1 if i < 4 else wlr).at[pl.ds(0, (groups - 1) * kb), pl.ds(starts[i], widths[i])]
        await_bytes(ref, w_send.at[i])
    for me, ops in enumerate(PLAN):
        @pl.when(place_z == me)
        def _():
            for key, buf, size in ((0, nt, part_rows), (1, nm, few)):
                count = sum(op[:3] == (1, 0, key) for stage in ops for op in stage)
                await_bytes(buf.at[pl.ds(0, count * size), :], a_send.at[key])
    pltpu.make_async_copy(fin, fin, store_sem.at[0]).wait()


def body(n_fs, *args):
    (tokens, norm_gain, w_query, w_key, w_value, w_gate, mixer_gain, w_out, channel_gain,
     w_left, w_right, taps_left, taps_right, w_down) = args
    groups = w_query.shape[1] // DK
    if (
        groups != 2 * len(PLAN)
        or n_fs % groups
        or n_fs != 4 * groups
        or lax.axis_size("tp") != 2
        or tokens.shape[0] != BLOCK
        or (w_left.shape[1] // groups) % 128
        or w_left.shape[1] % groups
        or w_out.shape[1] % 128
        or w_query.shape[0] % 32
        or tokens.shape[0] % (32 * CHUNKS)
    ):
        return plain_body(*args)
    length, width = tokens.shape
    heads = groups * lax.axis_size("tp")
    cq, cv, cf = w_query.shape[1] // groups, w_value.shape[1] // groups, w_left.shape[1] // groups
    planes = n_fs // groups
    span_c = length // CHUNKS
    few = span_c // 2
    classes = max(CLASS_OF) + 1
    cos_t, sin_t = turning(length, DK)
    gammas = log_gammas(heads)
    held = pl.BlockSpec(memory_space=pl.ANY)
    bf, f32, dma = jnp.bfloat16, jnp.float32, pltpu.SemaphoreType.DMA
    return pl.pallas_call(
        functools.partial(layer_kernel, n_fs, groups),
        out_shape=jax.ShapeDtypeStruct(tokens.shape, bf),
        in_specs=[held] * 17,
        out_specs=held,
        scratch_shapes=[
            pltpu.VMEM(tokens.shape, bf),
            pltpu.VMEM((1, width), f32),
            pltpu.VMEM((1, w_value.shape[1]), f32),
            pltpu.VMEM((1, width), f32),
            pltpu.VMEM(taps_left.shape, f32),
            pltpu.VMEM(taps_right.shape, f32),
            pltpu.VMEM(cos_t.shape, f32),
            pltpu.VMEM(sin_t.shape, f32),
            pltpu.VMEM(gammas.shape, f32),
            pltpu.VMEM((width, 2 * cq + 2 * cv), bf),
            pltpu.VMEM((cv, width), bf),
            pltpu.VMEM((width, 2 * cf), bf),
            pltpu.VMEM((cf, width), bf),
            pltpu.VMEM((groups * length, width), bf),
            pltpu.VMEM((groups * length, width), bf),
            pltpu.VMEM((groups * length, 2 * cq + cv), bf),
            pltpu.VMEM((groups * length, cv), f32),
            pltpu.VMEM((groups * length, cv), bf),
            pltpu.VMEM((groups * length, cf), bf),
            pltpu.VMEM((CHUNKS, 2, groups, few, width), bf),
            pltpu.VMEM((CHUNKS, 2, groups, few, width), bf),
            pltpu.VMEM((CHUNKS, groups, few, width), bf),
            pltpu.VMEM((CHUNKS, groups, few, width), bf),
            pltpu.VMEM((CHUNKS, 2, groups, few, width), bf),
            pltpu.VMEM((CHUNKS, 2, groups, few, width), bf),
            pltpu.VMEM((CHUNKS, 2, groups, few, width), bf),
            pltpu.VMEM((CHUNKS, 2, groups, few, width), bf),
            pltpu.VMEM((CHUNKS, few, width), f32),
            pltpu.VMEM((CHUNKS, few, width), f32),
            pltpu.VMEM((CHUNKS, groups * span_c, 2 * cf), bf),
            pltpu.VMEM((CHUNKS, few, width), bf),
            dma((8,)),
            dma((classes, groups)),
            dma((8,)),
            dma((classes,)),
            dma((classes, groups, 2)),
            dma((classes,)),
            dma((2,)),
            dma((NT_PARTS + CHUNKS, groups)),
            dma((2,)),
            dma((1 + CHUNKS,)),
            dma((2,)),
            dma((2, CHUNKS)),
            dma((2,)),
            dma((2, CHUNKS, 2, groups - 1)),
            dma((1,)),
            dma((1,)),
            dma((9,)),
            dma((1,)),
        ],
        compiler_params=pltpu.CompilerParams(
            collective_id=0, has_side_effects=True, vmem_limit_bytes=60 * 1024 * 1024
        ),
    )(
        tokens, norm_gain[None], w_query, w_key, w_value, w_gate, mixer_gain[None], w_out,
        channel_gain[None], w_left, w_right, taps_left, taps_right, w_down,
        cos_t, sin_t, gammas,
    )


def solution(mesh):
    placed = (
        P("fs", None),
        P(),
        P("fs", "tp"),
        P("fs", "tp"),
        P("fs", "tp"),
        P("fs", "tp"),
        P("tp"),
        P("tp", "fs"),
        P(),
        P("fs", "tp"),
        P("fs", "tp"),
        P(None, "tp"),
        P(None, "tp"),
        P("tp", "fs"),
    )
    return jax.shard_map(
        functools.partial(body, mesh.shape["fs"]), mesh=mesh, in_specs=placed, out_specs=P("fs", None), check_vma=False)
```

```python
import functools

import jax
import jax.numpy as jnp
import numpy as np
from jax import lax
from jax.experimental import pallas as pl
from jax.experimental.pallas import tpu as pltpu
from jax.sharding import PartitionSpec as P

DK = 128
DV = 256
BLOCK = 128
MESH = pl.DeviceIdType.MESH


highest = lax.Precision.HIGHEST


def scale_rows(rows_in, gain_vec):
    floats = rows_in.astype(jnp.float32)
    factor = lax.rsqrt(jnp.mean(floats * floats, axis=-1, keepdims=True) + 1e-06)
    return (floats * factor * gain_vec).astype(jnp.bfloat16)


def decays(first_head, count):
    head_ids = first_head + jnp.arange(count, dtype=jnp.float32)
    return jnp.log(1.0 - 2.0 ** (-5.0 - head_ids))


def rotate(heads_in, positions):
    width = heads_in.shape[-1]
    half = width // 2
    freqs = 10000.0 ** (-jnp.arange(half, dtype=jnp.float32) / half)
    angles = positions[:, None] * freqs[None, :]
    cosine = jnp.cos(angles)
    sine = jnp.sin(angles)
    first_half = heads_in[..., :half]
    second_half = heads_in[..., half:]
    return jnp.concatenate(
        [first_half * cosine - second_half * sine, first_half * sine + second_half * cosine],
        axis=-1,
    )


def retention(queries, keys_in, values_in, log_gamma):
    head_count, length, key_width = queries.shape
    value_width = values_in.shape[-1]
    blocks = length // BLOCK
    queries = queries.reshape(head_count, blocks, BLOCK, key_width)
    keys_in = keys_in.reshape(head_count, blocks, BLOCK, key_width)
    values_in = values_in.reshape(head_count, blocks, BLOCK, value_width)
    offsets = jnp.arange(BLOCK, dtype=jnp.float32)
    distance = offsets[:, None] - offsets[None, :]
    weights = jnp.where(
        distance >= 0, jnp.exp(log_gamma[:, None, None] * jnp.maximum(distance, 0.0)), 0.0
    )
    scores = jnp.einsum("hbnd,hbmd->hbnm", queries, keys_in, precision=highest) * weights[:, None]
    inner = jnp.einsum("hbnm,hbme->hbne", scores, values_in, precision=highest)
    key_weight = jnp.exp(log_gamma[:, None] * (BLOCK - 1 - offsets)[None, :])
    contrib = jnp.einsum(
        "hbjd,hbje->hbde", keys_in * key_weight[:, None, :, None], values_in, precision=highest
    )
    block_decay = jnp.exp(log_gamma * BLOCK)[:, None, None]

    def advance(state, contrib_block):
        return (state * block_decay + contrib_block, state)

    _, states = lax.scan(
        advance,
        jnp.zeros((head_count, key_width, value_width), jnp.float32),
        jnp.moveaxis(contrib, 1, 0),
    )
    states = jnp.moveaxis(states, 0, 1)
    query_weight = jnp.exp(log_gamma[:, None] * (offsets + 1.0)[None, :])
    carried = (
        jnp.einsum("hbnd,hbde->hbne", queries, states, precision=highest)
        * query_weight[:, None, :, None]
    )
    return (inner + carried).reshape(head_count, length, value_width)


def head_norm(retained):
    return retained * lax.rsqrt(jnp.mean(retained * retained, axis=-1, keepdims=True) + 1e-06)


def causal_taps(values_in, taps):
    length = values_in.shape[-2]
    padded = jnp.pad(values_in.astype(jnp.float32), ((taps.shape[0] - 1, 0), (0, 0)))
    result = padded[0:length] * taps[0]
    for tap_index in range(1, taps.shape[0]):
        result = result + padded[tap_index : tap_index + length] * taps[tap_index]
    return result


def fold_single(source, weight_piece):
    return jnp.dot(source, weight_piece, preferred_element_type=jnp.float32)


def collect_single(source, weight):
    return fold_single(source, lax.all_gather(weight, "fs", axis=0, tiled=True))


def plain_body(
    tokens,
    norm_gain,
    w_query,
    w_key,
    w_value,
    w_gate,
    mixer_gain,
    w_out,
    channel_gain,
    w_left,
    w_right,
    taps_left,
    taps_right,
    w_down,
):
    length = tokens.shape[0]
    normed = scale_rows(tokens, norm_gain)
    queries = collect_single(normed, w_query)
    keys_proj = collect_single(normed, w_key)
    values_proj = collect_single(normed, w_value)
    gates = collect_single(normed, w_gate)
    queries = queries.astype(jnp.bfloat16)
    keys_proj = keys_proj.astype(jnp.bfloat16)
    values_proj = values_proj.astype(jnp.bfloat16)
    gates = gates.astype(jnp.bfloat16)
    heads_here = w_query.shape[1] // DK
    first_head = (lax.axis_index("tp") * heads_here).astype(jnp.float32)
    log_gamma = decays(first_head, heads_here)
    positions = jnp.arange(length, dtype=jnp.float32)

    def split_heads(rows_in, width):
        return rows_in.astype(jnp.float32).reshape(length, heads_here, width).transpose(1, 0, 2)

    retained = head_norm(
        retention(
            rotate(split_heads(queries, DK), positions),
            rotate(split_heads(keys_proj, DK), positions),
            split_heads(values_proj, DV),
            log_gamma,
        )
    )
    retained = retained.transpose(1, 0, 2).reshape(length, heads_here * DV)
    hidden = (retained * mixer_gain * jax.nn.silu(gates.astype(jnp.float32))).astype(jnp.bfloat16)
    rows_own = length // lax.axis_size("tp")
    first_row = lax.axis_index("tp") * rows_own
    out_whole = lax.all_gather(w_out, "fs", axis=1, tiled=True)
    mixer_total = lax.psum_scatter(
        jnp.dot(hidden, out_whole, preferred_element_type=jnp.float32).astype(jnp.bfloat16),
        "tp",
        scatter_dimension=0,
        tiled=True,
    ).astype(jnp.float32)
    residual = lax.dynamic_slice_in_dim(tokens, first_row, rows_own, 0)
    middle_own = (residual.astype(jnp.float32) + mixer_total).astype(jnp.bfloat16)
    middle = lax.all_gather(middle_own, "tp", axis=0, tiled=True)
    normed_mid = scale_rows(middle, channel_gain)
    left = collect_single(normed_mid, w_left)
    right = collect_single(normed_mid, w_right)
    left = left.astype(jnp.bfloat16)
    right = right.astype(jnp.bfloat16)
    gated = (jax.nn.silu(causal_taps(left, taps_left)) * causal_taps(right, taps_right)).astype(
        jnp.bfloat16
    )
    down_whole = lax.all_gather(w_down, "fs", axis=1, tiled=True)
    channel_part = jnp.dot(gated, down_whole, preferred_element_type=jnp.float32)
    channel_total = lax.psum(channel_part.astype(jnp.bfloat16), "tp").astype(jnp.float32)
    return (middle.astype(jnp.float32) + channel_total).astype(jnp.bfloat16)


def log_gammas(head_count):
    table = np.log(1.0 - 2.0 ** (-5.0 - np.arange(head_count, dtype=np.float64)))
    return np.repeat(table[:, None], BLOCK, axis=1).astype(np.float32)


def turning(length, width):
    half = width // 2
    freqs = np.float32(10000.0) ** (-np.arange(half, dtype=np.float32) / np.float32(half))
    angles = (np.arange(length, dtype=np.float32)[:, None] * freqs[None, :]).astype(np.float64)
    cosine, sine = np.cos(angles), np.sin(angles)
    return (
        np.concatenate([cosine, cosine], axis=1).astype(np.float32),
        np.concatenate([-sine, sine], axis=1).astype(np.float32),
    )


def silu(v):
    return v / (1.0 + jnp.exp(-v))


def normed_rows(floats, gain):
    factor = lax.rsqrt(jnp.mean(floats * floats, axis=-1, keepdims=True) + 1e-06)
    return (floats * factor * gain).astype(jnp.bfloat16)


HOP, SUM, SWAP, WEIGHTS, HOPS, CORES = 3, 4, 5, 6, 7, 8
CHUNKS = 4
NT_PARTS = 2
CLASS_OF = (0, 0, 0, 1, 2, 3, 4, 5)
STAGES = (
    (7, 0),
    (0, 0),
    (0, 1),
    (1, 0),
    (1, 1),
    (8, 0),
    (8, 1),
    (2, 0),
    (2, 1),
    (2, 2),
    (2, 3),
    (3, 0),
    (3, 1),
    (3, 2),
    (3, 3),
    (4, 0),
    (5, 0),
    (4, 1),
    (5, 1),
    (4, 2),
    (5, 2),
    (4, 3),
    (5, 3),
    (6, 0),
    (6, 1),
    (6, 2),
    (6, 3),
)
PLAN = (
    (
        (
            (1, 2, 1, 3), (1, 2, 2, 3), (1, 2, 0, 3), (1, 2, 3, 3), (1, 3, 3, 0, 0), (1, 3, 3, 0, 3), (1, 3, 0, 0, 0),
            (1, 3, 2, 0, 0), (1, 3, 2, 0, 1), (1, 3, 4, 0, 0), (0, 6, 1, 1), (1, 3, 1, 1, 3), (1, 3, 1, 1, 1),
            (1, 3, 0, 0, 2), (1, 2, 3, 1),
        ),
        (
            (1, 0, 0, 1, 0, 0), (1, 1, 0, 0, 0, 0), (1, 1, 0, 1, 0, 0), (1, 3, 5, 0, 0), (1, 2, 1, 1), (0, 6, 0, 3),
            (1, 3, 0, 3, 1), (1, 3, 0, 3, 0), (1, 3, 0, 3, 2), (1, 3, 2, 0, 2), (1, 3, 2, 0, 3), (1, 0, 0, 0, 0, 0),
            (1, 3, 0, 0, 1), (0, 6, 2, 1), (1, 3, 2, 1, 1), (1, 3, 0, 3, 3), (0, 3, 1, 1, 1), (0, 3, 2, 0, 1),
            (0, 6, 1, 3), (1, 2, 0, 1), (1, 3, 1, 3, 1), (0, 3, 3, 0, 0), (0, 6, 0, 1), (1, 3, 0, 1, 1),
            (1, 3, 3, 0, 4), (1, 3, 2, 1, 0), (1, 3, 1, 3, 0), (1, 3, 0, 1, 3), (1, 3, 1, 1, 0), (1, 3, 4, 0, 1),
            (1, 3, 2, 1, 2), (0, 3, 0, 3, 1), (1, 3, 0, 3, 5), (1, 3, 0, 1, 0), (0, 3, 2, 0, 0), (1, 2, 4, 3),
            (0, 3, 1, 3, 1), (1, 2, 2, 1), (1, 2, 4, 1), (1, 3, 1, 0, 0), (1, 2, 5, 1), (1, 3, 1, 1, 5),
            (0, 3, 0, 0, 1), (1, 3, 2, 1, 3), (1, 3, 0, 0, 3), (0, 6, 1, 2), (1, 3, 1, 2, 2), (1, 3, 1, 0, 3),
            (1, 3, 1, 0, 1), (0, 3, 0, 0, 0), (1, 3, 1, 2, 0), (0, 3, 2, 1, 0), (1, 3, 2, 1, 4), (1, 3, 1, 2, 3),
            (1, 3, 1, 2, 1), (1, 3, 5, 0, 3), (1, 2, 3, 2), (1, 3, 0, 1, 2), (1, 3, 1, 3, 2), (0, 6, 4, 1),
            (0, 6, 2, 3), (1, 3, 2, 3, 3), (1, 3, 2, 3, 1), (1, 3, 2, 3, 0), (1, 3, 0, 0, 5), (0, 0, 0, 0, 1, 1),
            (0, 3, 1, 1, 0), (1, 3, 2, 3, 2), (1, 3, 4, 1, 2), (0, 6, 3, 1), (1, 3, 3, 1, 2), (1, 3, 2, 0, 4),
            (1, 3, 5, 0, 2), (1, 2, 1, 2), (1, 2, 0, 2), (1, 3, 1, 3, 3), (0, 3, 0, 3, 0), (1, 3, 4, 1, 3),
            (1, 3, 0, 3, 4), (1, 3, 4, 1, 0), (1, 3, 0, 0, 4), (1, 2, 2, 2), (1, 3, 1, 0, 2), (1, 3, 1, 3, 5),
            (1, 2, 4, 2), (0, 6, 0, 2), (1, 3, 0, 2, 1), (1, 3, 0, 2, 0), (1, 3, 0, 2, 3), (0, 3, 0, 1, 0),
            (1, 3, 2, 0, 5), (1, 3, 0, 1, 4), (0, 3, 1, 2, 1), (1, 3, 1, 2, 5), (1, 2, 5, 2), (1, 3, 0, 2, 2),
            (0, 6, 2, 2), (1, 3, 2, 2, 1), (1, 2, 7, 1), (1, 2, 6, 1), (0, 0, 0, 0, 1, 2), (1, 1, 0, 0, 1, 2),
            (1, 1, 0, 0, 1, 1), (1, 3, 2, 2, 3), (1, 3, 2, 2, 0), (0, 3, 0, 1, 1), (1, 3, 0, 1, 5), (0, 3, 0, 2, 1),
            (0, 3, 0, 2, 0), (1, 3, 0, 2, 4), (1, 3, 0, 2, 5), (0, 3, 1, 3, 0), (1, 3, 1, 3, 4), (0, 0, 0, 0, 1, 3),
            (0, 3, 2, 3, 1), (0, 3, 2, 2, 0), (1, 2, 7, 3), (1, 2, 6, 3), (0, 3, 1, 0, 0), (1, 3, 1, 0, 4),
            (1, 3, 2, 2, 4), (0, 0, 0, 1, 1, 1), (1, 3, 2, 3, 5), (1, 1, 0, 1, 1, 1), (1, 3, 1, 1, 4),
            (0, 3, 1, 0, 1), (1, 3, 1, 0, 5), (0, 3, 2, 2, 1), (1, 3, 2, 2, 5), (0, 3, 2, 3, 0), (1, 3, 2, 3, 4),
            (0, 0, 0, 1, 1, 2), (1, 1, 0, 1, 1, 2), (1, 3, 1, 1, 2), (0, 3, 2, 1, 1), (1, 3, 2, 1, 5),
            (1, 3, 2, 2, 2), (0, 3, 1, 2, 0), (1, 3, 1, 2, 4), (1, 3, 4, 0, 3), (1, 1, 0, 0, 1, 3), (1, 2, 7, 2),
            (1, 2, 5, 3), (0, 6, 5, 1), (1, 3, 5, 1, 0), (1, 3, 5, 1, 1), (1, 3, 3, 1, 1), (0, 3, 4, 0, 1),
            (1, 3, 4, 0, 5), (1, 3, 3, 0, 1), (0, 0, 0, 1, 1, 3), (1, 1, 0, 1, 1, 3), (0, 8, 0, 0), (0, 7, 0),
        ),
        (
        ),
        (
        ),
        (
        ),
        (
            (0, 7, 1),
        ),
        (
            (0, 7, 2),
        ),
        (
        ),
        (
            (0, 6, 5, 3), (1, 3, 5, 3, 0), (1, 3, 5, 3, 1),
        ),
        (
            (1, 3, 3, 1, 0), (0, 6, 3, 2), (0, 6, 4, 3), (1, 3, 4, 3, 2), (1, 3, 3, 2, 1), (1, 3, 4, 3, 0),
            (1, 3, 4, 3, 3),
        ),
        (
            (0, 3, 5, 0, 0), (1, 3, 5, 0, 4), (1, 3, 3, 0, 2), (1, 3, 5, 1, 2), (0, 5, 0, 0), (1, 4, 0, 0, 0, 2),
            (0, 3, 5, 1, 0),
        ),
        (
            (1, 4, 0, 0, 0, 3), (1, 3, 3, 2, 3), (0, 5, 0, 3), (1, 4, 0, 3, 0, 3), (1, 4, 0, 0, 0, 1),
            (1, 3, 3, 2, 0), (1, 3, 3, 1, 3), (1, 3, 5, 3, 2), (0, 5, 0, 1), (0, 3, 4, 1, 0), (1, 3, 4, 1, 4),
            (0, 3, 3, 2, 1), (1, 3, 3, 2, 5), (0, 6, 3, 3), (1, 3, 3, 3, 0), (1, 3, 3, 3, 3), (1, 4, 0, 1, 0, 3),
            (1, 3, 3, 3, 2), (1, 4, 0, 1, 0, 2), (0, 6, 4, 2), (1, 3, 4, 2, 1), (0, 3, 4, 3, 0), (1, 3, 4, 3, 4),
            (1, 3, 4, 2, 0), (1, 3, 4, 3, 1), (1, 3, 4, 1, 1), (1, 3, 4, 2, 3), (0, 3, 3, 0, 1), (0, 6, 5, 2),
            (1, 3, 5, 2, 3), (0, 5, 0, 2), (1, 4, 0, 2, 0, 3), (1, 4, 0, 3, 0, 2), (1, 3, 3, 3, 1), (1, 3, 5, 2, 1),
            (1, 3, 5, 0, 1), (1, 3, 5, 2, 0), (1, 4, 0, 1, 0, 1), (0, 3, 5, 3, 1), (1, 3, 5, 3, 5), (0, 3, 5, 1, 1),
            (1, 3, 5, 1, 5), (1, 3, 5, 1, 3), (0, 3, 3, 1, 0), (1, 3, 3, 2, 2), (1, 4, 0, 2, 0, 2),
            (0, 4, 0, 0, 1, 0),
        ),
        (
            (1, 0, 1, 0, 0, 0), (0, 3, 4, 1, 1), (1, 3, 5, 3, 3), (0, 3, 5, 3, 0), (1, 3, 5, 3, 4), (0, 3, 4, 2, 0),
            (1, 1, 1, 0, 0, 0), (1, 3, 4, 1, 5), (1, 3, 4, 0, 2), (1, 4, 0, 3, 0, 1), (0, 3, 5, 2, 0),
            (1, 3, 4, 2, 4), (1, 3, 5, 2, 4), (0, 3, 3, 1, 1), (1, 3, 3, 1, 5), (1, 4, 0, 2, 0, 1),
            (0, 4, 0, 1, 1, 0),
        ),
        (
            (1, 0, 1, 1, 0, 0), (1, 2, 6, 2), (1, 1, 1, 1, 0, 0), (1, 3, 5, 2, 2), (1, 3, 3, 0, 5), (0, 3, 4, 0, 0),
            (1, 3, 4, 0, 4), (0, 3, 4, 3, 1), (0, 3, 3, 3, 0), (1, 3, 4, 3, 5), (0, 3, 4, 2, 1), (0, 4, 0, 2, 1, 0),
        ),
        (
            (1, 0, 1, 2, 0, 0), (1, 3, 4, 2, 2), (0, 3, 5, 2, 1), (1, 3, 5, 2, 5), (0, 0, 1, 1, 1, 1),
            (1, 1, 1, 1, 1, 1), (0, 3, 3, 2, 0), (1, 3, 4, 2, 5), (1, 3, 3, 1, 4), (0, 3, 3, 3, 1), (1, 3, 3, 3, 5),
            (0, 4, 0, 3, 1, 0), (1, 3, 3, 3, 4),
        ),
        (
            (1, 0, 1, 3, 0, 0), (1, 3, 3, 2, 4), (0, 3, 5, 0, 1), (1, 3, 5, 0, 5), (0, 0, 1, 0, 1, 2),
            (1, 1, 1, 0, 1, 2), (1, 3, 5, 1, 4), (0, 0, 1, 0, 1, 1), (1, 1, 1, 0, 1, 1), (0, 0, 1, 0, 1, 3),
            (1, 1, 1, 0, 1, 3), (0, 0, 1, 1, 1, 2), (1, 1, 1, 1, 1, 2), (0, 0, 1, 3, 1, 1), (1, 1, 1, 3, 1, 1),
            (1, 1, 1, 3, 0, 0), (0, 8, 1, 0), (0, 7, 3), (0, 7, 4),
        ),
        (
            (0, 7, 5),
        ),
        (
            (0, 0, 1, 1, 1, 3), (1, 1, 1, 1, 1, 3), (1, 1, 1, 2, 0, 0), (0, 0, 1, 2, 1, 2), (1, 1, 1, 2, 1, 2),
            (0, 5, 1, 0), (1, 4, 1, 0, 0, 2), (0, 8, 1, 1),
        ),
        (
            (0, 0, 1, 2, 1, 1),
        ),
        (
            (1, 4, 1, 0, 0, 3), (1, 1, 1, 2, 1, 1), (1, 4, 1, 0, 0, 1), (0, 0, 1, 2, 1, 3), (1, 1, 1, 2, 1, 3),
            (0, 0, 1, 3, 1, 2), (1, 1, 1, 3, 1, 2), (0, 5, 1, 1), (1, 4, 1, 1, 0, 3), (1, 4, 1, 1, 0, 2),
            (0, 0, 1, 3, 1, 3), (1, 1, 1, 3, 1, 3), (0, 8, 1, 2),
        ),
        (
        ),
        (
            (0, 8, 1, 3),
        ),
        (
        ),
        (
            (0, 5, 1, 2), (1, 4, 1, 2, 0, 3), (0, 5, 1, 3), (1, 4, 1, 3, 0, 3), (1, 4, 1, 2, 0, 2),
            (1, 4, 1, 3, 0, 2), (0, 4, 1, 0, 1, 0),
        ),
        (
            (1, 4, 1, 3, 0, 1), (1, 4, 1, 1, 0, 1), (1, 4, 1, 2, 0, 1), (0, 4, 1, 1, 1, 0),
        ),
        (
            (0, 4, 1, 2, 1, 0),
        ),
        (
            (0, 4, 1, 3, 1, 0),
        ),
        (
        ),
    ),
    (
        (
            (1, 3, 5, 1, 0), (1, 3, 5, 1, 1), (1, 3, 5, 1, 3), (1, 3, 1, 1, 0), (1, 3, 1, 1, 1), (1, 3, 2, 1, 0),
            (1, 3, 2, 1, 3), (1, 3, 0, 1, 0), (1, 3, 0, 1, 3), (1, 3, 2, 1, 2), (1, 3, 5, 1, 2), (1, 3, 1, 1, 3),
            (1, 2, 4, 2), (1, 2, 3, 0), (1, 2, 0, 0), (1, 3, 4, 1, 0), (1, 2, 2, 2), (1, 3, 2, 1, 1),
        ),
        (
            (1, 2, 4, 0), (1, 2, 2, 0), (1, 0, 0, 1, 0, 0), (1, 3, 3, 1, 0), (0, 6, 2, 2), (1, 3, 2, 2, 2),
            (1, 3, 2, 2, 1), (1, 3, 3, 1, 1), (1, 2, 0, 2), (1, 3, 0, 1, 2), (1, 2, 1, 0), (1, 2, 3, 2),
            (1, 3, 2, 2, 3), (1, 2, 1, 2), (1, 3, 0, 1, 1), (1, 0, 0, 1, 1, 0), (0, 6, 1, 0), (1, 3, 1, 0, 2),
            (1, 3, 1, 0, 0), (1, 0, 0, 0, 0, 0), (0, 3, 2, 1, 0), (1, 3, 2, 2, 0), (1, 3, 1, 1, 2),
            (1, 0, 0, 0, 1, 0), (1, 2, 3, 3), (0, 3, 2, 1, 1), (0, 6, 0, 2), (1, 3, 0, 2, 3), (1, 3, 1, 0, 1),
            (1, 3, 0, 2, 1), (1, 3, 0, 2, 2), (1, 3, 2, 1, 4), (1, 3, 0, 2, 0), (0, 0, 0, 0, 0, 1), (1, 2, 5, 0),
            (0, 0, 0, 1, 0, 1), (1, 0, 0, 1, 0, 1), (1, 0, 0, 0, 0, 1), (0, 6, 1, 2), (1, 3, 1, 2, 2), (1, 2, 6, 0),
            (0, 3, 0, 1, 1), (1, 3, 1, 2, 3), (0, 3, 4, 1, 0), (0, 3, 0, 1, 0), (0, 3, 5, 1, 1), (0, 3, 1, 0, 0),
            (1, 3, 2, 1, 5), (1, 3, 0, 1, 5), (0, 0, 0, 1, 1, 1), (1, 0, 0, 1, 1, 1), (1, 1, 0, 1, 1, 1),
            (0, 0, 0, 0, 1, 1), (0, 6, 0, 0), (1, 0, 0, 0, 1, 1), (1, 3, 0, 0, 2), (1, 3, 0, 0, 0), (1, 3, 4, 1, 1),
            (0, 6, 2, 0), (0, 3, 0, 2, 1), (1, 3, 0, 2, 5), (0, 3, 2, 2, 0), (1, 3, 0, 0, 1), (1, 3, 2, 0, 0),
            (1, 2, 0, 3), (1, 3, 2, 2, 4), (1, 2, 2, 3), (0, 3, 4, 1, 1), (0, 3, 0, 2, 0), (1, 3, 0, 2, 4),
            (1, 2, 1, 3), (1, 3, 0, 1, 4), (1, 3, 1, 2, 1), (1, 3, 1, 2, 0), (1, 2, 4, 3), (0, 3, 0, 0, 1),
            (0, 6, 1, 3), (1, 3, 1, 3, 1), (1, 3, 4, 1, 3), (1, 3, 4, 1, 2), (1, 3, 1, 3, 0), (1, 3, 1, 0, 4),
            (1, 3, 1, 3, 3), (1, 3, 0, 0, 3), (0, 0, 0, 0, 1, 2), (1, 0, 0, 0, 1, 2), (1, 3, 1, 3, 2),
            (0, 3, 1, 2, 0), (0, 6, 0, 3), (1, 3, 0, 3, 0), (1, 3, 0, 3, 3), (0, 0, 0, 1, 1, 2), (1, 3, 0, 3, 1),
            (0, 3, 1, 0, 1), (1, 3, 1, 0, 5), (1, 1, 0, 1, 0, 0), (1, 2, 7, 0), (1, 0, 0, 1, 1, 2), (1, 3, 0, 3, 2),
            (1, 3, 2, 0, 1), (1, 2, 5, 2), (0, 3, 0, 0, 0), (0, 6, 2, 3), (1, 3, 2, 3, 1), (1, 3, 2, 3, 0),
            (1, 3, 2, 0, 3), (1, 2, 6, 2), (1, 2, 5, 3), (0, 3, 1, 1, 1), (1, 3, 1, 1, 5), (0, 3, 2, 2, 1),
            (1, 3, 0, 0, 4), (1, 3, 2, 2, 5), (1, 3, 0, 0, 5), (0, 6, 3, 3), (0, 3, 0, 3, 1), (1, 3, 0, 3, 5),
            (0, 6, 3, 0), (0, 6, 3, 2), (1, 3, 3, 3, 0), (1, 3, 5, 1, 5), (0, 3, 2, 3, 1), (0, 3, 2, 0, 1),
            (1, 3, 2, 0, 5), (0, 3, 1, 3, 0), (1, 3, 2, 3, 3), (0, 3, 2, 3, 0), (1, 3, 2, 3, 4), (0, 3, 2, 0, 0),
            (1, 3, 2, 0, 4), (1, 3, 1, 0, 3), (0, 3, 0, 3, 0), (1, 3, 0, 3, 4), (0, 3, 1, 2, 1), (0, 3, 1, 3, 1),
            (1, 3, 1, 3, 5), (1, 3, 1, 2, 5), (0, 6, 5, 0), (1, 3, 1, 3, 4), (1, 3, 5, 0, 0), (1, 3, 2, 0, 2),
            (1, 3, 1, 2, 4), (1, 1, 0, 1, 1, 2), (1, 3, 3, 0, 1), (1, 3, 2, 3, 2), (0, 3, 1, 1, 0), (1, 3, 1, 1, 4),
            (1, 1, 0, 0, 0, 0), (1, 1, 0, 0, 1, 2), (1, 1, 0, 1, 0, 1), (1, 1, 0, 0, 1, 1), (1, 1, 0, 0, 0, 1),
            (0, 8, 0, 0), (1, 3, 2, 3, 5), (1, 3, 3, 0, 2), (0, 7, 0), (0, 6, 4, 0), (1, 3, 4, 0, 2), (1, 3, 5, 0, 2),
        ),
        (
        ),
        (
            (1, 2, 7, 2), (1, 2, 6, 3), (1, 3, 3, 2, 1), (1, 3, 4, 0, 3), (1, 3, 4, 0, 1), (1, 3, 4, 0, 0),
            (0, 6, 4, 2),
        ),
        (
            (1, 3, 4, 2, 1), (1, 3, 4, 2, 2), (0, 3, 3, 1, 1), (1, 3, 5, 0, 3), (0, 3, 5, 0, 0),
        ),
        (
            (0, 6, 5, 3), (1, 3, 5, 3, 0), (1, 3, 5, 3, 2), (1, 3, 5, 3, 1), (0, 7, 1), (1, 3, 4, 2, 0),
            (1, 3, 3, 3, 1),
        ),
        (
        ),
        (
            (1, 3, 3, 2, 0), (0, 7, 2),
        ),
        (
            (1, 2, 7, 3), (1, 3, 3, 0, 3), (1, 3, 5, 0, 1), (0, 6, 5, 2), (1, 3, 5, 2, 1),
        ),
        (
        ),
        (
            (0, 4, 0, 0, 0, 1), (0, 5, 0, 0), (1, 4, 0, 0, 0, 1), (0, 5, 0, 1), (1, 3, 3, 0, 0),
        ),
        (
            (0, 4, 0, 0, 0, 2), (1, 4, 0, 0, 0, 2), (1, 3, 5, 2, 2), (1, 3, 3, 3, 2), (0, 5, 0, 3), (0, 5, 0, 2),
            (1, 3, 5, 2, 0), (1, 3, 5, 3, 3), (0, 4, 0, 3, 0, 2), (0, 3, 5, 3, 0), (1, 4, 0, 3, 0, 2),
            (0, 4, 0, 0, 0, 0), (0, 4, 0, 0, 1, 0),
        ),
        (
            (1, 0, 1, 0, 0, 0), (0, 4, 0, 0, 1, 1), (1, 4, 0, 0, 1, 1), (1, 0, 1, 0, 1, 0), (0, 4, 0, 1, 0, 2),
            (1, 3, 3, 2, 2), (1, 4, 0, 1, 0, 2), (1, 3, 5, 3, 4), (0, 3, 3, 1, 0), (1, 3, 3, 1, 4), (0, 3, 3, 0, 0),
            (0, 3, 4, 2, 0), (0, 3, 3, 0, 1), (0, 3, 5, 1, 0), (1, 3, 5, 2, 3), (0, 4, 0, 3, 1, 1), (0, 3, 4, 2, 1),
            (0, 4, 0, 1, 0, 1), (1, 4, 0, 1, 0, 1), (1, 3, 5, 1, 4), (1, 4, 0, 3, 1, 1), (0, 4, 0, 2, 0, 2),
            (1, 4, 0, 2, 0, 2), (1, 3, 4, 1, 5), (1, 3, 4, 2, 3), (0, 4, 0, 3, 0, 1), (1, 4, 0, 3, 0, 1),
            (0, 4, 0, 1, 1, 1), (1, 4, 0, 1, 1, 1), (0, 4, 0, 1, 1, 0), (0, 3, 3, 3, 0), (0, 4, 0, 1, 0, 0),
        ),
        (
            (1, 0, 1, 1, 0, 0), (1, 0, 1, 1, 1, 0), (0, 3, 5, 2, 0), (1, 3, 3, 2, 3), (0, 3, 3, 3, 1),
            (0, 3, 5, 2, 1), (1, 3, 5, 2, 5), (1, 3, 4, 2, 5), (1, 3, 4, 1, 4), (0, 4, 0, 2, 0, 1),
            (1, 4, 0, 2, 0, 1), (1, 3, 4, 2, 4), (0, 3, 3, 2, 1), (1, 3, 3, 2, 5), (0, 4, 0, 2, 1, 1),
            (1, 4, 0, 2, 1, 1), (1, 3, 3, 3, 5), (0, 3, 3, 2, 0), (1, 3, 5, 2, 4), (0, 0, 1, 0, 0, 1),
            (1, 0, 1, 0, 0, 1), (1, 3, 3, 2, 4), (1, 3, 3, 1, 5), (1, 3, 3, 3, 4), (0, 0, 1, 0, 1, 1),
            (1, 0, 1, 0, 1, 1), (0, 0, 1, 1, 1, 1), (1, 0, 1, 1, 1, 1), (1, 1, 1, 0, 1, 1), (1, 3, 5, 0, 4),
            (0, 4, 0, 2, 1, 0), (1, 3, 3, 0, 5), (0, 3, 5, 3, 1), (1, 3, 5, 3, 5), (0, 3, 4, 0, 0), (1, 3, 4, 0, 4),
            (1, 1, 1, 0, 0, 0), (0, 4, 0, 2, 0, 0),
        ),
        (
            (1, 0, 1, 2, 1, 0), (1, 1, 1, 2, 0, 0), (0, 0, 1, 1, 0, 1), (1, 0, 1, 1, 0, 1), (0, 0, 1, 0, 1, 2),
            (1, 0, 1, 0, 1, 2), (1, 1, 1, 0, 0, 1), (1, 1, 1, 1, 0, 1), (0, 4, 0, 3, 0, 0), (0, 4, 0, 3, 1, 0),
        ),
        (
            (1, 1, 1, 1, 1, 1), (1, 0, 1, 2, 0, 0), (1, 3, 3, 0, 4), (1, 0, 1, 3, 0, 0), (1, 0, 1, 3, 1, 0),
            (0, 6, 4, 3), (1, 3, 4, 3, 1), (1, 3, 4, 3, 0), (1, 1, 1, 3, 0, 0), (1, 3, 3, 1, 2), (1, 3, 4, 3, 2),
            (1, 3, 3, 1, 3), (0, 3, 4, 0, 1), (1, 3, 4, 0, 5), (0, 0, 1, 2, 0, 1), (1, 1, 1, 2, 0, 1),
            (1, 0, 1, 2, 0, 1), (0, 0, 1, 1, 1, 2), (1, 0, 1, 1, 1, 2), (1, 3, 3, 3, 3), (0, 0, 1, 3, 0, 1),
            (1, 1, 1, 3, 0, 1), (1, 0, 1, 3, 0, 1), (0, 0, 1, 2, 1, 1), (1, 0, 1, 2, 1, 1), (1, 1, 1, 2, 1, 1),
            (1, 3, 4, 3, 3), (0, 3, 4, 3, 0), (1, 3, 4, 3, 4), (1, 1, 1, 1, 0, 0), (0, 0, 1, 3, 1, 1),
            (1, 0, 1, 3, 1, 1), (0, 3, 4, 3, 1), (1, 3, 4, 3, 5), (0, 3, 5, 0, 1), (1, 3, 5, 0, 5),
            (1, 1, 1, 1, 1, 2), (1, 1, 1, 3, 1, 1), (0, 0, 1, 2, 1, 2), (1, 1, 1, 2, 1, 2), (1, 0, 1, 2, 1, 2),
            (0, 0, 1, 3, 1, 2), (1, 1, 1, 3, 1, 2), (1, 0, 1, 3, 1, 2), (0, 7, 3), (1, 1, 1, 0, 1, 2), (0, 8, 1, 0),
            (0, 7, 4),
        ),
        (
            (0, 7, 5),
        ),
        (
            (0, 8, 1, 1),
        ),
        (
            (0, 5, 1, 0), (0, 4, 1, 0, 0, 1), (0, 4, 1, 0, 0, 2), (1, 4, 1, 0, 0, 2),
        ),
        (
            (1, 4, 1, 0, 0, 1), (0, 8, 1, 2),
        ),
        (
        ),
        (
            (0, 5, 1, 1), (0, 4, 1, 1, 0, 2), (1, 4, 1, 1, 0, 2), (0, 8, 1, 3),
        ),
        (
            (0, 4, 1, 0, 1, 1), (1, 4, 1, 0, 1, 1), (0, 4, 1, 1, 0, 1), (1, 4, 1, 1, 0, 1),
        ),
        (
            (0, 4, 1, 2, 0, 2), (0, 5, 1, 2), (1, 4, 1, 2, 0, 2), (0, 4, 1, 1, 1, 1), (1, 4, 1, 1, 1, 1),
            (0, 5, 1, 3), (0, 4, 1, 3, 0, 2), (1, 4, 1, 3, 0, 2), (0, 4, 1, 2, 0, 1), (1, 4, 1, 2, 0, 1),
            (0, 4, 1, 0, 0, 0), (0, 4, 1, 2, 1, 1), (1, 4, 1, 2, 1, 1), (0, 4, 1, 1, 1, 0), (0, 4, 1, 3, 1, 1),
            (1, 4, 1, 3, 1, 1), (0, 4, 1, 3, 0, 1), (1, 4, 1, 3, 0, 1), (0, 4, 1, 0, 1, 0),
        ),
        (
            (0, 4, 1, 1, 0, 0),
        ),
        (
            (0, 4, 1, 2, 1, 0), (0, 4, 1, 2, 0, 0),
        ),
        (
            (0, 4, 1, 3, 0, 0), (0, 4, 1, 3, 1, 0),
        ),
        (
        ),
    ),
)

OWN_FIRST = {}
for at, ops in enumerate(PLAN):
    for op in (op for stage in ops for op in stage):
        if op[:2] == (1, HOP) and op[3] == at:
            OWN_FIRST.setdefault((op[2], at), op[4])


def layer_kernel(
    n_fs,
    groups,
    tokens_in,
    norm_gain_in,
    wq,
    wk,
    wv,
    wg,
    mixer_gain_in,
    wo,
    channel_gain_in,
    wl,
    wr,
    taps_left_in,
    taps_right_in,
    wd,
    cos_in,
    sin_in,
    gammas_in,
    out,
    tokens,
    norm_gain,
    mixer_gain,
    channel_gain,
    taps_left,
    taps_right,
    cos_t,
    sin_t,
    gammas,
    w1,
    wout,
    wlr,
    wdown,
    nt,
    nm,
    qkvg,
    held_kept,
    hid,
    gated,
    part1,
    part2,
    xb1,
    xb2,
    sb1,
    sb2,
    rb1,
    rb2,
    mid,
    acc,
    both,
    fin,
    w_send,
    w_recv,
    self_sem,
    h_send,
    h_recv,
    h_rest,
    a_send,
    a_recv,
    f_send,
    f_recv,
    x_send,
    x_recv,
    r_send,
    r_recv,
    o_send,
    o_recv,
    load_sem,
    store_sem,
):
    fs, tp = lax.axis_index("fs"), lax.axis_index("tp")
    planes = n_fs // groups
    z, q = fs // planes, lax.rem(fs, planes)
    other = 1 - tp
    length, width = tokens_in.shape
    own = length // 2
    part_rows = own // NT_PARTS
    span_c = length // CHUNKS
    few = span_c // 2
    kb = wq.shape[0]
    nb = wo.shape[1]
    cq, cv, cf = wq.shape[1] // groups, wv.shape[1] // groups, wl.shape[1] // groups
    upper = z * 2 >= groups
    place_z = jnp.where(upper, groups - 1 - z, z)

    def real(plane):
        return jnp.where(upper, groups - 1 - plane, plane)

    def flip(side):
        return jnp.where(upper, 1 - side, side)

    def zdev(target):
        return {"fs": target * planes + q, "tp": tp}

    partner = {"fs": fs, "tp": other}

    def lanes(index, size):
        return pl.ds(pl.multiple_of(index * size, 128), size)

    def rows(index, size):
        return pl.ds(pl.multiple_of(index * size, size), size)

    pieces = (
        (lambda c: wq.at[:, lanes(c, cq)], lambda f: w1.at[rows(f, kb), pl.ds(0, cq)]),
        (lambda c: wk.at[:, lanes(c, cq)], lambda f: w1.at[rows(f, kb), pl.ds(cq, cq)]),
        (lambda c: wv.at[:, lanes(c, cv)], lambda f: w1.at[rows(f, kb), pl.ds(2 * cq, cv)]),
        (lambda c: wg.at[:, lanes(c, cv)], lambda f: w1.at[rows(f, kb), pl.ds(2 * cq + cv, cv)]),
        (lambda c: wo.at[rows(c, cv), :], lambda f: wout.at[:, lanes(f, nb)]),
        (lambda c: wl.at[:, lanes(c, cf)], lambda f: wlr.at[rows(f, kb), pl.ds(0, cf)]),
        (lambda c: wr.at[:, lanes(c, cf)], lambda f: wlr.at[rows(f, kb), pl.ds(cf, cf)]),
        (lambda c: wd.at[rows(c, cf), :], lambda f: wdown.at[:, lanes(f, nb)]),
    )
    starts = (0, cq, 2 * cq, 2 * cq + cv, 0, 0, cf, 0)
    widths = (cq, cq, cv, cv, 0, cf, cf, 0)

    def stretch(cls, first, count, half=None):
        members = [i for i in range(len(pieces)) if CLASS_OF[i] == cls]
        low = starts[members[0]]
        wide = sum(widths[i] for i in members)
        if members[0] == 4 or members[0] == 7:
            buf, size = (wout, cv) if members[0] == 4 else (wdown, cf)
            across = pl.ds(pl.multiple_of(first * nb, 128), count * nb)
            if half is None:
                return buf.at[:, across]
            return buf.at[pl.ds(half * (size // 2), size // 2), across]
        buf = w1 if members[0] < 4 else wlr
        if half is None:
            return buf.at[pl.ds(pl.multiple_of(first * kb, kb), count * kb), pl.ds(low, wide)]
        start = pl.multiple_of(first * kb + half * (kb // 2), kb // 2)
        return buf.at[pl.ds(start, kb // 2), pl.ds(low, wide)]

    barrier = pltpu.get_barrier_semaphore()
    for step in range(1, groups):
        pl.semaphore_signal(barrier, inc=1, device_id=zdev(lax.rem(z + step, groups)), device_id_type=MESH)
    qx = q + 1 - 2 * lax.rem(q, 2)
    qy = q + 2 - 4 * (q // 2)
    diagonal = planes - 1 - q
    to_x = {"fs": z * planes + qx, "tp": tp}
    to_y = {"fs": z * planes + qy, "tp": tp}
    for device in (to_x, to_y):
        pl.semaphore_signal(barrier, inc=1, device_id=device, device_id_type=MESH)
    pl.semaphore_signal(barrier, inc=1, device_id=partner, device_id_type=MESH)

    loads = []
    for i, (source, held_here) in enumerate((
        (tokens_in, tokens), (norm_gain_in, norm_gain), (mixer_gain_in, mixer_gain),
        (channel_gain_in, channel_gain), (taps_left_in, taps_left), (taps_right_in, taps_right),
        (cos_in, cos_t), (sin_in, sin_t), (gammas_in, gammas),
    )):
        load = pltpu.make_async_copy(source, held_here, load_sem.at[i])
        load.start()
        loads.append(load)
    keeps = []
    for i, (src, dst) in enumerate(pieces):
        keep = pltpu.make_async_copy(src(z), dst(fs), self_sem.at[i])
        keep.start()
        keeps.append(keep)

    def prepare(_):
        for load in loads:
            load.wait()
        my_half = pl.ds(pl.multiple_of(tp * own, own), own)
        nt[pl.ds(pl.multiple_of(z * length + tp * own, own), own), :] = normed_rows(
            tokens[my_half, :].astype(jnp.float32), norm_gain[...]
        )

    pl.semaphore_wait(barrier, groups - 1 + 2 + 1)

    def remote(src, dst, ssem, rsem, device):
        return pltpu.make_async_remote_copy(
            src_ref=src, dst_ref=dst, send_sem=ssem, recv_sem=rsem,
            device_id=device, device_id_type=MESH,
        )

    def block(key, c, seq, core):
        if key:
            first = c * groups * span_c + seq * span_c + core * few
            return nm.at[pl.ds(pl.multiple_of(first, few), few), :]
        first = seq * length + core * own + c * part_rows
        return nt.at[pl.ds(pl.multiple_of(first, part_rows), part_rows), :]

    part, xb, sb, rb = (part1, part2), (xb1, xb2), (sb1, sb2), (rb1, rb2)

    def pair(which, c, g):
        return part[which][c, tp, g].astype(jnp.float32) + xb[which][c, g].astype(jnp.float32)

    def exchange(which, c):
        return remote(part[which].at[c, other], xb[which].at[c], x_send.at[which], x_recv.at[c], partner)

    def gather_copy(me, key, c, side, d, landing=False):
        move = 1 - 2 * side
        source = real(me - move * d)
        ref = block(key, c, source, tp)
        at = c
        device = partner if landing else zdev(real(me + move))
        return remote(ref, ref, a_send.at[key], a_recv.at[at, source], device)

    def core_copy(me, key, c, side, d):
        move = 1 - 2 * side
        ref = block(key, c, real(me - move * d), tp)
        return remote(ref, ref, f_send.at[key], f_recv.at[key * (1 + c)], partner)

    def weight_copy(me, i, plane):
        src, dst = pieces[i]
        far = real(plane)
        return remote(src(far), dst(fs), w_send.at[i], w_recv.at[CLASS_OF[i], z], zdev(far))

    def hop_copy(me, cls, plane, slot, landing=False):
        origin = (qx, qy)[slot] if landing else (q, q, q, q, qx, qy)[slot]
        source = real(plane)
        ref = stretch(cls, source * planes + origin, 1, (0, 1, 1, 0, 0, 1)[slot])
        device = (to_x, to_y, to_x, to_y, to_y, to_x)[slot]
        landed = h_recv.at[cls, source, slot] if slot < 2 else h_rest.at[cls]
        return remote(ref, ref, h_send.at[cls], landed, device)

    def sum_copy(me, which, c, side, d, landing=False):
        ref = sb[which].at[c, flip(side), d]
        at = d if landing else d - 1
        device = partner if landing else zdev(real(me + 1 - 2 * side))
        return remote(ref, rb[which].at[c, flip(side), at], r_send.at[which], r_recv.at[c, flip(side), at], device)

    makers = (gather_copy, core_copy, weight_copy, hop_copy, sum_copy)

    def await_bytes(ref, sem):
        remote(ref, ref, sem, sem, partner).wait_recv()

    def act(me, op):
        sends, kind, args = op[0], op[1], op[2:]
        if not sends:
            if kind == SWAP:
                exchange(*args).wait_recv()
            elif kind == WEIGHTS:
                cls, far = args[0], real(args[1])
                await_bytes(stretch(cls, far * planes + q, 1), w_recv.at[cls, far])
            elif kind == HOPS:
                await_bytes(stretch(args[0], 0, 2 * groups), h_rest.at[args[0]])
            elif kind == CORES:
                key, c = args
                if key:
                    await_bytes(nm.at[pl.ds(0, groups * few), :], f_recv.at[1 + c])
                else:
                    await_bytes(nt.at[pl.ds(0, groups * own), :], f_recv.at[0])
            else:
                makers[kind](me, *args, True).wait_recv()
            return
        if kind == HOP and args[1] == me and args[2] == OWN_FIRST[args[0], me]:
            for i, keep in enumerate(keeps):
                if CLASS_OF[i] == args[0]:
                    keep.wait()
        if kind == SUM:
            which, c, side, d = args
            move = 1 - 2 * side
            value = pair(which, c, real(me + move * d))
            if 0 <= me - move < groups:
                value = value + rb[which][c, flip(side), d].astype(jnp.float32)
            sb[which][c, flip(side), d] = value.astype(jnp.bfloat16)
        makers[kind](me, *args).start()

    def perform(stage):
        for me, ops in enumerate(PLAN):
            @pl.when(place_z == me)
            def _():
                for op in ops[stage]:
                    act(me, op)

    def multiply(left, weight, which, c):
        value = jnp.dot(
            left[rows(c, groups * span_c), :], weight[...], preferred_element_type=jnp.float32
        ).astype(jnp.bfloat16)
        for g in range(groups):
            part[which][c, 0, g] = value[g * span_c : g * span_c + few]
            part[which][c, 1, g] = value[g * span_c + few : (g + 1) * span_c]
        exchange(which, c).start()

    def collect(which, c):
        acc[c] = pair(which, c, z)
        for side, has in ((0, z > 0), (1, z < groups - 1)):
            @pl.when(has)
            def _():
                acc[c] = acc[c] + rb[which][c, side, 0].astype(jnp.float32)
        return acc[c]

    def natural(c, core):
        return pl.ds(pl.multiple_of(c * span_c + core * few, few), few)

    head = tp * groups + z
    chunk = groups * length // 2

    def project(at):
        span = rows(at, chunk)
        qkvg[span, :] = jnp.dot(
            nt[span, :], w1[:, pl.ds(0, 2 * cq + cv)], preferred_element_type=jnp.float32
        ).astype(jnp.bfloat16)

    def gate(at):
        span = rows(at, chunk)
        gates = jnp.dot(
            nt[span, :], w1[:, pl.ds(2 * cq + cv, cv)], preferred_element_type=jnp.float32
        ).astype(jnp.bfloat16).astype(jnp.float32)
        whole = (held_kept[span, :] * mixer_gain[:, lanes(z, cv)] * silu(gates)).astype(jnp.bfloat16)
        for i in range(chunk // length):
            for c in range(CHUNKS):
                first = i * length + c * span_c
                hid[rows(at * (chunk // length) + i + c * groups, span_c), :] = whole[first : first + span_c]

    def two_parts(x):
        high = x.astype(jnp.bfloat16)
        return high, (x - high.astype(jnp.float32)).astype(jnp.bfloat16)

    def retain(first):
        log_gamma = gammas[pl.ds(head, 1), :]
        distance = (
            lax.broadcasted_iota(jnp.int32, (length, length), 0)
            - lax.broadcasted_iota(jnp.int32, (length, length), 1)
        ).astype(jnp.float32)
        decay = jnp.where(distance >= 0, jnp.exp(log_gamma * jnp.maximum(distance, 0.0)), 0.0)

        @pl.loop(first * groups // 2, (first + 1) * groups // 2)
        def _(at):
            span = rows(at, length)
            held = qkvg[span, pl.ds(0, 2 * cq)].astype(jnp.float32)

            def turn(x):
                return x * cos_t[...] + pltpu.roll(x, cq // 2, 1) * sin_t[...]

            rq = turn(held[:, :cq])
            rk = turn(held[:, cq : 2 * cq])
            q_high, q_low = two_parts(rq)
            k_high, k_low = two_parts(rk)
            scores = lax.dot_general(
                jnp.concatenate([q_high, q_high, q_low], axis=1),
                jnp.concatenate([k_high, k_low, k_high], axis=1),
                (((1,), (1,)), ((), ())), preferred_element_type=jnp.float32,
            ) * decay
            s_high, s_low = two_parts(scores)
            v_exact = qkvg[span, pl.ds(2 * cq, cv)]
            kept = jnp.dot(
                jnp.concatenate([s_high, s_low], axis=1),
                jnp.concatenate([v_exact, v_exact], axis=0), preferred_element_type=jnp.float32,
            )
            kept = kept * lax.rsqrt(jnp.mean(kept * kept, axis=-1, keepdims=True) + 1e-06)
            held_kept[span, :] = kept

    def renorm(c):
        middle = (
            tokens[natural(c, tp), :].astype(jnp.float32) + collect(0, c)
        ).astype(jnp.bfloat16).astype(jnp.float32)
        mid[c] = middle
        first = c * groups * span_c + z * span_c + tp * few
        nm[pl.ds(pl.multiple_of(first, few), few), :] = normed_rows(middle, channel_gain[...])

    place = lax.rem(lax.broadcasted_iota(jnp.int32, (groups * span_c, 1), 0), span_c)

    def convolve(c, low, taps):
        x = both[c, :, low : low + cf].astype(jnp.float32)
        count = taps.shape[0]
        weights = taps[:, lanes(z, cf)]
        result = x * weights[count - 1 :, :]
        for back in range(1, count):
            if c:
                before = both[c - 1, :, low : low + cf].astype(jnp.float32)
                before = pltpu.roll(before, back + (groups - 1) * span_c, 0)
            else:
                before = 0.0
            moved = jnp.where(place >= back, pltpu.roll(x, back, 0), before)
            result = result + moved * weights[count - 1 - back : count - back, :]
        return result

    def mix(c):
        both[c] = jnp.dot(
            nm[rows(c, groups * span_c), :], wlr[...], preferred_element_type=jnp.float32
        ).astype(jnp.bfloat16)
        gated[rows(c, groups * span_c), :] = (
            silu(convolve(c, 0, taps_left)) * convolve(c, cf, taps_right)
        ).astype(jnp.bfloat16)

    def finish(c):
        mine = natural(c, tp)
        fin[c] = (mid[c] + collect(1, c)).astype(jnp.bfloat16)
        remote(fin.at[c], out.at[mine, :], o_send.at[0], o_recv.at[0], partner).start()
        pltpu.make_async_copy(fin.at[c], out.at[mine, :], store_sem.at[0]).start()

    steps = (
        project,
        retain,
        lambda c: multiply(hid, wout, 0, c),
        renorm,
        mix,
        lambda c: multiply(gated, wdown, 1, c),
        finish,
        prepare,
        gate,
    )
    perform(0)
    for stage, (name, index) in enumerate(STAGES):
        steps[name](index)
        perform(stage + 1)
    await_bytes(fin, o_recv.at[0])
    await_bytes(fin, o_send.at[0])
    for key, buf in ((0, nt), (1, nm)):
        await_bytes(buf.at[pl.ds(0, groups * own), :], f_send.at[key])
        await_bytes(part[key].at[:, 0], x_send.at[key])
        await_bytes(sb[key].at[:, 0, pl.ds(0, groups - 1)], r_send.at[key])
    for cls in range(max(CLASS_OF) + 1):
        await_bytes(stretch(cls, 0, 3 * groups), h_send.at[cls])
    for i, (_, dst) in enumerate(pieces):
        if i == 4 or i == 7:
            ref = (wout if i == 4 else wdown).at[:, pl.ds(0, (groups - 1) * nb)]
        else:
            ref = (w1 if i < 4 else wlr).at[pl.ds(0, (groups - 1) * kb), pl.ds(starts[i], widths[i])]
        await_bytes(ref, w_send.at[i])
    for me, ops in enumerate(PLAN):
        @pl.when(place_z == me)
        def _():
            for key, buf, size in ((0, nt, part_rows), (1, nm, few)):
                count = sum(op[:3] == (1, 0, key) for stage in ops for op in stage)
                await_bytes(buf.at[pl.ds(0, count * size), :], a_send.at[key])
    pltpu.make_async_copy(fin, fin, store_sem.at[0]).wait()


def body(n_fs, *args):
    (tokens, norm_gain, w_query, w_key, w_value, w_gate, mixer_gain, w_out, channel_gain,
     w_left, w_right, taps_left, taps_right, w_down) = args
    groups = w_query.shape[1] // DK
    if (
        groups != 2 * len(PLAN)
        or n_fs % groups
        or n_fs != 4 * groups
        or lax.axis_size("tp") != 2
        or tokens.shape[0] != BLOCK
        or (w_left.shape[1] // groups) % 128
        or w_left.shape[1] % groups
        or w_out.shape[1] % 128
        or w_query.shape[0] % 32
        or tokens.shape[0] % (32 * CHUNKS)
    ):
        return plain_body(*args)
    length, width = tokens.shape
    heads = groups * lax.axis_size("tp")
    cq, cv, cf = w_query.shape[1] // groups, w_value.shape[1] // groups, w_left.shape[1] // groups
    planes = n_fs // groups
    span_c = length // CHUNKS
    few = span_c // 2
    classes = max(CLASS_OF) + 1
    cos_t, sin_t = turning(length, DK)
    gammas = log_gammas(heads)
    held = pl.BlockSpec(memory_space=pl.ANY)
    bf, f32, dma = jnp.bfloat16, jnp.float32, pltpu.SemaphoreType.DMA
    return pl.pallas_call(
        functools.partial(layer_kernel, n_fs, groups),
        out_shape=jax.ShapeDtypeStruct(tokens.shape, bf),
        in_specs=[held] * 17,
        out_specs=held,
        scratch_shapes=[
            pltpu.VMEM(tokens.shape, bf),
            pltpu.VMEM((1, width), f32),
            pltpu.VMEM((1, w_value.shape[1]), f32),
            pltpu.VMEM((1, width), f32),
            pltpu.VMEM(taps_left.shape, f32),
            pltpu.VMEM(taps_right.shape, f32),
            pltpu.VMEM(cos_t.shape, f32),
            pltpu.VMEM(sin_t.shape, f32),
            pltpu.VMEM(gammas.shape, f32),
            pltpu.VMEM((width, 2 * cq + 2 * cv), bf),
            pltpu.VMEM((cv, width), bf),
            pltpu.VMEM((width, 2 * cf), bf),
            pltpu.VMEM((cf, width), bf),
            pltpu.VMEM((groups * length, width), bf),
            pltpu.VMEM((groups * length, width), bf),
            pltpu.VMEM((groups * length, 2 * cq + cv), bf),
            pltpu.VMEM((groups * length, cv), f32),
            pltpu.VMEM((groups * length, cv), bf),
            pltpu.VMEM((groups * length, cf), bf),
            pltpu.VMEM((CHUNKS, 2, groups, few, width), bf),
            pltpu.VMEM((CHUNKS, 2, groups, few, width), bf),
            pltpu.VMEM((CHUNKS, groups, few, width), bf),
            pltpu.VMEM((CHUNKS, groups, few, width), bf),
            pltpu.VMEM((CHUNKS, 2, groups, few, width), bf),
            pltpu.VMEM((CHUNKS, 2, groups, few, width), bf),
            pltpu.VMEM((CHUNKS, 2, groups, few, width), bf),
            pltpu.VMEM((CHUNKS, 2, groups, few, width), bf),
            pltpu.VMEM((CHUNKS, few, width), f32),
            pltpu.VMEM((CHUNKS, few, width), f32),
            pltpu.VMEM((CHUNKS, groups * span_c, 2 * cf), bf),
            pltpu.VMEM((CHUNKS, few, width), bf),
            dma((8,)),
            dma((classes, groups)),
            dma((8,)),
            dma((classes,)),
            dma((classes, groups, 2)),
            dma((classes,)),
            dma((2,)),
            dma((max(NT_PARTS, CHUNKS), groups)),
            dma((2,)),
            dma((1 + CHUNKS,)),
            dma((2,)),
            dma((CHUNKS,)),
            dma((2,)),
            dma((CHUNKS, 2, groups - 1)),
            dma((1,)),
            dma((1,)),
            dma((9,)),
            dma((1,)),
        ],
        compiler_params=pltpu.CompilerParams(
            collective_id=0, has_side_effects=True, vmem_limit_bytes=60 * 1024 * 1024
        ),
    )(
        tokens, norm_gain[None], w_query, w_key, w_value, w_gate, mixer_gain[None], w_out,
        channel_gain[None], w_left, w_right, taps_left, taps_right, w_down,
        cos_t, sin_t, gammas,
    )


def solution(mesh):
    placed = (
        P("fs", None),
        P(),
        P("fs", "tp"),
        P("fs", "tp"),
        P("fs", "tp"),
        P("fs", "tp"),
        P("tp"),
        P("tp", "fs"),
        P(),
        P("fs", "tp"),
        P("fs", "tp"),
        P(None, "tp"),
        P(None, "tp"),
        P("tp", "fs"),
    )
    return jax.shard_map(
        functools.partial(body, mesh.shape["fs"]), mesh=mesh, in_specs=placed, out_specs=P("fs", None), check_vma=False)
```
